32 devices in a mesh: sp: 8 (over z, x), tp: 4 (over y, core).
Axes of the slice: x: 2, y: 2, z: 4, core: 2. Of those that a mesh axis runs over, the one named last changes fastest.
Arguments:
- tokens: bfloat16 [4096, 4096], P('sp', 'tp'), may hold values from -8 to 8
- w_key: bfloat16 [4096, 2048], P(None, 'tp'), may hold values from -0.09375 to 0.09375
- w_value: bfloat16 [4096, 2048], P(None, 'tp'), may hold values from -0.09375 to 0.09375
- w_beta: bfloat16 [4096, 16], replicated, may hold values from -0.09375 to 0.09375
- w_decay: bfloat16 [4096, 16], replicated, may hold values from -0.09375 to 0.09375
- beta_bias: float32 [16], replicated, may hold values from -6 to -4
- decay_rate: float32 [16], replicated, as said below
- forgetting_increment: float32 [16, 4096], P('tp', 'sp')
- new_query: bfloat16 [16, 128], P('tp', 'sp'), may hold values from -6 to 6
- read_gain: bfloat16 [128], replicated, may hold values from 0.099609375 to 1.8984375
Outputs:
- state_cache: bfloat16 [16, 128, 128], P('tp', 'sp')
- first_read: float32 [16, 128], P('tp')
The draws below stay inside these ranges and needn't reach their ends.
Inputs may be any that keep to these rules, and one draw needn't show every extreme that they name: `decay_rate`: positive.
All inputs are finite; a program needn't handle non-finite values.
Results may differ from the reference program's by a relative error of at most 0.0075.
Values may be sent and summed in bfloat16 or wider, within the bound.
No kernel may reach another device: no remote copies, remote signals or barrier semaphores. Data moves between devices by JAX's collectives and lax.ppermute only.
A program may use at most 64 MiB of HBM per device.

```python
import math
import jax
import jax.numpy as jnp
from jax import lax

D = 4096
HEADS = 16
DK = 128
DV = 128
BLOCK = 64
LENGTH = 4096


def draw_tokens(key, part):
    perturbation_seed, common_key = jax.random.split(key, 2)
    blocks = LENGTH // BLOCK
    noise = jnp.clip(jax.random.normal(perturbation_seed, (LENGTH, D), jnp.float32), -4.5, 4.5)
    common = jnp.clip(jax.random.normal(common_key, (blocks, D), jnp.float32), -4.5, 4.5)
    mixed = noise + 0.7 * jnp.repeat(common, BLOCK, axis=0)
    return mixed.astype(jnp.bfloat16)


def draw_decay_rate(key, part):
    slow_key, fast_key, pick_key = jax.random.split(key, 3)
    slow = jnp.exp(jax.random.uniform(slow_key, (HEADS,), jnp.float32, math.log(0.2 / LENGTH), math.log(1.0 / LENGTH)))
    fast = jnp.exp(jax.random.uniform(fast_key, (HEADS,), jnp.float32, math.log(0.02), math.log(0.06)))
    picked = jax.random.bernoulli(pick_key, 0.5, (HEADS,))
    return jnp.where(picked, fast, slow)


def draw_forgetting_increment(key, part):
    scale_key, location_seed, drop_key = jax.random.split(key, 3)
    blocks = LENGTH // BLOCK
    factor = jnp.exp(jax.random.uniform(scale_key, (HEADS, blocks), jnp.float32, math.log(0.25), math.log(4.0)))
    starting_displacement = -jnp.repeat(factor, BLOCK, axis=1) / LENGTH
    location_positions = jax.random.randint(location_seed, (HEADS, 4), 0, LENGTH)
    discarded_elements = jnp.log(jax.random.uniform(drop_key, (HEADS, 4), jnp.float32, 0.5, 0.8))
    breadth_across = jnp.arange(LENGTH)
    cluster_batches = jnp.sum(jnp.where(breadth_across[None, None, :] == location_positions[:, :, None], discarded_elements[:, :, None], 0.0), axis=1)
    return starting_displacement + cluster_batches


def levels(stream_key, dims, shards, least, largest):
    level, own = 1.0, jax.random.fold_in(stream_key, 6)
    for dim, shards_of in shards:
        draws = jnp.exp(jax.random.uniform(jax.random.fold_in(own, dim), (shards_of,), jnp.float32, least / len(shards), largest / len(shards)))
        level = level * jnp.repeat(draws, dims[dim] // shards_of).reshape([-1 if axis == dim else 1 for axis in range(len(dims))])
    return level


def centred(own_key, shape, scale, limit, pieces=(), kind=jnp.bfloat16):
    array = jax.random.normal(own_key, shape, jnp.float32) * scale
    if len(pieces) > 0:
        array = levels(own_key, shape, pieces, -0.22, 0.18) * array
    return jnp.clip(array, min=-limit, max=limit).astype(kind)


def setup_inputs(seed: int = 0) -> dict:
    streams_of = jax.random.split(jax.random.key(seed), 11)
    return {
        "tokens": draw_tokens(jax.random.fold_in(streams_of[10], 71), 0),
        "w_key": centred(streams_of[1], (D, HEADS * DK), D ** -0.5, 0.09375, ((1, 4),)),
        "w_value": centred(streams_of[2], (D, HEADS * DV), D ** -0.5, 0.09375, ((1, 4),)),
        "w_beta": centred(streams_of[3], (D, HEADS), D ** -0.5, 0.09375),
        "w_decay": centred(streams_of[4], (D, HEADS), D ** -0.5, 0.09375),
        "beta_bias": jnp.clip(jax.random.uniform(streams_of[5], (HEADS,), jnp.float32, -6.0, -4.0), -6.0, -4.0),
        "decay_rate": draw_decay_rate(jax.random.fold_in(streams_of[10], 71), 0),
        "forgetting_increment": draw_forgetting_increment(jax.random.fold_in(streams_of[10], 71), 0),
        "new_query": centred(streams_of[8], (HEADS, DK), 1.0, 6.0, ((0, 4), (1, 8))),
        "read_gain": jnp.clip(1.0 + 0.18 * jax.random.normal(streams_of[9], (DV,), jnp.float32), 0.099609375, 1.8984375).astype(jnp.bfloat16),
    }


norm_eps = 1e-06

def matmul_f32(left, right):
    return jnp.dot(left, right, precision=lax.Precision.HIGHEST)

def unit_inverse(lower):
    current_size = lower.shape[0]
    identity = jnp.eye(current_size, dtype=jnp.float32)
    result = identity - lower
    lower_power = lower
    covered = 2
    while covered < current_size:
        lower_power = matmul_f32(lower_power, lower_power)
        result = matmul_f32(result, identity + lower_power)
        covered = covered * 2
    return result

def block_terms(key_blk, value_blk, beta_blk, logd_blk):
    current_size = key_blk.shape[0]
    cumulative = jnp.cumsum(logd_blk)
    spread = cumulative[:, None] - cumulative[None, :]
    location_positions = jnp.arange(current_size)
    causal = location_positions[:, None] >= location_positions[None, :]
    strict = location_positions[:, None] > location_positions[None, :]
    decay_table = jnp.where(causal, jnp.exp(jnp.where(causal, spread, 0.0)), 0.0)
    key_beta = key_blk * beta_blk[:, None]
    lower = jnp.where(strict, matmul_f32(key_beta, key_blk.T) * decay_table, 0.0)
    inverse = unit_inverse(lower)
    update = matmul_f32(inverse, value_blk * beta_blk[:, None])
    erase = matmul_f32(inverse, key_beta * jnp.exp(cumulative)[:, None])
    key_remainder = key_blk * jnp.exp(cumulative[-1] - cumulative)[:, None]
    return (update, erase, key_remainder, jnp.exp(cumulative[-1]))

def reference(tokens, w_key, w_value, w_beta, w_decay, beta_bias, decay_rate, forgetting_increment, new_query, read_gain):
    key_raw = jnp.dot(tokens, w_key, preferred_element_type=jnp.float32).astype(jnp.bfloat16)
    value_raw = jnp.dot(tokens, w_value, preferred_element_type=jnp.float32).astype(jnp.bfloat16)
    key_wide = lax.optimization_barrier(key_raw).astype(jnp.float32).reshape(LENGTH, HEADS, DK)
    key_unit = key_wide * lax.rsqrt(lax.optimization_barrier(jnp.sum(key_wide * key_wide, axis=-1, keepdims=True)) + norm_eps)
    value_wide = lax.optimization_barrier(value_raw).astype(jnp.float32).reshape(LENGTH, HEADS, DV)
    beta = jax.nn.sigmoid(jnp.dot(tokens, w_beta, preferred_element_type=jnp.float32) + beta_bias)
    log_decay = -decay_rate * jax.nn.softplus(jnp.dot(tokens, w_decay, preferred_element_type=jnp.float32)) + forgetting_increment.T
    blocks = LENGTH // BLOCK
    key_heads = key_unit.transpose(1, 0, 2).reshape(HEADS, blocks, BLOCK, DK)
    value_heads = value_wide.transpose(1, 0, 2).reshape(HEADS, blocks, BLOCK, DV)
    beta_heads = beta.T.reshape(HEADS, blocks, BLOCK)
    logd_heads = log_decay.T.reshape(HEADS, blocks, BLOCK)
    terms = jax.vmap(jax.vmap(block_terms))(key_heads, value_heads, beta_heads, logd_heads)
    inputs = tuple((jnp.moveaxis(item, 1, 0) for item in terms))

    def advance(state, block_in):
        update, erase, key_remainder, keep = block_in
        fresh = update - jnp.einsum('hcd,hde->hce', erase, state, precision=lax.Precision.HIGHEST)
        state = keep[:, None, None] * state + jnp.einsum('hcd,hce->hde', key_remainder, fresh, precision=lax.Precision.HIGHEST)
        return (state, None)
    final_state, _ = lax.scan(advance, jnp.zeros((HEADS, DK, DV), jnp.float32), inputs)
    state_cache = final_state.astype(jnp.bfloat16)
    raw_read = lax.optimization_barrier(jnp.sum(new_query.astype(jnp.float32)[:, :, None] * state_cache.astype(jnp.float32), axis=1))
    first_read = raw_read * lax.rsqrt(lax.optimization_barrier(jnp.mean(raw_read * raw_read, axis=-1, keepdims=True)) + norm_eps) * read_gain.astype(jnp.float32)
    return (state_cache, first_read)
```

```python
import functools

import jax
import jax.numpy as jnp
from jax import lax
from jax.experimental import pallas as pl
from jax.experimental.pallas import tpu as pltpu
from jax.sharding import PartitionSpec as P

DK = 128
DV = 128
CHUNK = 128
SUB = 8

norm_eps = 1e-06
bf16 = jnp.bfloat16
f32 = jnp.float32


def flip(axis, mask):
    return [(i, i ^ mask) for i in range(lax.axis_size(axis))]


def swap(x, axis, mask):
    return lax.ppermute(x, axis, flip(axis, mask))


def dot(left, right):
    return jnp.dot(left.astype(bf16), right.astype(bf16), preferred_element_type=f32)


def dot_exact(left, right):
    return jnp.dot(left, right, precision=lax.Precision.HIGHEST, preferred_element_type=f32)


def dot_nt(left, right):
    return lax.dot_general(
        left.astype(bf16), right.astype(bf16), (((1,), (1,)), ((), ())), preferred_element_type=f32
    )


def dot_tn(left, right):
    return lax.dot_general(
        left.astype(bf16), right.astype(bf16), (((0,), (0,)), ((), ())), preferred_element_type=f32
    )


def unit_inverses(lowers, size):
    row = lax.broadcasted_iota(jnp.int32, (size, size), 0)
    col = lax.broadcasted_iota(jnp.int32, (size, size), 1)
    identity = jnp.where(row == col, 1.0, 0.0)

    def same(width):
        return (row // width) == (col // width)

    width = min(16, size)
    inner = [jnp.where(same(width), low, 0.0) for low in lowers]
    results = [identity - low for low in inner]
    powers = inner
    covered = 2
    while covered < width:
        powers = [dot(p, p) for p in powers]
        results = [r + dot(r, p) for r, p in zip(results, powers)]
        covered *= 2
    while width < size:
        off = jnp.logical_and(same(2 * width), jnp.logical_not(same(width)))
        right = [dot(jnp.where(off, low, 0.0), r) for low, r in zip(lowers, results)]
        results = [r - dot(r, x) for r, x in zip(results, right)]
        width *= 2
    return results


def chunk_kernel(ranks, heads, first, pieces, *refs):
    order_ref, lead_ref = refs[0], refs[1]
    piece_refs = refs[2 : 2 + pieces]
    wk_ref, wv_ref, wg_ref, bias_ref, rate_ref, forget_ref = refs[2 + pieces : 8 + pieces]
    rest = refs[8 + pieces :]
    if first:
        state_ref = None
    else:
        state_ref, rest = rest[0], rest[1:]
    last = len(rest) > 1
    size = piece_refs[0].shape[0]
    width = piece_refs[0].shape[1]

    key_acc = value_acc = gate_acc = None
    for p, piece_ref in enumerate(piece_refs):
        rows = pl.ds(pl.multiple_of(order_ref[p] * width, width), width)
        x = piece_ref[...]
        k = jnp.dot(x, wk_ref[rows, :], preferred_element_type=f32)
        v = jnp.dot(x, wv_ref[rows, :], preferred_element_type=f32)
        g = jnp.dot(x, wg_ref[rows, :], preferred_element_type=f32)
        key_acc = k if key_acc is None else key_acc + k
        value_acc = v if value_acc is None else value_acc + v
        gate_acc = g if gate_acc is None else gate_acc + g

    key_raw = key_acc.astype(bf16).astype(f32)
    value_raw = value_acc.astype(bf16).astype(f32)
    lanes = gate_acc.shape[1]
    gates = gate_acc.T
    beta_row = jax.nn.sigmoid(gates[0:SUB] + bias_ref[...][:, 0:1])
    log_row = -rate_ref[...][:, 0:1] * jax.nn.softplus(gates[SUB : 2 * SUB]) + forget_ref[...]
    row = lax.broadcasted_iota(jnp.int32, (size, size), 0)
    col = lax.broadcasted_iota(jnp.int32, (size, size), 1)
    upper = jnp.where(row <= col, 1.0, 0.0)
    cum_row = dot_exact(log_row, upper)
    total = cum_row[:, size - 1 : size]
    stacked = jnp.concatenate(
        [
            beta_row,
            cum_row,
            beta_row * jnp.exp(cum_row),
            jnp.exp(total - cum_row),
            jnp.zeros((lanes - 4 * SUB, size), f32),
        ],
        axis=0,
    )
    columns = stacked.T
    keep = jnp.exp(total)
    strict = row > col
    keys, lowers, base = [], [], []
    for h in range(heads):
        kw = key_raw[:, h * DK : (h + 1) * DK]
        ku = kw * lax.rsqrt(jnp.sum(kw * kw, axis=-1, keepdims=True) + norm_eps)
        beta = columns[:, h : h + 1]
        cum = columns[:, SUB + h : SUB + h + 1]
        spread = jnp.where(strict, cum - cum_row[h : h + 1, :], 0.0)
        table = jnp.where(strict, jnp.exp(spread), 0.0)
        keys.append(ku)
        lowers.append(dot_nt(ku, ku) * table * beta)
    if first:
        kr = lax.broadcasted_iota(jnp.int32, (DK, DV + DK), 0)
        kc = lax.broadcasted_iota(jnp.int32, (DK, DV + DK), 1)
        start = jnp.where(kc == kr + DV, 1.0, 0.0)
        states = [start] * heads
    else:
        states = [state_ref[h] for h in range(heads)]
    for h in range(heads):
        beta = columns[:, h : h + 1]
        erase = keys[h] * columns[:, 2 * SUB + h : 2 * SUB + h + 1]
        value = value_raw[:, h * DV : (h + 1) * DV] * beta
        padded = jnp.concatenate([value, jnp.zeros((size, DK), f32)], axis=1)
        base.append(padded - dot(erase, states[h]))
    inverses = unit_inverses(lowers, size)
    fresh = [dot(inv, b) for inv, b in zip(inverses, base)]
    for h in range(heads):
        remain = keys[h] * columns[:, 3 * SUB + h : 3 * SUB + h + 1]
        new = keep[h : h + 1, :] * states[h] + dot_tn(remain, fresh[h])
        rest[-1][h] = new
    if last:
        lead = lead_ref[0]
        for k in range(heads):
            rest[k][...] = rest[-1][lead ^ k].astype(bf16)


def compose(pairs):
    while len(pairs) > 1:
        merged = []
        for early, late in zip(pairs[0::2], pairs[1::2]):
            new = dot_exact(late[:, DV:], early)
            merged.append(
                jnp.concatenate([new[:, :DV] + late[:, :DV], new[:, DV:]], axis=1)
            )
        pairs = merged
    return pairs[0]


def split(x):
    high = x.astype(bf16)
    return high, (x - high.astype(f32)).astype(bf16)


def pad_rows(x, rows):
    return jnp.concatenate([x, jnp.zeros((rows - x.shape[0], x.shape[1]), x.dtype)], axis=0)


def message(high, own, query):
    half = DK // 2
    through = dot_exact(query, own)
    a, b = own[:, DV:], own[:, :DV]
    body = jnp.where(high, jnp.concatenate([a[:half], b[:half]], axis=0), b)
    ah, al = split(through[0:1, DV:])
    bh, bl = split(through[0:1, :DV])
    tail = pad_rows(jnp.concatenate([ah, al, bh, bl], axis=0).astype(f32), 16)
    return jnp.concatenate([body, tail], axis=0).astype(bf16)


def compose_kernel(heads, groups, lead_ref, *refs):
    own_ref, got = refs[0], refs[1:heads]
    query_ref = refs[heads]
    out = refs[heads + 1 :]
    lead = lead_ref[0]
    map_ref, scratch = out[0], out[-1]
    scratch[lead] = own_ref[...].astype(f32)
    for k in range(1, heads):
        scratch[lead ^ k] = got[k - 1][...].astype(f32)
    total = compose([scratch[i] for i in range(heads)])
    map_ref[...] = total
    if groups == 2:
        out[1][...] = message(lead_ref[1] == 1, total, query_ref[...])


def merge_kernel(final, high_ref, own_ref, got_ref, query_ref, map_ref, send_ref=None):
    high = high_ref[0] == 1
    own, got = own_ref[...], got_ref[...].astype(f32)
    early, late = jnp.where(high, got, own), jnp.where(high, own, got)
    total = compose([early, late])
    map_ref[...] = total
    if final:
        send_ref[...] = message(high_ref[1] == 1, total, query_ref[...])


def rows_kernel(heads, groups, rows, lead_ref, own_ref, *refs):
    if groups > 1:
        got_ref, refs = refs[0], refs[1:]
    query_ref, refs = refs[0], refs[1:]
    scratch = refs[-1]
    lead = lead_ref[0]
    own = own_ref[...]
    half = DK // 2
    if groups > 1:
        high = lead_ref[1] == 1
        got = got_ref[...].astype(f32)
        a, b = own[:, DV:], own[:, :DV]
        early = jnp.where(high, got[:DK], b)
        late_a = jnp.where(high, a[half:], got[:half])
        late_b = jnp.where(high, b[half:], got[half:DK])
        mine = dot_exact(query_ref[...], own)
        through_a = jnp.where(high, mine[0:1, DV:], got[DK : DK + 1] + got[DK + 1 : DK + 2])
        through_b = jnp.where(high, mine[0:1, :DV], got[DK + 2 : DK + 3] + got[DK + 3 : DK + 4])
        both = dot_exact(pad_rows(jnp.concatenate([late_a, through_a], axis=0), half + 8), early)
        state = both[:half] + late_b
        read = both[half : half + 1] + through_b
    else:
        state = own[:, :DV]
        read = dot_exact(query_ref[...], own)[0:1, :DV]
    members = state.shape[0] // rows
    for i in range(members):
        scratch[i] = state[i * rows : (i + 1) * rows]
    place = lead_ref[2]
    rh, rl = split(read)
    tail = pad_rows(jnp.concatenate([rh, rl], axis=0).astype(f32), 16)
    for k in range(heads):
        body = scratch[place ^ k]
        refs[k][...] = jnp.concatenate([body, tail], axis=0).astype(bf16)


def final_kernel(heads, rows, lead_ref, gain_ref, *refs):
    lead = lead_ref[0]
    state_ref, read_ref, scratch = refs[heads:]
    for k in range(heads):
        part = refs[k][...]
        state_ref[lead ^ k] = part[:rows]
        wide = part[rows : rows + 2].astype(f32)
        scratch[lead ^ k] = jnp.broadcast_to(wide[0:1] + wide[1:2], (SUB, DV))
    raw = jnp.concatenate([scratch[h][0:1] for h in range(heads)], axis=0)
    norm = lax.rsqrt(jnp.mean(raw * raw, axis=-1, keepdims=True) + norm_eps)
    read_ref[...] = raw * norm * gain_ref[...]


def shape(dims, dtype=f32):
    return jax.ShapeDtypeStruct(dims, dtype)


smem = pl.BlockSpec(memory_space=pltpu.SMEM)
vmem = pl.BlockSpec(memory_space=pltpu.VMEM)


def params(mib):
    return pltpu.CompilerParams(vmem_limit_bytes=mib * 1024 * 1024)


def call(body, scalars, arrays, outs, scratch=(), mib=8, flops=0):
    return pl.pallas_call(
        body,
        out_shape=outs,
        in_specs=[smem] * len(scalars) + [vmem] * len(arrays),
        out_specs=jax.tree.map(lambda _: vmem, outs),
        scratch_shapes=list(scratch),
        compiler_params=params(mib),
        cost_estimate=pl.CostEstimate(flops=flops, bytes_accessed=0, transcendentals=0)
        if flops
        else None,
    )(*scalars, *arrays)


def per_device(
    tokens,
    w_key,
    w_value,
    w_beta,
    w_decay,
    beta_bias,
    decay_rate,
    forgetting_increment,
    new_query,
    read_gain,
):
    heads = w_key.shape[1] // DK
    length, width = tokens.shape
    count, place = lax.axis_size("sp"), lax.axis_index("sp")
    ranks, rank = lax.axis_size("tp"), lax.axis_index("tp")
    groups = count // heads
    rows = DK // count
    lead = place % heads
    chunk = min(CHUNK, length)
    chunks = length // chunk
    start = rank * heads

    owns = [tokens[c * chunk : (c + 1) * chunk] for c in range(chunks)]
    gathered = []
    for c in range(chunks):
        found = [(0, owns[c])]
        pair = ranks // 2
        current = owns[c]
        for hop in range(1, pair):
            found.append((2 * hop, swap(owns[c], "tp", 2 * hop)))
        found = found + [(m ^ 1, swap(x, "tp", 1)) for m, x in found]
        gathered.append(found)

    def head_slice(x):
        part = lax.dynamic_slice_in_dim(x, start, heads, x.ndim - 1)
        return jnp.pad(part, [(0, 0)] * (x.ndim - 1) + [(0, SUB - heads)])

    gate_weights = jnp.pad(
        jnp.concatenate([head_slice(w_beta), head_slice(w_decay)], axis=1),
        ((0, 0), (0, DK - 2 * SUB)),
    )
    bias = jnp.broadcast_to(head_slice(beta_bias)[:, None], (SUB, DK))
    rate = jnp.broadcast_to(head_slice(decay_rate)[:, None], (SUB, DK))
    forget = jnp.pad(forgetting_increment, ((0, SUB - heads), (0, 0)))
    gain = read_gain.astype(f32)[None, :]

    seat = lax.broadcasted_iota(jnp.int32, (count, heads, rows), 0)
    query = jnp.where(seat == place, new_query[None], jnp.zeros((), bf16))
    mask = 1
    while mask < count:
        query = query + swap(query, "sp", mask)
        mask *= 2
    query = lax.dynamic_index_in_dim(query, lead, 1, False).reshape(1, DK).astype(f32)
    query = jnp.pad(query, ((0, SUB - 1), (0, 0)))

    lead_one = jnp.reshape(lead, (1,)).astype(jnp.int32)
    state = None
    flops = 2 * chunk * width * ranks * (2 * heads * DK + DK) + heads * 24 * 2 * chunk * chunk * DK
    for c in range(chunks):
        found = gathered[c]
        order = jnp.stack([rank ^ m for m, _ in found]).astype(jnp.int32)
        first, last = c == 0, c == chunks - 1
        arrays = [x for _, x in found] + [
            w_key,
            w_value,
            gate_weights,
            bias,
            rate,
            forget[:, c * chunk : (c + 1) * chunk],
        ]
        if not first:
            arrays.append(state)
        outs = [shape((heads, DK, DV + DK))]
        if last:
            outs = [shape((DK, DV + DK), bf16)] * heads + outs
        result = call(
            functools.partial(chunk_kernel, ranks, heads, first, len(found)),
            [order, lead_one],
            arrays,
            outs,
            mib=28,
            flops=flops,
        )
        state = result[-1]
    maps = result[:heads]

    got = [swap(maps[k], "sp", k) for k in range(1, heads)]
    top = (place // (count // 2)) % 2
    info = jnp.stack([lead, top]).astype(jnp.int32)
    outs = [shape((DK, DV + DK))]
    if groups == 2:
        outs.append(shape((DK + 16, DV), bf16))
    result = call(
        functools.partial(compose_kernel, heads, groups),
        [info],
        [maps[0], *got, query],
        outs,
        [pltpu.VMEM((heads, DK, DV + DK), f32)],
    )
    total = result[0]
    mask = heads
    while 2 * mask < count:
        final = 4 * mask == count
        high = (place // mask) % 2
        partner = swap(total.astype(bf16), "sp", mask)
        outs = [shape((DK, DV + DK))]
        if final:
            outs.append(shape((DK + 16, DV), bf16))
        result = call(
            functools.partial(merge_kernel, final),
            [jnp.stack([high, top]).astype(jnp.int32)],
            [total, partner, query],
            outs,
        )
        total = result[0]
        mask *= 2
    arrays = [total]
    if groups > 1:
        arrays.append(swap(result[1], "sp", count // 2))
    members = count // 2 if groups > 1 else count
    info = jnp.stack([lead, top, place % members]).astype(jnp.int32)
    parts = call(
        functools.partial(rows_kernel, heads, groups, rows),
        [info],
        arrays + [query],
        [shape((rows + 16, DV), bf16)] * heads,
        [pltpu.VMEM((members, rows, DV), f32)],
    )
    parts = [parts[0]] + [swap(parts[k], "sp", k) for k in range(1, heads)]
    own_rows, first_read = call(
        functools.partial(final_kernel, heads, rows),
        [lead_one],
        [gain, *parts],
        [shape((heads, rows, DV), bf16), shape((heads, DV))],
        [pltpu.VMEM((heads, SUB, DV), f32)],
    )
    return (own_rows, first_read)


def solution(mesh):
    return jax.shard_map(
        per_device,
        mesh=mesh,
        in_specs=(
            P("sp", "tp"),
            P(None, "tp"),
            P(None, "tp"),
            P(),
            P(),
            P(),
            P(),
            P("tp", "sp"),
            P("tp", "sp"),
            P(),
        ),
        out_specs=(P("tp", "sp", None), P("tp", None)),
        check_vma=False,
    )
```

```python
import functools

import jax
import jax.numpy as jnp
from jax import lax
from jax.experimental import pallas as pl
from jax.experimental.pallas import tpu as pltpu
from jax.sharding import PartitionSpec as P


DK = 128
DV = 128
CHUNK = 128
SUB = 8

norm_eps = 1e-06
bf16 = jnp.bfloat16
f32 = jnp.float32


def flip(axis, mask):
    return [(i, i ^ mask) for i in range(lax.axis_size(axis))]


def swap(x, axis, mask):
    return lax.ppermute(x, axis, flip(axis, mask))


def dot(left, right):
    return jnp.dot(left.astype(bf16), right.astype(bf16), preferred_element_type=f32)


def dot_exact(left, right):
    return jnp.dot(left, right, precision=lax.Precision.HIGHEST, preferred_element_type=f32)


def dot_nt(left, right):
    return lax.dot_general(
        left.astype(bf16), right.astype(bf16), (((1,), (1,)), ((), ())), preferred_element_type=f32
    )


def dot_tn(left, right):
    return lax.dot_general(
        left.astype(bf16), right.astype(bf16), (((0,), (0,)), ((), ())), preferred_element_type=f32
    )


def unit_inverses(lowers, size):
    row = lax.broadcasted_iota(jnp.int32, (size, size), 0)
    col = lax.broadcasted_iota(jnp.int32, (size, size), 1)
    identity = jnp.where(row == col, 1.0, 0.0)

    def same(width):
        return (row // width) == (col // width)

    width = min(16, size)
    inner = [jnp.where(same(width), low, 0.0) for low in lowers]
    results = [identity - low for low in inner]
    powers = inner
    covered = 2
    while covered < width:
        powers = [dot(p, p) for p in powers]
        results = [r + dot(r, p) for r, p in zip(results, powers)]
        covered *= 2
    while width < size:
        off = jnp.logical_and(same(2 * width), jnp.logical_not(same(width)))
        right = [dot(jnp.where(off, low, 0.0), r) for low, r in zip(lowers, results)]
        results = [r - dot(r, x) for r, x in zip(results, right)]
        width *= 2
    return results


def load_kernel(wk_hbm, wv_hbm, wk_ref, wv_ref, sems):
    copies = [
        pltpu.make_async_copy(wk_hbm, wk_ref, sems.at[0]),
        pltpu.make_async_copy(wv_hbm, wv_ref, sems.at[1]),
    ]
    for copy in copies:
        copy.start()
    for copy in copies:
        copy.wait()


def chunk_kernel(heads, index, last, masks, *refs):
    pieces = len(masks)
    piece_refs = refs[:pieces]
    wk_ref, wv_ref, wg_ref, small_ref, forget_ref = refs[pieces : pieces + 5]
    rest = refs[pieces + 5 :]
    if index > 0:
        state_ref, rest = rest[0], rest[1:]
    if last or index == 0:
        query_ref, rest = rest[0], rest[1:]
    if index == 0 and not last:
        rest[0][0:heads, :] = query_ref[...].astype(f32)
    size, width = piece_refs[0].shape
    rank = lax.axis_index("tp")
    starts = [pl.multiple_of((rank ^ m) * width, width) for m in masks]

    gates = None
    for start, piece_ref in zip(starts, piece_refs):
        g = dot_nt(wg_ref[:, pl.ds(start, width)], piece_ref[...])
        gates = g if gates is None else gates + g
    total_heads = heads * lax.axis_size("tp")
    lane = lax.broadcasted_iota(jnp.int32, (SUB, DK), 1)
    head = lax.broadcasted_iota(jnp.int32, (SUB, DK), 0) + rank * heads
    small = small_ref[0:1, :]
    bias = jnp.sum(jnp.where(lane == head, small, 0.0), axis=1, keepdims=True)
    rate = jnp.sum(jnp.where(lane == head + total_heads, small, 0.0), axis=1, keepdims=True)
    forget = forget_ref[:, index * size : (index + 1) * size]
    if heads < SUB:
        forget = jnp.concatenate([forget, jnp.zeros((SUB - heads, size), f32)], axis=0)
    beta_row = jax.nn.sigmoid(gates[0:SUB] + bias)
    log_row = forget - rate * jax.nn.softplus(gates[SUB : 2 * SUB])
    row = lax.broadcasted_iota(jnp.int32, (size, size), 0)
    col = lax.broadcasted_iota(jnp.int32, (size, size), 1)
    cum_row = dot_exact(log_row, jnp.where(row <= col, 1.0, 0.0))
    total = cum_row[:, size - 1 : size]
    stacked = jnp.concatenate(
        [
            beta_row,
            cum_row,
            beta_row * jnp.exp(cum_row),
            jnp.exp(total - cum_row),
            jnp.zeros((DK - 4 * SUB, size), f32),
        ],
        axis=0,
    )
    columns = stacked.T
    keep = jnp.exp(total)

    key_acc = value_acc = None
    for start, piece_ref in zip(starts, piece_refs):
        rows = pl.ds(start, width)
        x = piece_ref[...]
        k = jnp.dot(x, wk_ref[rows, :], preferred_element_type=f32)
        key_acc = k if key_acc is None else key_acc + k
    for start, piece_ref in zip(starts, piece_refs):
        rows = pl.ds(start, width)
        x = piece_ref[...]
        v = jnp.dot(x, wv_ref[rows, :], preferred_element_type=f32)
        value_acc = v if value_acc is None else value_acc + v
    key_raw = key_acc.astype(bf16).astype(f32)
    value_raw = value_acc.astype(bf16).astype(f32)

    strict = row > col
    keys, lowers, base = [], [], []
    for h in range(heads):
        kw = key_raw[:, h * DK : (h + 1) * DK]
        ku = kw * lax.rsqrt(jnp.sum(kw * kw, axis=-1, keepdims=True) + norm_eps)
        beta = columns[:, h : h + 1]
        cum = columns[:, SUB + h : SUB + h + 1]
        spread = jnp.where(strict, cum - cum_row[h : h + 1, :], 0.0)
        table = jnp.where(strict, jnp.exp(spread), 0.0)
        keys.append(ku)
        lowers.append(dot_nt(ku, ku) * table * beta)
    if index > 0:
        states = [state_ref[h] for h in range(heads)]
    else:
        kr = lax.broadcasted_iota(jnp.int32, (DK, DV + DK), 0)
        kc = lax.broadcasted_iota(jnp.int32, (DK, DV + DK), 1)
        states = [jnp.where(kc == kr + DV, 1.0, 0.0)] * heads
    for h in range(heads):
        beta = columns[:, h : h + 1]
        erase = keys[h] * columns[:, 2 * SUB + h : 2 * SUB + h + 1]
        value = value_raw[:, h * DV : (h + 1) * DV] * beta
        padded = jnp.concatenate([value, jnp.zeros((size, DK), f32)], axis=1)
        base.append(padded - dot(erase, states[h]))
    inverses = unit_inverses(lowers, size)
    fresh = [dot(inv, b) for inv, b in zip(inverses, base)]
    for h in range(heads):
        remain = keys[h] * columns[:, 3 * SUB + h : 3 * SUB + h + 1]
        new = keep[h : h + 1, :] * states[h] + dot_tn(remain, fresh[h])
        rest[-1][h] = new
    if last:
        lead = lax.axis_index("sp") % heads
        for k in range(heads):
            rest[k][0:DK, :] = rest[-1][lead ^ k].astype(bf16)
            asked = jnp.broadcast_to(query_ref[pl.ds(lead ^ k, 1), :].astype(f32), (2 * SUB, DK))
            asked = jnp.concatenate([asked, jnp.zeros((2 * SUB, DV), f32)], axis=1)
            rest[k][DK:, :] = asked.astype(bf16)


def compose(pairs):
    while len(pairs) > 1:
        merged = []
        for early, late in zip(pairs[0::2], pairs[1::2]):
            new = dot_exact(late[:, DV:], early)
            merged.append(
                jnp.concatenate([new[:, :DV] + late[:, :DV], new[:, DV:]], axis=1)
            )
        pairs = merged
    return pairs[0]


def split(x):
    high = x.astype(bf16)
    return high, (x - high.astype(f32)).astype(bf16)


def pad_rows(x, rows):
    return jnp.concatenate([x, jnp.zeros((rows - x.shape[0], x.shape[1]), x.dtype)], axis=0)


def message(high, own, query):
    half = DK // 2
    through = dot_exact(query, own)
    a, b = own[:, DV:], own[:, :DV]
    body = jnp.where(high, jnp.concatenate([a[:half], b[:half]], axis=0), b)
    ah, al = split(through[0:1, DV:])
    bh, bl = split(through[0:1, :DV])
    tail = pad_rows(jnp.concatenate([ah, al, bh, bl], axis=0).astype(f32), 16)
    return through, jnp.concatenate([body, tail], axis=0).astype(bf16)


def late_side(mask):
    return lax.rem(lax.div(lax.axis_index("sp"), jnp.int32(mask)), jnp.int32(2)) == 1


def finish(total, query, out):
    out[0][...] = total
    through, send = message(late_side(lax.axis_size("sp") // 2), total, query)
    out[1][...] = through
    if len(out) > 2:
        out[2][...] = send


def compose_kernel(heads, final, *refs):
    own_ref, got = refs[0], refs[1:heads]
    out, scratch = refs[heads:-1], refs[-1]
    lead = lax.axis_index("sp") % heads
    scratch[lead] = own_ref[:DK, :].astype(f32)
    query = own_ref[DK:, :DK].astype(f32)[:SUB]
    for k in range(1, heads):
        scratch[lead ^ k] = got[k - 1][:DK, :].astype(f32)
        query = query + got[k - 1][DK:, :DK].astype(f32)[:SUB]
    total = compose([scratch[i] for i in range(heads)])
    if final:
        finish(total, query, out)
    else:
        out[0][...] = total
        out[1][...] = query


def merge_kernel(mask, final, own_ref, got_ref, query_ref, *out):
    high = late_side(mask)
    own, got = own_ref[...], got_ref[...].astype(f32)
    early, late = jnp.where(high, got, own), jnp.where(high, own, got)
    total = compose([early, late])
    if final:
        finish(total, query_ref[...], out)
    else:
        out[0][...] = total
        out[1][...] = query_ref[...]


def rows_kernel(heads, groups, rows, own_ref, mine_ref, *refs):
    if groups > 1:
        got_ref, refs = refs[0], refs[1:]
    scratch = refs[-1]
    own, mine = own_ref[...], mine_ref[...]
    half = DK // 2
    place = lax.axis_index("sp")
    if groups > 1:
        high = late_side(lax.axis_size("sp") // 2)
        got = got_ref[...].astype(f32)
        a, b = own[:, DV:], own[:, :DV]
        early = jnp.where(high, got[:DK], b)
        late_a = jnp.where(high, a[half:], got[:half])
        late_b = jnp.where(high, b[half:], got[half:DK])
        through_a = jnp.where(high, mine[0:1, DV:], got[DK : DK + 1] + got[DK + 1 : DK + 2])
        through_b = jnp.where(high, mine[0:1, :DV], got[DK + 2 : DK + 3] + got[DK + 3 : DK + 4])
        both = dot_exact(pad_rows(jnp.concatenate([late_a, through_a], axis=0), half + 8), early)
        state = both[:half] + late_b
        read = both[half : half + 1] + through_b
    else:
        state = own[:, :DV]
        read = mine[0:1, :DV]
    members = state.shape[0] // rows
    for i in range(members):
        scratch[i] = state[i * rows : (i + 1) * rows]
    place = place % members
    rh, rl = split(read)
    tail = pad_rows(jnp.concatenate([rh, rl], axis=0).astype(f32), 16)
    for k in range(heads):
        body = scratch[place ^ k]
        refs[k][...] = jnp.concatenate([body, tail], axis=0).astype(bf16)


def final_kernel(heads, rows, small_ref, *refs):
    lead = lax.axis_index("sp") % heads
    state_ref, read_ref, scratch = refs[heads:]
    for k in range(heads):
        part = refs[k][...]
        state_ref[lead ^ k] = part[:rows]
        wide = part[rows : rows + 2].astype(f32)
        scratch[lead ^ k] = jnp.broadcast_to(wide[0:1] + wide[1:2], (SUB, DV))
    raw = jnp.concatenate([scratch[h][0:1] for h in range(heads)], axis=0)
    norm = lax.rsqrt(jnp.mean(raw * raw, axis=-1, keepdims=True) + norm_eps)
    read_ref[...] = raw * norm * small_ref[1:2, :]


def shape(dims, dtype=f32):
    return jax.ShapeDtypeStruct(dims, dtype)


vmem = pl.BlockSpec(memory_space=pltpu.VMEM)


def call(body, arrays, outs, scratch=(), mib=8, flops=0):
    return pl.pallas_call(
        body,
        out_shape=outs,
        in_specs=[vmem] * len(arrays),
        out_specs=jax.tree.map(lambda _: vmem, outs),
        scratch_shapes=list(scratch),
        compiler_params=pltpu.CompilerParams(vmem_limit_bytes=mib * 1024 * 1024),
        cost_estimate=pl.CostEstimate(flops=flops, bytes_accessed=0, transcendentals=0)
        if flops
        else None,
    )(*arrays)


def per_device(
    tokens,
    w_key,
    w_value,
    w_beta,
    w_decay,
    beta_bias,
    decay_rate,
    forgetting_increment,
    new_query,
    read_gain,
):
    heads = w_key.shape[1] // DK
    length, width = tokens.shape
    count, place = lax.axis_size("sp"), lax.axis_index("sp")
    ranks, rank = lax.axis_size("tp"), lax.axis_index("tp")
    groups = count // heads
    rows = DK // count
    chunk = min(CHUNK, length)
    chunks = length // chunk

    owns = [tokens[:chunk]]
    later = lax.optimization_barrier(tokens)
    owns += [later[c * chunk : (c + 1) * chunk] for c in range(1, chunks)]
    gathered = []
    for c in range(chunks):
        found = [(0, owns[c])]
        for hop in range(1, ranks // 2):
            found.append((2 * hop, swap(owns[c], "tp", 2 * hop)))
        found.append((1, swap(owns[c], "tp", 1)))
        found += [(m ^ 1, swap(x, "tp", 1)) for m, x in found[1:-1]]
        gathered.append(found)

    def head_rows(x):
        part = lax.dynamic_slice_in_dim(x.T, rank * heads, heads, 0)
        return jnp.pad(part, ((0, SUB - heads), (0, 0)))

    gate_weights = jnp.concatenate([head_rows(w_beta), head_rows(w_decay)], axis=0)
    named = jnp.concatenate([beta_bias, decay_rate])
    small = jnp.stack([jnp.pad(named, (0, DK - named.shape[0])), read_gain.astype(f32)])

    seat = lax.broadcasted_iota(jnp.int32, (heads, DK), 1) // rows
    query = jnp.where(seat == place, jnp.tile(new_query, (1, count)), jnp.zeros((), bf16))
    mask = heads
    while mask < count:
        query = query + swap(query, "sp", mask)
        mask *= 2

    w_key, w_value = pl.pallas_call(
        load_kernel,
        out_shape=[shape(w_key.shape, bf16), shape(w_value.shape, bf16)],
        in_specs=[pl.BlockSpec(memory_space=pltpu.HBM)] * 2,
        out_specs=[vmem] * 2,
        scratch_shapes=[pltpu.SemaphoreType.DMA((2,))],
        compiler_params=pltpu.CompilerParams(vmem_limit_bytes=20 * 1024 * 1024),
    )(*[pltpu.with_memory_space_constraint(w, pltpu.HBM) for w in (w_key, w_value)])

    state = None
    flops = 2 * chunk * width * ranks * (2 * heads * DK + DK) + heads * 24 * 2 * chunk * chunk * DK
    for c in range(chunks):
        found = gathered[c]
        last = c == chunks - 1
        arrays = [x for _, x in found] + [w_key, w_value, gate_weights, small, forgetting_increment]
        if c > 0:
            arrays.append(state)
        outs = [shape((heads, DK, DV + DK))]
        if last or c == 0:
            arrays.append(query)
        if last:
            outs = [shape((DK + 2 * SUB, DV + DK), bf16)] * heads + outs
        elif c == 0:
            outs = [shape((SUB, DK))] + outs
        result = call(
            functools.partial(chunk_kernel, heads, c, last, tuple(m for m, _ in found)),
            arrays,
            outs,
            mib=28,
            flops=flops,
        )
        state = result[-1]
        if c == 0 and not last:
            query = result[0]
    maps = result[:heads]

    got = {}
    for k in reversed(range(1, heads)):
        got[k] = swap(maps[k], "sp", k)
    done = [shape((DK, DV + DK)), shape((SUB, DV + DK))]
    if groups > 1:
        done.append(shape((DK + 16, DV), bf16))
    open_ended = [shape((DK, DV + DK)), shape((SUB, DK))]
    result = call(
        functools.partial(compose_kernel, heads, groups <= 2),
        [maps[0]] + [got[k] for k in range(1, heads)],
        done if groups <= 2 else open_ended,
        [pltpu.VMEM((heads, DK, DV + DK), f32)],
    )
    mask = heads
    while 2 * mask < count:
        final = 4 * mask == count
        partner = swap(result[0].astype(bf16), "sp", mask)
        result = call(
            functools.partial(merge_kernel, mask, final),
            [result[0], partner, result[1]],
            done if final else open_ended,
        )
        mask *= 2
    arrays = list(result[:2])
    if groups > 1:
        arrays.append(swap(result[2], "sp", count // 2))
    members = count // 2 if groups > 1 else count
    parts = call(
        functools.partial(rows_kernel, heads, groups, rows),
        arrays,
        [shape((rows + 16, DV), bf16)] * heads,
        [pltpu.VMEM((members, rows, DV), f32)],
    )
    moved = {}
    for k in reversed(range(1, heads)):
        moved[k] = swap(parts[k], "sp", k)
    own_rows, first_read = call(
        functools.partial(final_kernel, heads, rows),
        [small, parts[0]] + [moved[k] for k in range(1, heads)],
        [shape((heads, rows, DV), bf16), shape((heads, DV))],
        [pltpu.VMEM((heads, SUB, DV), f32)],
    )
    return (own_rows, first_read)


def solution(mesh):
    return jax.shard_map(
        per_device,
        mesh=mesh,
        in_specs=(
            P("sp", "tp"),
            P(None, "tp"),
            P(None, "tp"),
            P(),
            P(),
            P(),
            P(),
            P("tp", "sp"),
            P("tp", "sp"),
            P(),
        ),
        out_specs=(P("tp", "sp", None), P("tp", None)),
        check_vma=False,
    )
```

```python
import functools

import jax
import jax.numpy as jnp
from jax import lax
from jax.experimental import pallas as pl
from jax.experimental.pallas import tpu as pltpu
from jax.sharding import PartitionSpec as P


DK = 128
DV = 128
CHUNK = 128
SUB = 8

norm_eps = 1e-06
bf16 = jnp.bfloat16
f32 = jnp.float32


def flip(axis, mask):
    return [(i, i ^ mask) for i in range(lax.axis_size(axis))]


def swap(x, axis, mask):
    return lax.ppermute(x, axis, flip(axis, mask))


def dot(left, right):
    return jnp.dot(left.astype(bf16), right.astype(bf16), preferred_element_type=f32)


def split(x):
    high = x.astype(bf16)
    return high, (x - high.astype(f32)).astype(bf16)


def dot3(left, right):
    lh, ll = split(left)
    rh, rl = split(right)
    return dot(lh, rh) + (dot(lh, rl) + dot(ll, rh))


def dot_ones(left, ones):
    high, rest = split(left)
    mid = rest
    low = (left - high.astype(f32) - mid.astype(f32)).astype(bf16)
    n = left.shape[0]
    parts = jnp.concatenate([high.astype(f32), mid.astype(f32), low.astype(f32)], axis=0)
    out = dot(parts, ones)
    return out[:n] + out[n : 2 * n] + out[2 * n :]


def dot_nt(left, right):
    return lax.dot_general(
        left.astype(bf16), right.astype(bf16), (((1,), (1,)), ((), ())), preferred_element_type=f32
    )


def dot_tn(left, right):
    return lax.dot_general(
        left.astype(bf16), right.astype(bf16), (((0,), (0,)), ((), ())), preferred_element_type=f32
    )


def unit_inverses(lowers, size):
    row = lax.broadcasted_iota(jnp.int32, (size, size), 0)
    col = lax.broadcasted_iota(jnp.int32, (size, size), 1)
    identity = jnp.where(row == col, 1.0, 0.0)

    def same(width):
        return (row // width) == (col // width)

    width = min(16, size)
    inner = [jnp.where(same(width), low, 0.0) for low in lowers]
    results = [identity - low for low in inner]
    powers = inner
    covered = 2
    while covered < width:
        powers = [dot(p, p) for p in powers]
        results = [r + dot(r, p) for r, p in zip(results, powers)]
        covered *= 2
    while width < size:
        off = jnp.logical_and(same(2 * width), jnp.logical_not(same(width)))
        right = [dot(jnp.where(off, low, 0.0), r) for low, r in zip(lowers, results)]
        results = [r - dot(r, x) for r, x in zip(results, right)]
        width *= 2
    return results


def prepare_kernel(heads, *refs):
    wk_hbm, wv_hbm = refs[:2]
    wk_ref, wv_ref, wg_ref, small_ref, forget_ref, query_ref = refs[8:14]
    few, sems = refs[14:20], refs[20]
    wb_ref, wd_ref, bias_ref, rate_ref, forget_in, query_in = few
    lead = lax.axis_index("sp") % heads
    first = lax.axis_index("tp") * heads
    early = [
        pltpu.make_async_copy(hbm, ref, sems.at[2 * heads + i])
        for i, (hbm, ref) in enumerate(zip(refs[2:8], few))
    ]
    copies = []
    for k in range(heads):
        source = pl.ds(pl.multiple_of((lead ^ k) * DK, DK), DK)
        target = pl.ds(k * DK, DK)
        for i, (hbm, ref) in enumerate(((wk_hbm, wk_ref), (wv_hbm, wv_ref))):
            copies.append(
                pltpu.make_async_copy(hbm.at[:, source], ref.at[:, target], sems.at[2 * k + i])
            )
    for copy in early + copies:
        copy.start()
    for copy in early:
        copy.wait()
    many = bias_ref.shape[1]
    row = lax.broadcasted_iota(jnp.int32, (2 * SUB, 2 * many), 0)
    col = lax.broadcasted_iota(jnp.int32, (2 * SUB, 2 * many), 1)
    k = row & (SUB - 1)
    wanted = first + (lead ^ k) + jnp.where(row >= SUB, many, 0)
    pick = jnp.where(jnp.logical_and(col == wanted, k < heads), 1.0, 0.0)
    both = jnp.concatenate([wb_ref[...], wd_ref[...]], axis=0)
    wg_ref[...] = dot(pick, both).astype(bf16)
    row = lax.broadcasted_iota(jnp.int32, (SUB, many), 0)
    col = lax.broadcasted_iota(jnp.int32, (SUB, many), 1)
    mine = col == first + (lead ^ row)
    bias = jnp.sum(jnp.where(mine, bias_ref[...], 0.0), axis=1, keepdims=True)
    rate = jnp.sum(jnp.where(mine, rate_ref[...], 0.0), axis=1, keepdims=True)
    lane = lax.broadcasted_iota(jnp.int32, (SUB, DK), 1)
    small_ref[...] = jnp.where(lane == 0, bias, jnp.where(lane == 1, rate, 0.0))
    seats = query_in.shape[1]
    place = lax.axis_index("sp") * seats
    row = lax.broadcasted_iota(jnp.int32, (seats, DK), 0)
    col = lax.broadcasted_iota(jnp.int32, (seats, DK), 1)
    query = dot(query_in[...], jnp.where(col == row + place, 1.0, 0.0))
    forget = forget_in[...]
    size = forget.shape[1]
    wide = lax.broadcasted_iota(jnp.int32, (SUB, size), 0)
    slim = lax.broadcasted_iota(jnp.int32, (SUB, DK), 0)
    forget_out = jnp.zeros((SUB, size), f32)
    query_out = jnp.zeros((SUB, DK), f32)
    for h in range(heads):
        forget_out = jnp.where((lead ^ wide) == h, forget[h : h + 1], forget_out)
        query_out = jnp.where((lead ^ slim) == h, query[h : h + 1], query_out)
    forget_ref[...] = forget_out
    query_ref[...] = query_out
    for copy in copies:
        copy.wait()


def chunk_kernel(heads, index, last, masks, *refs):
    pieces = len(masks)
    piece_refs = refs[:pieces]
    wk_ref, wv_ref, wg_ref, small_ref, forget_ref = refs[pieces : pieces + 5]
    rest = refs[pieces + 5 :]
    if index > 0:
        state_ref, rest = rest[0], rest[1:]
    if last:
        query_ref, rest = rest[0], rest[1:]
    size, width = piece_refs[0].shape
    rank = lax.axis_index("tp")
    starts = [pl.multiple_of((rank ^ m) * width, width) for m in masks]

    gates = None
    for start, piece_ref in zip(starts, piece_refs):
        g = dot_nt(wg_ref[:, pl.ds(start, width)], piece_ref[...])
        gates = g if gates is None else gates + g
    bias, rate = small_ref[:, 0:1], small_ref[:, 1:2]
    forget = forget_ref[:, index * size : (index + 1) * size]
    beta_row = jax.nn.sigmoid(gates[0:SUB] + bias)
    log_row = forget - rate * jax.nn.softplus(gates[SUB : 2 * SUB])
    row = lax.broadcasted_iota(jnp.int32, (size, size), 0)
    col = lax.broadcasted_iota(jnp.int32, (size, size), 1)
    cum_row = dot_ones(log_row, jnp.where(row <= col, 1.0, 0.0))
    total = cum_row[:, size - 1 : size]
    stacked = jnp.concatenate(
        [
            beta_row,
            cum_row,
            beta_row * jnp.exp(cum_row),
            jnp.exp(total - cum_row),
            jnp.zeros((DK - 4 * SUB, size), f32),
        ],
        axis=0,
    )
    columns = stacked.T
    keep = jnp.exp(total)

    key_acc = value_acc = None
    for start, piece_ref in zip(starts, piece_refs):
        rows = pl.ds(start, width)
        x = piece_ref[...]
        k = jnp.dot(x, wk_ref[rows, :], preferred_element_type=f32)
        key_acc = k if key_acc is None else key_acc + k
    for start, piece_ref in zip(starts, piece_refs):
        rows = pl.ds(start, width)
        x = piece_ref[...]
        v = jnp.dot(x, wv_ref[rows, :], preferred_element_type=f32)
        value_acc = v if value_acc is None else value_acc + v
    key_raw = key_acc.astype(bf16).astype(f32)
    value_raw = value_acc.astype(bf16).astype(f32)

    strict = row > col
    keys, lowers, base = [], [], []
    for h in range(heads):
        kw = key_raw[:, h * DK : (h + 1) * DK]
        ku = kw * lax.rsqrt(jnp.sum(kw * kw, axis=-1, keepdims=True) + norm_eps)
        beta = columns[:, h : h + 1]
        cum = columns[:, SUB + h : SUB + h + 1]
        spread = jnp.where(strict, cum - cum_row[h : h + 1, :], 0.0)
        table = jnp.where(strict, jnp.exp(spread), 0.0)
        keys.append(ku)
        lowers.append(dot_nt(ku, ku) * table * beta)
    if index > 0:
        states = [state_ref[h] for h in range(heads)]
    else:
        kr = lax.broadcasted_iota(jnp.int32, (DK, DV + DK), 0)
        kc = lax.broadcasted_iota(jnp.int32, (DK, DV + DK), 1)
        states = [jnp.where(kc == kr + DV, 1.0, 0.0)] * heads
    for h in range(heads):
        beta = columns[:, h : h + 1]
        erase = keys[h] * columns[:, 2 * SUB + h : 2 * SUB + h + 1]
        value = value_raw[:, h * DV : (h + 1) * DV] * beta
        padded = jnp.concatenate([value, jnp.zeros((size, DK), f32)], axis=1)
        base.append(padded - dot(erase, states[h]))
    inverses = unit_inverses(lowers, size)
    fresh = [dot(inv, b) for inv, b in zip(inverses, base)]
    for h in range(heads):
        remain = keys[h] * columns[:, 3 * SUB + h : 3 * SUB + h + 1]
        new = keep[h : h + 1, :] * states[h] + dot_tn(remain, fresh[h])
        if last:
            rest[h][0:DK, :] = new.astype(bf16)
            asked = jnp.broadcast_to(query_ref[h : h + 1, :], (2 * SUB, DK))
            asked = jnp.concatenate([asked, jnp.zeros((2 * SUB, DV), f32)], axis=1)
            rest[h][DK:, :] = asked.astype(bf16)
        else:
            rest[-1][h] = new


def compose(pairs, product):
    while len(pairs) > 1:
        merged = []
        for early, late in zip(pairs[0::2], pairs[1::2]):
            new = product(late[:, DV:], early)
            merged.append(jnp.concatenate([new[:, :DV] + late[:, :DV], new[:, DV:]], axis=1))
        pairs, product = merged, dot3
    return pairs[0]


def pad_rows(x, rows):
    return jnp.concatenate([x, jnp.zeros((rows - x.shape[0], x.shape[1]), x.dtype)], axis=0)


def late_side(mask):
    return lax.rem(lax.div(lax.axis_index("sp"), jnp.int32(mask)), jnp.int32(2)) == 1


def finish(total, query, out):
    out[0][...] = total
    out[1][...] = query
    if len(out) == 2:
        return
    half = DK // 2
    through = dot3(query, total)
    a, b = total[:, DV:], total[:, :DV]
    high = late_side(lax.axis_size("sp") // 2)
    body = jnp.where(high, jnp.concatenate([a[:half], b[:half]], axis=0), b)
    ah, al = split(through[0:1, DV:])
    bh, bl = split(through[0:1, :DV])
    tail = [query[0:1]] + [x.astype(f32) for x in (ah, al, bh, bl)]
    tail = pad_rows(jnp.concatenate(tail, axis=0), 2 * SUB)
    out[2][0:DK, :] = body.astype(bf16)
    out[2][DK:, :] = tail.astype(bf16)


def passed_on(total, query):
    asked = jnp.concatenate([query, query], axis=0)
    asked = jnp.concatenate([asked, jnp.zeros((2 * SUB, DV), f32)], axis=1)
    return jnp.concatenate([total, asked], axis=0).astype(bf16)


def compose_kernel(heads, final, *refs):
    own_ref, got = refs[0], refs[1:heads]
    out, scratch = refs[heads:-1], refs[-1]
    lead = lax.axis_index("sp") % heads
    scratch[lead] = own_ref[:DK, :].astype(f32)
    query = own_ref[DK:, :DK].astype(f32)
    for k in range(1, heads):
        scratch[lead ^ k] = got[k - 1][:DK, :].astype(f32)
        query = query + got[k - 1][DK:, :DK].astype(f32)
    total = compose([scratch[i] for i in range(heads)], dot)
    query = query[:SUB]
    if final:
        finish(total, query, out)
    else:
        out[0][...], out[1][...] = total, query
        out[2][...] = passed_on(total, query)


def merge_kernel(mask, final, own_ref, query_ref, got_ref, *out):
    high = late_side(mask)
    own, got = own_ref[...], got_ref[:DK, :].astype(f32)
    query = query_ref[...] + got_ref[DK:, :DK].astype(f32)[:SUB]
    early, late = jnp.where(high, got, own), jnp.where(high, own, got)
    total = compose([early, late], dot3)
    if final:
        finish(total, query, out)
    else:
        out[0][...], out[1][...] = total, query
        out[2][...] = passed_on(total, query)


def rows_kernel(heads, groups, rows, own_ref, query_ref, *refs):
    if groups > 1:
        got_ref, refs = refs[0], refs[1:]
    scratch = refs[-1]
    own, query = own_ref[...], query_ref[...]
    half = DK // 2
    place = lax.axis_index("sp")
    if groups > 1:
        high = late_side(lax.axis_size("sp") // 2)
        got = got_ref[...].astype(f32)
        a, b = own[:, DV:], own[:, :DV]
        early = jnp.where(high, got[:DK], b)
        late_a = jnp.where(high, a[half:], got[:half])
        late_b = jnp.where(high, b[half:], got[half:DK])
        tail = got[DK:]
        cross = dot3(jnp.broadcast_to(tail[0:1], (SUB, DK)), own)[0:1]
        through_a = jnp.where(high, cross[:, DV:], tail[1:2] + tail[2:3])
        through_b = jnp.where(high, cross[:, :DV], tail[3:4] + tail[4:5])
        both = dot3(pad_rows(jnp.concatenate([late_a, through_a], axis=0), half + SUB), early)
        state = both[:half] + late_b
        asked = jnp.where(high, query[:, half:], query[:, :half])
        read = dot3(asked, state)[0:1] + (both[half : half + 1] + through_b)
    else:
        state = own[:, :DV]
        read = dot3(query, state)[0:1]
    members = state.shape[0] // rows
    for i in range(members):
        scratch[i] = state[i * rows : (i + 1) * rows]
    place = place % members
    rh, rl = split(read)
    tail = pad_rows(jnp.concatenate([rh.astype(f32), rl.astype(f32)], axis=0), 16)
    for k in range(heads):
        body = scratch[place ^ k]
        refs[k][...] = jnp.concatenate([body, tail], axis=0).astype(bf16)


def final_kernel(heads, rows, gain_ref, *refs):
    lead = lax.axis_index("sp") % heads
    state_ref, read_ref, scratch = refs[heads:]
    for k in range(heads):
        part = refs[k][...]
        state_ref[lead ^ k] = part[:rows]
        wide = part[rows : rows + 2].astype(f32)
        scratch[lead ^ k] = jnp.broadcast_to(wide[0:1] + wide[1:2], (SUB, DV))
    raw = jnp.concatenate([scratch[h][0:1] for h in range(heads)], axis=0)
    norm = lax.rsqrt(jnp.mean(raw * raw, axis=-1, keepdims=True) + norm_eps)
    read_ref[...] = raw * norm * gain_ref[...].astype(f32)


def shape(dims, dtype=f32):
    return jax.ShapeDtypeStruct(dims, dtype)


vmem = pl.BlockSpec(memory_space=pltpu.VMEM)


def call(body, arrays, outs, scratch=(), mib=8, flops=0):
    return pl.pallas_call(
        body,
        out_shape=outs,
        in_specs=[vmem] * len(arrays),
        out_specs=jax.tree.map(lambda _: vmem, outs),
        scratch_shapes=list(scratch),
        compiler_params=pltpu.CompilerParams(vmem_limit_bytes=mib * 1024 * 1024),
        cost_estimate=pl.CostEstimate(flops=flops, bytes_accessed=0, transcendentals=0)
        if flops
        else None,
    )(*arrays)


def per_device(
    tokens,
    w_key,
    w_value,
    w_beta,
    w_decay,
    beta_bias,
    decay_rate,
    forgetting_increment,
    new_query,
    read_gain,
):
    heads = w_key.shape[1] // DK
    length, width = tokens.shape
    count = lax.axis_size("sp")
    ranks = lax.axis_size("tp")
    groups = count // heads
    rows = DK // count
    chunk = min(CHUNK, length)
    chunks = length // chunk

    owns = [tokens[:chunk]]
    later = lax.optimization_barrier(tokens)
    owns += [later[c * chunk : (c + 1) * chunk] for c in range(1, chunks)]
    gathered = []
    for c in range(chunks):
        found = [(0, owns[c])]
        for hop in range(1, ranks // 2):
            found.append((2 * hop, swap(owns[c], "tp", 2 * hop)))
        found.append((1, swap(owns[c], "tp", 1)))
        found += [(m ^ 1, swap(x, "tp", 1)) for m, x in found[1:-1]]
        gathered.append(found)

    plain = [
        pltpu.with_memory_space_constraint(x, pltpu.HBM)
        for x in (
            w_key,
            w_value,
            w_beta.T,
            w_decay.T,
            beta_bias[None],
            decay_rate[None],
            forgetting_increment,
            new_query,
        )
    ]
    w_key, w_value, gate_weights, small, forget, query = pl.pallas_call(
        functools.partial(prepare_kernel, heads),
        out_shape=[
            shape(w_key.shape, bf16),
            shape(w_value.shape, bf16),
            shape((2 * SUB, w_beta.shape[0]), bf16),
            shape((SUB, DK)),
            shape((SUB, length)),
            shape((SUB, DK)),
        ],
        in_specs=[pl.BlockSpec(memory_space=pltpu.HBM)] * 8,
        out_specs=[vmem] * 6,
        scratch_shapes=[pltpu.VMEM(x.shape, x.dtype) for x in plain[2:]]
        + [pltpu.SemaphoreType.DMA((2 * heads + 6,))],
        compiler_params=pltpu.CompilerParams(vmem_limit_bytes=24 * 1024 * 1024),
    )(*plain)

    state = None
    flops = 2 * chunk * width * ranks * (2 * heads * DK + DK) + heads * 24 * 2 * chunk * chunk * DK
    for c in range(chunks):
        found = gathered[c]
        last = c == chunks - 1
        arrays = [x for _, x in found] + [w_key, w_value, gate_weights, small, forget]
        if c > 0:
            arrays.append(state)
        outs = [shape((heads, DK, DV + DK))]
        if last:
            arrays.append(query)
            outs = [shape((DK + 2 * SUB, DV + DK), bf16)] * heads
        result = call(
            functools.partial(chunk_kernel, heads, c, last, tuple(m for m, _ in found)),
            arrays,
            outs,
            mib=28,
            flops=flops,
        )
        state = result[-1]
    maps = result

    got = {}
    for k in reversed(range(1, heads)):
        got[k] = swap(maps[k], "sp", k)
    done = [shape((DK, DV + DK)), shape((SUB, DK))]
    open_ended = done + [shape((DK + 2 * SUB, DV + DK), bf16)]
    if groups > 1:
        done.append(shape((DK + 2 * SUB, DV), bf16))
    result = call(
        functools.partial(compose_kernel, heads, groups <= 2),
        [maps[0]] + [got[k] for k in range(1, heads)],
        done if groups <= 2 else open_ended,
        [pltpu.VMEM((heads, DK, DV + DK), f32)],
    )
    mask = heads
    while 2 * mask < count:
        final = 4 * mask == count
        result = call(
            functools.partial(merge_kernel, mask, final),
            [result[0], result[1], swap(result[2], "sp", mask)],
            done if final else open_ended,
        )
        mask *= 2
    arrays = list(result[:2])
    if groups > 1:
        arrays.append(swap(result[2], "sp", count // 2))
    members = count // 2 if groups > 1 else count
    parts = call(
        functools.partial(rows_kernel, heads, groups, rows),
        arrays,
        [shape((rows + 16, DV), bf16)] * heads,
        [pltpu.VMEM((members, rows, DV), f32)],
    )
    moved = {}
    for k in reversed(range(1, heads)):
        moved[k] = swap(parts[k], "sp", k)
    own_rows, first_read = call(
        functools.partial(final_kernel, heads, rows),
        [read_gain[None], parts[0]] + [moved[k] for k in range(1, heads)],
        [shape((heads, rows, DV), bf16), shape((heads, DV))],
        [pltpu.VMEM((heads, SUB, DV), f32)],
    )
    return (own_rows, first_read)


def solution(mesh):
    return jax.shard_map(
        per_device,
        mesh=mesh,
        in_specs=(
            P("sp", "tp"),
            P(None, "tp"),
            P(None, "tp"),
            P(),
            P(),
            P(),
            P(),
            P("tp", "sp"),
            P("tp", "sp"),
            P(),
        ),
        out_specs=(P("tp", "sp", None), P("tp", None)),
        check_vma=False,
    )
```

```python
import functools

import jax
import jax.numpy as jnp
from jax import lax
from jax.experimental import pallas as pl
from jax.experimental.pallas import tpu as pltpu
from jax.sharding import PartitionSpec as P


DK = 128
DV = 128
CHUNK = 128
SUB = 8

norm_eps = 1e-06
bf16 = jnp.bfloat16
f32 = jnp.float32


def flip(axis, mask):
    return [(i, i ^ mask) for i in range(lax.axis_size(axis))]


def swap(x, axis, mask):
    return lax.ppermute(x, axis, flip(axis, mask))


def dot(left, right):
    return jnp.dot(left.astype(bf16), right.astype(bf16), preferred_element_type=f32)


def split(x):
    high = x.astype(bf16)
    return high, (x - high.astype(f32)).astype(bf16)


def dot3(left, right):
    lh, ll = split(left)
    rh, rl = split(right)
    return dot(lh, rh) + (dot(lh, rl) + dot(ll, rh))


def dot_ones(left, ones):
    high, rest = split(left)
    mid = rest
    low = (left - high.astype(f32) - mid.astype(f32)).astype(bf16)
    n = left.shape[0]
    parts = jnp.concatenate([high.astype(f32), mid.astype(f32), low.astype(f32)], axis=0)
    out = dot(parts, ones)
    return out[:n] + out[n : 2 * n] + out[2 * n :]


def dot_nt(left, right):
    return lax.dot_general(
        left.astype(bf16), right.astype(bf16), (((1,), (1,)), ((), ())), preferred_element_type=f32
    )


def dot_tn(left, right):
    return lax.dot_general(
        left.astype(bf16), right.astype(bf16), (((0,), (0,)), ((), ())), preferred_element_type=f32
    )


def unit_inverses(lowers, size):
    row = lax.broadcasted_iota(jnp.int32, (size, size), 0)
    col = lax.broadcasted_iota(jnp.int32, (size, size), 1)
    width = min(16, size)
    near = (row // width) == (col // width)
    inner = [jnp.where(near, low, 0.0) for low in lowers]
    results = [jnp.where(row == col, 1.0, 0.0) - low for low in inner]
    powers = inner
    covered = 2
    while covered < width:
        powers = [dot(p, p) for p in powers]
        results = [r + dot(r, p) for r, p in zip(results, powers)]
        covered *= 2
    if width == size:
        return results
    powers = [dot(r, jnp.where(near, 0.0, low)) for r, low in zip(results, lowers)]
    results = [r - dot(p, r) for r, p in zip(results, powers)]
    covered = 2
    while covered * width < size:
        powers = [dot(p, p) for p in powers]
        results = [r + dot(p, r) for r, p in zip(results, powers)]
        covered *= 2
    return results


def project(masks, piece_refs, wk_ref, wv_ref, wg_ref, sums):
    rank = lax.axis_index("tp")
    gates, keys, values = sums
    placed = []
    for m, ref in zip(masks, piece_refs):
        width = ref.shape[1]
        placed.append((pl.ds(pl.multiple_of((rank ^ m) * width, width), width), ref))
    for rows, ref in placed:
        g = dot_nt(wg_ref[:, rows], ref[...])
        gates = g if gates is None else gates + g
    for rows, ref in placed:
        k = jnp.dot(ref[...], wk_ref[rows, :], preferred_element_type=f32)
        keys = k if keys is None else keys + k
    for rows, ref in placed:
        v = jnp.dot(ref[...], wv_ref[rows, :], preferred_element_type=f32)
        values = v if values is None else values + v
    return gates, keys, values


def part_kernel(masks, prior, *refs):
    pieces = len(masks)
    weights, rest = refs[pieces : pieces + 3], refs[pieces + 3 :]
    sums = (None, None, None)
    if prior:
        sums, rest = tuple(ref[...] for ref in rest[:3]), rest[3:]
    for ref, x in zip(rest, project(masks, refs[:pieces], *weights, sums)):
        ref[...] = x


def prepare_kernel(heads, *refs):
    wk_hbm, wv_hbm = refs[:2]
    wk_ref, wv_ref, wg_ref, small_ref, forget_ref, query_ref = refs[8:14]
    few, sems = refs[14:20], refs[20]
    wb_ref, wd_ref, bias_ref, rate_ref, forget_in, query_in = few
    lead = lax.axis_index("sp") % heads
    first = lax.axis_index("tp") * heads
    early = [
        pltpu.make_async_copy(hbm, ref, sems.at[2 * heads + i])
        for i, (hbm, ref) in enumerate(zip(refs[2:8], few))
    ]
    copies = []
    for k in range(heads):
        source = pl.ds(pl.multiple_of((lead ^ k) * DK, DK), DK)
        target = pl.ds(k * DK, DK)
        for i, (hbm, ref) in enumerate(((wk_hbm, wk_ref), (wv_hbm, wv_ref))):
            copies.append(
                pltpu.make_async_copy(hbm.at[:, source], ref.at[:, target], sems.at[2 * k + i])
            )
    for copy in early + copies:
        copy.start()
    for copy in early:
        copy.wait()
    many = bias_ref.shape[1]
    row = lax.broadcasted_iota(jnp.int32, (2 * SUB, 2 * many), 0)
    col = lax.broadcasted_iota(jnp.int32, (2 * SUB, 2 * many), 1)
    k = row & (SUB - 1)
    wanted = first + (lead ^ k) + jnp.where(row >= SUB, many, 0)
    pick = jnp.where(jnp.logical_and(col == wanted, k < heads), 1.0, 0.0)
    both = jnp.concatenate([wb_ref[...], wd_ref[...]], axis=0)
    wg_ref[...] = dot(pick, both).astype(bf16)
    row = lax.broadcasted_iota(jnp.int32, (SUB, many), 0)
    col = lax.broadcasted_iota(jnp.int32, (SUB, many), 1)
    mine = col == first + (lead ^ row)
    bias = jnp.sum(jnp.where(mine, bias_ref[...], 0.0), axis=1, keepdims=True)
    rate = jnp.sum(jnp.where(mine, rate_ref[...], 0.0), axis=1, keepdims=True)
    lane = lax.broadcasted_iota(jnp.int32, (SUB, DK), 1)
    small_ref[...] = jnp.where(lane == 0, bias, jnp.where(lane == 1, rate, 0.0))
    seats = query_in.shape[1]
    place = lax.axis_index("sp") * seats
    row = lax.broadcasted_iota(jnp.int32, (seats, DK), 0)
    col = lax.broadcasted_iota(jnp.int32, (seats, DK), 1)
    query = dot(query_in[...], jnp.where(col == row + place, 1.0, 0.0))
    forget = forget_in[...]
    size = forget.shape[1]
    wide = lax.broadcasted_iota(jnp.int32, (SUB, size), 0)
    slim = lax.broadcasted_iota(jnp.int32, (SUB, DK), 0)
    forget_out = jnp.zeros((SUB, size), f32)
    query_out = jnp.zeros((SUB, DK), f32)
    for h in range(heads):
        forget_out = jnp.where((lead ^ wide) == h, forget[h : h + 1], forget_out)
        query_out = jnp.where((lead ^ slim) == h, query[h : h + 1], query_out)
    forget_ref[...] = forget_out
    query_ref[...] = query_out
    for copy in copies:
        copy.wait()


def chunk_kernel(heads, index, last, masks, prior, *refs):
    pieces = len(masks)
    piece_refs = refs[:pieces]
    wk_ref, wv_ref, wg_ref, small_ref, forget_ref = refs[pieces : pieces + 5]
    rest = refs[pieces + 5 :]
    sums = (None, None, None)
    if prior:
        sums, rest = tuple(ref[...] for ref in rest[:3]), rest[3:]
    if index > 0:
        state_ref, rest = rest[0], rest[1:]
    if last:
        query_ref, rest = rest[0], rest[1:]
    gates, key_acc, value_acc = project(masks, piece_refs, wk_ref, wv_ref, wg_ref, sums)
    size = key_acc.shape[0]
    bias, rate = small_ref[:, 0:1], small_ref[:, 1:2]
    forget = forget_ref[:, index * size : (index + 1) * size]
    beta_row = jax.nn.sigmoid(gates[0:SUB] + bias)
    log_row = forget - rate * jax.nn.softplus(gates[SUB : 2 * SUB])
    row = lax.broadcasted_iota(jnp.int32, (size, size), 0)
    col = lax.broadcasted_iota(jnp.int32, (size, size), 1)
    cum_row = dot_ones(log_row, jnp.where(row <= col, 1.0, 0.0))
    total = cum_row[:, size - 1 : size]
    stacked = jnp.concatenate(
        [
            beta_row,
            cum_row,
            beta_row * jnp.exp(cum_row),
            jnp.exp(total - cum_row),
            jnp.zeros((DK - 4 * SUB, size), f32),
        ],
        axis=0,
    )
    columns = stacked.T
    keep = jnp.exp(total)

    key_raw = key_acc.astype(bf16).astype(f32)
    value_raw = value_acc.astype(bf16).astype(f32)

    strict = row > col
    keys, lowers, base = [], [], []
    for h in range(heads):
        kw = key_raw[:, h * DK : (h + 1) * DK]
        ku = kw * lax.rsqrt(jnp.sum(kw * kw, axis=-1, keepdims=True) + norm_eps)
        beta = columns[:, h : h + 1]
        cum = columns[:, SUB + h : SUB + h + 1]
        spread = jnp.where(strict, cum - cum_row[h : h + 1, :], 0.0)
        table = jnp.where(strict, jnp.exp(spread), 0.0)
        keys.append(ku)
        lowers.append(dot_nt(ku, ku) * table * beta)
    if index > 0:
        states = [state_ref[h] for h in range(heads)]
    else:
        kr = lax.broadcasted_iota(jnp.int32, (DK, DV + DK), 0)
        kc = lax.broadcasted_iota(jnp.int32, (DK, DV + DK), 1)
        states = [jnp.where(kc == kr + DV, 1.0, 0.0)] * heads
    for h in range(heads):
        beta = columns[:, h : h + 1]
        erase = keys[h] * columns[:, 2 * SUB + h : 2 * SUB + h + 1]
        value = value_raw[:, h * DV : (h + 1) * DV] * beta
        padded = jnp.concatenate([value, jnp.zeros((size, DK), f32)], axis=1)
        base.append(padded - dot(erase, states[h]))
    inverses = unit_inverses(lowers, size)
    fresh = [dot(inv, b) for inv, b in zip(inverses, base)]
    for h in range(heads):
        remain = keys[h] * columns[:, 3 * SUB + h : 3 * SUB + h + 1]
        new = keep[h : h + 1, :] * states[h] + dot_tn(remain, fresh[h])
        if last:
            rest[h][0:DK, :] = new.astype(bf16)
            asked = jnp.broadcast_to(query_ref[h : h + 1, :], (2 * SUB, DK))
            asked = jnp.concatenate([asked, jnp.zeros((2 * SUB, DV), f32)], axis=1)
            rest[h][DK:, :] = asked.astype(bf16)
        else:
            rest[-1][h] = new


def compose(pairs, product):
    while len(pairs) > 1:
        merged = []
        for early, late in zip(pairs[0::2], pairs[1::2]):
            new = product(late[:, DV:], early)
            merged.append(jnp.concatenate([new[:, :DV] + late[:, :DV], new[:, DV:]], axis=1))
        pairs, product = merged, dot3
    return pairs[0]


def pad_rows(x, rows):
    return jnp.concatenate([x, jnp.zeros((rows - x.shape[0], x.shape[1]), x.dtype)], axis=0)


def late_side(mask):
    return lax.rem(lax.div(lax.axis_index("sp"), jnp.int32(mask)), jnp.int32(2)) == 1


def finish(total, query, out):
    out[0][...] = total
    out[1][...] = query
    if len(out) == 2:
        return
    half = DK // 2
    through = dot3(query, total)
    a, b = total[:, DV:], total[:, :DV]
    high = late_side(lax.axis_size("sp") // 2)
    body = jnp.where(high, jnp.concatenate([a[:half], b[:half]], axis=0), b)
    ah, al = split(through[0:1, DV:])
    bh, bl = split(through[0:1, :DV])
    tail = [query[0:1]] + [x.astype(f32) for x in (ah, al, bh, bl)]
    tail = pad_rows(jnp.concatenate(tail, axis=0), 2 * SUB)
    out[2][0:DK, :] = body.astype(bf16)
    out[2][DK:, :] = tail.astype(bf16)


def passed_on(total, query):
    asked = jnp.concatenate([query, query], axis=0)
    asked = jnp.concatenate([asked, jnp.zeros((2 * SUB, DV), f32)], axis=1)
    return jnp.concatenate([total, asked], axis=0).astype(bf16)


def compose_kernel(heads, final, *refs):
    own_ref, got = refs[0], refs[1:heads]
    out, scratch = refs[heads:-1], refs[-1]
    lead = lax.axis_index("sp") % heads
    scratch[lead] = own_ref[:DK, :].astype(f32)
    query = own_ref[DK:, :DK].astype(f32)
    for k in range(1, heads):
        scratch[lead ^ k] = got[k - 1][:DK, :].astype(f32)
        query = query + got[k - 1][DK:, :DK].astype(f32)
    total = compose([scratch[i] for i in range(heads)], dot)
    query = query[:SUB]
    if final:
        finish(total, query, out)
    else:
        out[0][...], out[1][...] = total, query
        out[2][...] = passed_on(total, query)


def merge_kernel(mask, final, own_ref, query_ref, got_ref, *out):
    high = late_side(mask)
    own, got = own_ref[...], got_ref[:DK, :].astype(f32)
    query = query_ref[...] + got_ref[DK:, :DK].astype(f32)[:SUB]
    early, late = jnp.where(high, got, own), jnp.where(high, own, got)
    total = compose([early, late], dot3)
    if final:
        finish(total, query, out)
    else:
        out[0][...], out[1][...] = total, query
        out[2][...] = passed_on(total, query)


def rows_kernel(heads, groups, rows, own_ref, query_ref, *refs):
    if groups > 1:
        got_ref, refs = refs[0], refs[1:]
    scratch = refs[-1]
    own, query = own_ref[...], query_ref[...]
    half = DK // 2
    place = lax.axis_index("sp")
    if groups > 1:
        high = late_side(lax.axis_size("sp") // 2)
        got = got_ref[...].astype(f32)
        a, b = own[:, DV:], own[:, :DV]
        early = jnp.where(high, got[:DK], b)
        late_a = jnp.where(high, a[half:], got[:half])
        late_b = jnp.where(high, b[half:], got[half:DK])
        tail = got[DK:]
        cross = dot3(jnp.broadcast_to(tail[0:1], (SUB, DK)), own)[0:1]
        through_a = jnp.where(high, cross[:, DV:], tail[1:2] + tail[2:3])
        through_b = jnp.where(high, cross[:, :DV], tail[3:4] + tail[4:5])
        both = dot3(pad_rows(jnp.concatenate([late_a, through_a], axis=0), half + SUB), early)
        state = both[:half] + late_b
        asked = jnp.where(high, query[:, half:], query[:, :half])
        read = dot3(asked, state)[0:1] + (both[half : half + 1] + through_b)
    else:
        state = own[:, :DV]
        read = dot3(query, state)[0:1]
    members = state.shape[0] // rows
    for i in range(members):
        scratch[i] = state[i * rows : (i + 1) * rows]
    place = place % members
    rh, rl = split(read)
    tail = pad_rows(jnp.concatenate([rh.astype(f32), rl.astype(f32)], axis=0), 16)
    for k in range(heads):
        body = scratch[place ^ k]
        refs[k][...] = jnp.concatenate([body, tail], axis=0).astype(bf16)


def final_kernel(heads, rows, gain_ref, *refs):
    lead = lax.axis_index("sp") % heads
    state_ref, read_ref, scratch = refs[heads:]
    for k in range(heads):
        part = refs[k][...]
        state_ref[lead ^ k] = part[:rows]
        wide = part[rows : rows + 2].astype(f32)
        scratch[lead ^ k] = jnp.broadcast_to(wide[0:1] + wide[1:2], (SUB, DV))
    raw = jnp.concatenate([scratch[h][0:1] for h in range(heads)], axis=0)
    norm = lax.rsqrt(jnp.mean(raw * raw, axis=-1, keepdims=True) + norm_eps)
    read_ref[...] = raw * norm * gain_ref[...].astype(f32)


def shape(dims, dtype=f32):
    return jax.ShapeDtypeStruct(dims, dtype)


vmem = pl.BlockSpec(memory_space=pltpu.VMEM)


def call(body, arrays, outs, scratch=(), mib=8, flops=0):
    return pl.pallas_call(
        body,
        out_shape=outs,
        in_specs=[vmem] * len(arrays),
        out_specs=jax.tree.map(lambda _: vmem, outs),
        scratch_shapes=list(scratch),
        compiler_params=pltpu.CompilerParams(vmem_limit_bytes=mib * 1024 * 1024),
        cost_estimate=pl.CostEstimate(flops=flops, bytes_accessed=0, transcendentals=0)
        if flops
        else None,
    )(*arrays)


def per_device(
    tokens,
    w_key,
    w_value,
    w_beta,
    w_decay,
    beta_bias,
    decay_rate,
    forgetting_increment,
    new_query,
    read_gain,
):
    heads = w_key.shape[1] // DK
    length, width = tokens.shape
    count = lax.axis_size("sp")
    ranks = lax.axis_size("tp")
    groups = count // heads
    rows = DK // count
    chunk = min(CHUNK, length)
    chunks = length // chunk

    owns = [tokens[:chunk]]
    later = lax.optimization_barrier(tokens)
    owns += [later[c * chunk : (c + 1) * chunk] for c in range(1, chunks)]
    gathered = []
    for c in range(chunks):
        found = [(0, owns[c])]
        for hop in range(1, ranks // 2):
            found.append((2 * hop, swap(owns[c], "tp", 2 * hop)))
        found.append((1, swap(owns[c], "tp", 1)))
        found += [(m ^ 1, swap(x, "tp", 1)) for m, x in found[1:-1]]
        gathered.append(found)

    plain = [
        pltpu.with_memory_space_constraint(x, pltpu.HBM)
        for x in (
            w_key,
            w_value,
            w_beta.T,
            w_decay.T,
            beta_bias[None],
            decay_rate[None],
            forgetting_increment,
            new_query,
        )
    ]
    w_key, w_value, gate_weights, small, forget, query = pl.pallas_call(
        functools.partial(prepare_kernel, heads),
        out_shape=[
            shape(w_key.shape, bf16),
            shape(w_value.shape, bf16),
            shape((2 * SUB, w_beta.shape[0]), bf16),
            shape((SUB, DK)),
            shape((SUB, length)),
            shape((SUB, DK)),
        ],
        in_specs=[pl.BlockSpec(memory_space=pltpu.HBM)] * 8,
        out_specs=[vmem] * 6,
        scratch_shapes=[pltpu.VMEM(x.shape, x.dtype) for x in plain[2:]]
        + [pltpu.SemaphoreType.DMA((2 * heads + 6,))],
        compiler_params=pltpu.CompilerParams(vmem_limit_bytes=24 * 1024 * 1024),
    )(*plain)

    state = None
    flops = 2 * chunk * width * ranks * (2 * heads * DK + DK) + heads * 24 * 2 * chunk * chunk * DK
    weights = [w_key, w_value, gate_weights]
    sums_shape = [shape((2 * SUB, chunk)), shape((chunk, heads * DK)), shape((chunk, heads * DV))]

    def part(found, sums):
        return call(
            functools.partial(part_kernel, tuple(m for m, _ in found), len(sums) > 0),
            [x for _, x in found] + weights + sums,
            sums_shape,
            mib=16,
            flops=2 * chunk * width * len(found) * (2 * heads * DK + DK),
        )

    for c in range(chunks):
        found = gathered[c]
        last = c == chunks - 1
        sums = []
        if c > 0:
            here = [f for f in found if f[0] < 2]
            found = [f for f in found if f[0] >= 2]
            sums = list(part(here, sums))
        if last and len(found) > 1:
            near = [f for f in found if f[0] % 2 == 0]
            found = [f for f in found if f[0] % 2 == 1]
            sums = list(part(near, sums))
        arrays = [x for _, x in found] + weights + [small, forget] + sums
        if c > 0:
            arrays.append(state)
        outs = [shape((heads, DK, DV + DK))]
        if last:
            arrays.append(query)
            outs = [shape((DK + 2 * SUB, DV + DK), bf16)] * heads
        result = call(
            functools.partial(
                chunk_kernel, heads, c, last, tuple(m for m, _ in found), len(sums) > 0
            ),
            arrays,
            outs,
            mib=28,
            flops=flops,
        )
        state = result[-1]
    maps = result

    got = {}
    for k in reversed(range(1, heads)):
        got[k] = swap(maps[k], "sp", k)
    done = [shape((DK, DV + DK)), shape((SUB, DK))]
    open_ended = done + [shape((DK + 2 * SUB, DV + DK), bf16)]
    if groups > 1:
        done.append(shape((DK + 2 * SUB, DV), bf16))
    result = call(
        functools.partial(compose_kernel, heads, groups <= 2),
        [maps[0]] + [got[k] for k in range(1, heads)],
        done if groups <= 2 else open_ended,
        [pltpu.VMEM((heads, DK, DV + DK), f32)],
    )
    mask = heads
    while 2 * mask < count:
        final = 4 * mask == count
        result = call(
            functools.partial(merge_kernel, mask, final),
            [result[0], result[1], swap(result[2], "sp", mask)],
            done if final else open_ended,
        )
        mask *= 2
    arrays = list(result[:2])
    if groups > 1:
        arrays.append(swap(result[2], "sp", count // 2))
    members = count // 2 if groups > 1 else count
    parts = call(
        functools.partial(rows_kernel, heads, groups, rows),
        arrays,
        [shape((rows + 16, DV), bf16)] * heads,
        [pltpu.VMEM((members, rows, DV), f32)],
    )
    moved = {}
    for k in reversed(range(1, heads)):
        moved[k] = swap(parts[k], "sp", k)
    own_rows, first_read = call(
        functools.partial(final_kernel, heads, rows),
        [read_gain[None], parts[0]] + [moved[k] for k in range(1, heads)],
        [shape((heads, rows, DV), bf16), shape((heads, DV))],
        [pltpu.VMEM((heads, SUB, DV), f32)],
    )
    return (own_rows, first_read)


def solution(mesh):
    return jax.shard_map(
        per_device,
        mesh=mesh,
        in_specs=(
            P("sp", "tp"),
            P(None, "tp"),
            P(None, "tp"),
            P(),
            P(),
            P(),
            P(),
            P("tp", "sp"),
            P("tp", "sp"),
            P(),
        ),
        out_specs=(P("tp", "sp", None), P("tp", None)),
        check_vma=False,
    )
```

```python
import functools

import jax
import jax.numpy as jnp
from jax import lax
from jax.experimental import pallas as pl
from jax.experimental.pallas import tpu as pltpu
from jax.sharding import PartitionSpec as P


DK = 128
DV = 128
CHUNK = 128
SUB = 8

norm_eps = 1e-06
bf16 = jnp.bfloat16
f32 = jnp.float32


def flip(axis, mask):
    return [(i, i ^ mask) for i in range(lax.axis_size(axis))]


def swap(x, axis, mask):
    return lax.ppermute(x, axis, flip(axis, mask))


def dot(left, right):
    return jnp.dot(left.astype(bf16), right.astype(bf16), preferred_element_type=f32)


def split(x):
    high = x.astype(bf16)
    return high, (x - high.astype(f32)).astype(bf16)


def dot3(left, right):
    lh, ll = split(left)
    rh, rl = split(right)
    return dot(lh, rh) + (dot(lh, rl) + dot(ll, rh))


def dot_ones(left, ones):
    high, rest = split(left)
    mid = rest
    low = (left - high.astype(f32) - mid.astype(f32)).astype(bf16)
    n = left.shape[0]
    parts = jnp.concatenate([high.astype(f32), mid.astype(f32), low.astype(f32)], axis=0)
    out = dot(parts, ones)
    return out[:n] + out[n : 2 * n] + out[2 * n :]


def dot_nt(left, right):
    return lax.dot_general(
        left.astype(bf16), right.astype(bf16), (((1,), (1,)), ((), ())), preferred_element_type=f32
    )


def unit_inverses(lowers, size):
    row = lax.broadcasted_iota(jnp.int32, (size, size), 0)
    col = lax.broadcasted_iota(jnp.int32, (size, size), 1)
    width = min(16, size)
    near = (row // width) == (col // width)
    inner = [jnp.where(near, low, 0.0) for low in lowers]
    results = [jnp.where(row == col, 1.0, 0.0) - low for low in inner]
    powers = inner
    covered = 2
    while covered < width:
        powers = [dot(p, p) for p in powers]
        results = [r + dot(r, p) for r, p in zip(results, powers)]
        covered *= 2
    if width == size:
        return results
    powers = [dot(r, jnp.where(near, 0.0, low)) for r, low in zip(results, lowers)]
    results = [r - dot(p, r) for r, p in zip(results, powers)]
    covered = 2
    while covered * width < size:
        powers = [dot(p, p) for p in powers]
        results = [r + dot(p, r) for r, p in zip(results, powers)]
        covered *= 2
    return results


def project(masks, piece_refs, wk_ref, wv_ref, wg_ref, sums):
    rank = lax.axis_index("tp")
    gates, keys, values = sums
    placed = []
    for m, ref in zip(masks, piece_refs):
        width = ref.shape[1]
        placed.append((pl.ds(pl.multiple_of((rank ^ m) * width, width), width), ref))
    for rows, ref in placed:
        g = dot_nt(wg_ref[:, rows], ref[...])
        gates = g if gates is None else gates + g
    for rows, ref in placed:
        k = jnp.dot(ref[...], wk_ref[rows, :], preferred_element_type=f32)
        keys = k if keys is None else keys + k
    for rows, ref in placed:
        v = jnp.dot(ref[...], wv_ref[rows, :], preferred_element_type=f32)
        values = v if values is None else values + v
    return gates, keys, values


def part_kernel(masks, prior, *refs):
    pieces = len(masks)
    weights, rest = refs[pieces : pieces + 3], refs[pieces + 3 :]
    sums = (None, None, None)
    if prior:
        sums, rest = tuple(ref[...] for ref in rest[:3]), rest[3:]
    for ref, x in zip(rest, project(masks, refs[:pieces], *weights, sums)):
        ref[...] = x


def prepare_kernel(heads, *refs):
    wk_hbm, wv_hbm = refs[:2]
    wk_ref, wv_ref, wg_ref, small_ref, forget_ref, query_ref = refs[8:14]
    few, sems = refs[14:20], refs[20]
    wb_ref, wd_ref, bias_ref, rate_ref, forget_in, query_in = few
    lead = lax.axis_index("sp") % heads
    first = lax.axis_index("tp") * heads
    early = [
        pltpu.make_async_copy(hbm, ref, sems.at[2 * heads + i])
        for i, (hbm, ref) in enumerate(zip(refs[2:8], few))
    ]
    copies = []
    for k in range(heads):
        source = pl.ds(pl.multiple_of((lead ^ k) * DK, DK), DK)
        target = pl.ds(k * DK, DK)
        for i, (hbm, ref) in enumerate(((wk_hbm, wk_ref), (wv_hbm, wv_ref))):
            copies.append(
                pltpu.make_async_copy(hbm.at[:, source], ref.at[:, target], sems.at[2 * k + i])
            )
    for copy in early + copies:
        copy.start()
    for copy in early:
        copy.wait()
    many = bias_ref.shape[1]
    row = lax.broadcasted_iota(jnp.int32, (2 * SUB, 2 * many), 0)
    col = lax.broadcasted_iota(jnp.int32, (2 * SUB, 2 * many), 1)
    k = row & (SUB - 1)
    wanted = first + (lead ^ k) + jnp.where(row >= SUB, many, 0)
    pick = jnp.where(jnp.logical_and(col == wanted, k < heads), 1.0, 0.0)
    both = jnp.concatenate([wb_ref[...], wd_ref[...]], axis=0)
    wg_ref[...] = dot(pick, both).astype(bf16)
    row = lax.broadcasted_iota(jnp.int32, (SUB, many), 0)
    col = lax.broadcasted_iota(jnp.int32, (SUB, many), 1)
    mine = col == first + (lead ^ row)
    bias = jnp.sum(jnp.where(mine, bias_ref[...], 0.0), axis=1, keepdims=True)
    rate = jnp.sum(jnp.where(mine, rate_ref[...], 0.0), axis=1, keepdims=True)
    lane = lax.broadcasted_iota(jnp.int32, (SUB, DK), 1)
    small_ref[...] = jnp.where(lane == 0, bias, jnp.where(lane == 1, rate, 0.0))
    seats = query_in.shape[1]
    place = lax.axis_index("sp") * seats
    row = lax.broadcasted_iota(jnp.int32, (seats, DK), 0)
    col = lax.broadcasted_iota(jnp.int32, (seats, DK), 1)
    query = dot(query_in[...], jnp.where(col == row + place, 1.0, 0.0))
    forget = forget_in[...]
    size = forget.shape[1]
    wide = lax.broadcasted_iota(jnp.int32, (SUB, size), 0)
    slim = lax.broadcasted_iota(jnp.int32, (SUB, DK), 0)
    forget_out = jnp.zeros((SUB, size), f32)
    query_out = jnp.zeros((SUB, DK), f32)
    for h in range(heads):
        forget_out = jnp.where((lead ^ wide) == h, forget[h : h + 1], forget_out)
        query_out = jnp.where((lead ^ slim) == h, query[h : h + 1], query_out)
    forget_ref[...] = forget_out
    query_ref[...] = query_out
    for copy in copies:
        copy.wait()


def chunk_kernel(heads, index, last, masks, prior, *refs):
    pieces = len(masks)
    piece_refs = refs[:pieces]
    wk_ref, wv_ref, wg_ref, small_ref, forget_ref = refs[pieces : pieces + 5]
    rest = refs[pieces + 5 :]
    sums = (None, None, None)
    if prior:
        sums, rest = tuple(ref[...] for ref in rest[:3]), rest[3:]
    if index > 0:
        state_ref, rest = rest[0], rest[1:]
    if last:
        query_ref, rest = rest[0], rest[1:]
    gates, key_acc, value_acc = project(masks, piece_refs, wk_ref, wv_ref, wg_ref, sums)
    size = key_acc.shape[0]
    bias, rate = small_ref[:, 0:1], small_ref[:, 1:2]
    forget = forget_ref[:, index * size : (index + 1) * size]
    beta_row = jax.nn.sigmoid(gates[0:SUB] + bias)
    log_row = forget - rate * jax.nn.softplus(gates[SUB : 2 * SUB])
    row = lax.broadcasted_iota(jnp.int32, (size, size), 0)
    col = lax.broadcasted_iota(jnp.int32, (size, size), 1)
    strict = row > col
    after = dot_ones(log_row, jnp.where(strict, 1.0, 0.0))
    keep = jnp.exp(after[:, 0:1] + log_row[:, 0:1])
    remain = jnp.exp(after)

    key_raw = key_acc.astype(bf16).astype(f32)
    value_raw = value_acc.astype(bf16)
    keys, lowers = [], []
    for h in range(heads):
        kw = key_raw[:, h * DK : (h + 1) * DK]
        ku = kw * lax.rsqrt(jnp.sum(kw * kw, axis=-1, keepdims=True) + norm_eps)
        keys.append(ku)
        lowers.append(jnp.where(strict, dot_nt(ku, ku), 0.0) * beta_row[h : h + 1, :])
    if index > 0:
        states = [state_ref[h] for h in range(heads)]
    else:
        kr = lax.broadcasted_iota(jnp.int32, (DK, DV + DK), 0)
        kc = lax.broadcasted_iota(jnp.int32, (DK, DV + DK), 1)
        states = [jnp.where(kc == kr + DV, 1.0, 0.0)] * heads
    rights, turned = [], []
    for h in range(heads):
        value = value_raw[:, h * DV : (h + 1) * DV]
        padded = jnp.concatenate([value, jnp.zeros((size, DK), bf16)], axis=1)
        seen = dot(keys[h], states[h]).astype(bf16)
        rights.append(jnp.concatenate([padded, seen], axis=0))
        turned.append(keys[h].T * beta_row[h : h + 1, :])
    fresh = []
    for h, inverse in enumerate(unit_inverses(lowers, size)):
        left = jnp.concatenate(
            [inverse * remain[h : h + 1, :], inverse * -keep[h : h + 1, :]], axis=1
        )
        fresh.append(dot(left, rights[h]))
    for h in range(heads):
        new = keep[h : h + 1, :] * states[h] + dot(turned[h], fresh[h])
        if last:
            rest[h][0:DK, :] = new.astype(bf16)
            asked = jnp.broadcast_to(query_ref[h : h + 1, :], (2 * SUB, DK))
            asked = jnp.concatenate([asked, jnp.zeros((2 * SUB, DV), f32)], axis=1)
            rest[h][DK:, :] = asked.astype(bf16)
        else:
            rest[-1][h] = new


def compose(pairs, product):
    while len(pairs) > 1:
        merged = []
        for early, late in zip(pairs[0::2], pairs[1::2]):
            new = product(late[:, DV:], early)
            merged.append(jnp.concatenate([new[:, :DV] + late[:, :DV], new[:, DV:]], axis=1))
        pairs, product = merged, dot3
    return pairs[0]


def pad_rows(x, rows):
    return jnp.concatenate([x, jnp.zeros((rows - x.shape[0], x.shape[1]), x.dtype)], axis=0)


def late_side(mask):
    return lax.rem(lax.div(lax.axis_index("sp"), jnp.int32(mask)), jnp.int32(2)) == 1


def finish(total, query, out):
    out[0][...] = total
    out[1][...] = query
    if len(out) == 2:
        return
    half = DK // 2
    through = dot3(query, total)
    a, b = total[:, DV:], total[:, :DV]
    high = late_side(lax.axis_size("sp") // 2)
    body = jnp.where(high, jnp.concatenate([a[:half], b[:half]], axis=0), b)
    ah, al = split(through[0:1, DV:])
    bh, bl = split(through[0:1, :DV])
    tail = [query[0:1]] + [x.astype(f32) for x in (ah, al, bh, bl)]
    tail = pad_rows(jnp.concatenate(tail, axis=0), 2 * SUB)
    out[2][0:DK, :] = body.astype(bf16)
    out[2][DK:, :] = tail.astype(bf16)


def passed_on(total, query):
    asked = jnp.concatenate([query, query], axis=0)
    asked = jnp.concatenate([asked, jnp.zeros((2 * SUB, DV), f32)], axis=1)
    return jnp.concatenate([total, asked], axis=0).astype(bf16)


def compose_kernel(heads, final, *refs):
    own_ref, got = refs[0], refs[1:heads]
    out, scratch = refs[heads:-1], refs[-1]
    lead = lax.axis_index("sp") % heads
    scratch[lead] = own_ref[:DK, :].astype(f32)
    query = own_ref[DK:, :DK].astype(f32)
    for k in range(1, heads):
        scratch[lead ^ k] = got[k - 1][:DK, :].astype(f32)
        query = query + got[k - 1][DK:, :DK].astype(f32)
    total = compose([scratch[i] for i in range(heads)], dot)
    query = query[:SUB]
    if final:
        finish(total, query, out)
    else:
        out[0][...], out[1][...] = total, query
        out[2][...] = passed_on(total, query)


def merge_kernel(mask, final, own_ref, query_ref, got_ref, *out):
    high = late_side(mask)
    own, got = own_ref[...], got_ref[:DK, :].astype(f32)
    query = query_ref[...] + got_ref[DK:, :DK].astype(f32)[:SUB]
    early, late = jnp.where(high, got, own), jnp.where(high, own, got)
    total = compose([early, late], dot3)
    if final:
        finish(total, query, out)
    else:
        out[0][...], out[1][...] = total, query
        out[2][...] = passed_on(total, query)


def rows_kernel(heads, groups, rows, own_ref, query_ref, *refs):
    if groups > 1:
        got_ref, refs = refs[0], refs[1:]
    scratch = refs[-1]
    own, query = own_ref[...], query_ref[...]
    half = DK // 2
    place = lax.axis_index("sp")
    if groups > 1:
        high = late_side(lax.axis_size("sp") // 2)
        got = got_ref[...].astype(f32)
        a, b = own[:, DV:], own[:, :DV]
        early = jnp.where(high, got[:DK], b)
        late_a = jnp.where(high, a[half:], got[:half])
        late_b = jnp.where(high, b[half:], got[half:DK])
        tail = got[DK:]
        cross = dot3(jnp.broadcast_to(tail[0:1], (SUB, DK)), own)[0:1]
        through_a = jnp.where(high, cross[:, DV:], tail[1:2] + tail[2:3])
        through_b = jnp.where(high, cross[:, :DV], tail[3:4] + tail[4:5])
        both = dot3(pad_rows(jnp.concatenate([late_a, through_a], axis=0), half + SUB), early)
        state = both[:half] + late_b
        asked = jnp.where(high, query[:, half:], query[:, :half])
        read = dot3(asked, state)[0:1] + (both[half : half + 1] + through_b)
    else:
        state = own[:, :DV]
        read = dot3(query, state)[0:1]
    members = state.shape[0] // rows
    for i in range(members):
        scratch[i] = state[i * rows : (i + 1) * rows]
    place = place % members
    rh, rl = split(read)
    tail = pad_rows(jnp.concatenate([rh.astype(f32), rl.astype(f32)], axis=0), 16)
    for k in range(heads):
        body = scratch[place ^ k]
        refs[k][...] = jnp.concatenate([body, tail], axis=0).astype(bf16)


def final_kernel(heads, rows, gain_ref, *refs):
    lead = lax.axis_index("sp") % heads
    state_ref, read_ref, scratch = refs[heads:]
    for k in range(heads):
        part = refs[k][...]
        state_ref[lead ^ k] = part[:rows]
        wide = part[rows : rows + 2].astype(f32)
        scratch[lead ^ k] = jnp.broadcast_to(wide[0:1] + wide[1:2], (SUB, DV))
    raw = jnp.concatenate([scratch[h][0:1] for h in range(heads)], axis=0)
    norm = lax.rsqrt(jnp.mean(raw * raw, axis=-1, keepdims=True) + norm_eps)
    read_ref[...] = raw * norm * gain_ref[...].astype(f32)


def shape(dims, dtype=f32):
    return jax.ShapeDtypeStruct(dims, dtype)


vmem = pl.BlockSpec(memory_space=pltpu.VMEM)


def call(body, arrays, outs, scratch=(), mib=8, flops=0):
    return pl.pallas_call(
        body,
        out_shape=outs,
        in_specs=[vmem] * len(arrays),
        out_specs=jax.tree.map(lambda _: vmem, outs),
        scratch_shapes=list(scratch),
        compiler_params=pltpu.CompilerParams(vmem_limit_bytes=mib * 1024 * 1024),
        cost_estimate=pl.CostEstimate(flops=flops, bytes_accessed=0, transcendentals=0)
        if flops
        else None,
    )(*arrays)


def per_device(
    tokens,
    w_key,
    w_value,
    w_beta,
    w_decay,
    beta_bias,
    decay_rate,
    forgetting_increment,
    new_query,
    read_gain,
):
    heads = w_key.shape[1] // DK
    length, width = tokens.shape
    count = lax.axis_size("sp")
    ranks = lax.axis_size("tp")
    groups = count // heads
    rows = DK // count
    chunk = min(CHUNK, length)
    chunks = length // chunk

    owns = [tokens[:chunk]]
    later = lax.optimization_barrier(tokens)
    owns += [later[c * chunk : (c + 1) * chunk] for c in range(1, chunks)]
    gathered = []
    for c in range(chunks):
        found = [(0, owns[c])]
        for hop in range(1, ranks // 2):
            found.append((2 * hop, swap(owns[c], "tp", 2 * hop)))
        found.append((1, swap(owns[c], "tp", 1)))
        found += [(m ^ 1, swap(x, "tp", 1)) for m, x in found[1:-1]]
        gathered.append(found)

    plain = [
        pltpu.with_memory_space_constraint(x, pltpu.HBM)
        for x in (
            w_key,
            w_value,
            w_beta.T,
            w_decay.T,
            beta_bias[None],
            decay_rate[None],
            forgetting_increment,
            new_query,
        )
    ]
    w_key, w_value, gate_weights, small, forget, query = pl.pallas_call(
        functools.partial(prepare_kernel, heads),
        out_shape=[
            shape(w_key.shape, bf16),
            shape(w_value.shape, bf16),
            shape((2 * SUB, w_beta.shape[0]), bf16),
            shape((SUB, DK)),
            shape((SUB, length)),
            shape((SUB, DK)),
        ],
        in_specs=[pl.BlockSpec(memory_space=pltpu.HBM)] * 8,
        out_specs=[vmem] * 6,
        scratch_shapes=[pltpu.VMEM(x.shape, x.dtype) for x in plain[2:]]
        + [pltpu.SemaphoreType.DMA((2 * heads + 6,))],
        compiler_params=pltpu.CompilerParams(vmem_limit_bytes=24 * 1024 * 1024),
    )(*plain)

    state = None
    flops = 2 * chunk * width * ranks * (2 * heads * DK + DK) + heads * 24 * 2 * chunk * chunk * DK
    weights = [w_key, w_value, gate_weights]
    sums_shape = [shape((2 * SUB, chunk)), shape((chunk, heads * DK)), shape((chunk, heads * DV))]

    def part(found, sums):
        return call(
            functools.partial(part_kernel, tuple(m for m, _ in found), len(sums) > 0),
            [x for _, x in found] + weights + sums,
            sums_shape,
            mib=16,
            flops=2 * chunk * width * len(found) * (2 * heads * DK + DK),
        )

    for c in range(chunks):
        found = gathered[c]
        last = c == chunks - 1
        sums = []
        if c > 0:
            here = [f for f in found if f[0] < 2]
            found = [f for f in found if f[0] >= 2]
            sums = list(part(here, sums))
        if last and len(found) > 1:
            near = [f for f in found if f[0] % 2 == 0]
            found = [f for f in found if f[0] % 2 == 1]
            sums = list(part(near, sums))
        arrays = [x for _, x in found] + weights + [small, forget] + sums
        if c > 0:
            arrays.append(state)
        outs = [shape((heads, DK, DV + DK))]
        if last:
            arrays.append(query)
            outs = [shape((DK + 2 * SUB, DV + DK), bf16)] * heads
        result = call(
            functools.partial(
                chunk_kernel, heads, c, last, tuple(m for m, _ in found), len(sums) > 0
            ),
            arrays,
            outs,
            mib=28,
            flops=flops,
        )
        state = result[-1]
    maps = result

    got = {}
    for k in reversed(range(1, heads)):
        got[k] = swap(maps[k], "sp", k)
    done = [shape((DK, DV + DK)), shape((SUB, DK))]
    open_ended = done + [shape((DK + 2 * SUB, DV + DK), bf16)]
    if groups > 1:
        done.append(shape((DK + 2 * SUB, DV), bf16))
    result = call(
        functools.partial(compose_kernel, heads, groups <= 2),
        [maps[0]] + [got[k] for k in range(1, heads)],
        done if groups <= 2 else open_ended,
        [pltpu.VMEM((heads, DK, DV + DK), f32)],
    )
    mask = heads
    while 2 * mask < count:
        final = 4 * mask == count
        result = call(
            functools.partial(merge_kernel, mask, final),
            [result[0], result[1], swap(result[2], "sp", mask)],
            done if final else open_ended,
        )
        mask *= 2
    arrays = list(result[:2])
    if groups > 1:
        arrays.append(swap(result[2], "sp", count // 2))
    members = count // 2 if groups > 1 else count
    parts = call(
        functools.partial(rows_kernel, heads, groups, rows),
        arrays,
        [shape((rows + 16, DV), bf16)] * heads,
        [pltpu.VMEM((members, rows, DV), f32)],
    )
    moved = {}
    for k in reversed(range(1, heads)):
        moved[k] = swap(parts[k], "sp", k)
    own_rows, first_read = call(
        functools.partial(final_kernel, heads, rows),
        [read_gain[None], parts[0]] + [moved[k] for k in range(1, heads)],
        [shape((heads, rows, DV), bf16), shape((heads, DV))],
        [pltpu.VMEM((heads, SUB, DV), f32)],
    )
    return (own_rows, first_read)


def solution(mesh):
    return jax.shard_map(
        per_device,
        mesh=mesh,
        in_specs=(
            P("sp", "tp"),
            P(None, "tp"),
            P(None, "tp"),
            P(),
            P(),
            P(),
            P(),
            P("tp", "sp"),
            P("tp", "sp"),
            P(),
        ),
        out_specs=(P("tp", "sp", None), P("tp", None)),
        check_vma=False,
    )
```

```python
import functools
import math

import jax
import jax.numpy as jnp
from jax import lax
from jax.experimental import pallas as pl
from jax.experimental.pallas import tpu as pltpu
from jax.sharding import PartitionSpec as P


DK = 128
DV = 128
CHUNK = 128
SUB = 8

norm_eps = 1e-06
bf16 = jnp.bfloat16
f32 = jnp.float32


def flip(axis, mask):
    return [(i, i ^ mask) for i in range(lax.axis_size(axis))]


def swap(x, axis, mask):
    return lax.ppermute(x, axis, flip(axis, mask))


def dot(left, right):
    return jnp.dot(left.astype(bf16), right.astype(bf16), preferred_element_type=f32)


def split(x):
    high = x.astype(bf16)
    return high, (x - high.astype(f32)).astype(bf16)


def dot3(left, right):
    lh, ll = split(left)
    rh, rl = split(right)
    return dot(lh, rh) + (dot(lh, rl) + dot(ll, rh))


def dot_ones(left, ones):
    high, rest = split(left)
    mid = rest
    low = (left - high.astype(f32) - mid.astype(f32)).astype(bf16)
    n = left.shape[0]
    parts = jnp.concatenate([high.astype(f32), mid.astype(f32), low.astype(f32)], axis=0)
    out = dot(parts, ones)
    return out[:n] + out[n : 2 * n] + out[2 * n :]


def dot_nt(left, right):
    return lax.dot_general(
        left.astype(bf16), right.astype(bf16), (((1,), (1,)), ((), ())), preferred_element_type=f32
    )


def unit_inverses(lowers, size):
    row = lax.broadcasted_iota(jnp.int32, (size, size), 0)
    col = lax.broadcasted_iota(jnp.int32, (size, size), 1)
    width = min(16, size)
    near = (row // width) == (col // width)
    inner = [jnp.where(near, low, 0.0) for low in lowers]
    results = [jnp.where(row == col, 1.0, 0.0) - low for low in inner]
    powers = inner
    covered = 2
    while covered < width:
        powers = [dot(p, p) for p in powers]
        results = [r + dot(r, p) for r, p in zip(results, powers)]
        covered *= 2
    if width == size:
        return results
    powers = [dot(r, jnp.where(near, 0.0, low)) for r, low in zip(results, lowers)]
    results = [r - dot(p, r) for r, p in zip(results, powers)]
    covered = 2
    while covered * width < size:
        powers = [dot(p, p) for p in powers]
        results = [r + dot(p, r) for r, p in zip(results, powers)]
        covered *= 2
    return results


def project(masks, piece_refs, wk_ref, wv_ref, wg_ref, sums):
    rank = lax.axis_index("tp")
    gates, keys, values = sums
    share = wk_ref.shape[0] // lax.axis_size("tp")
    placed = []
    for (m, shift), ref in zip(masks, piece_refs):
        width = ref.shape[1]
        start = pl.multiple_of((rank ^ m) * share + shift, math.gcd(share, width))
        placed.append((pl.ds(start, width), ref))
    for rows, ref in placed:
        g = dot_nt(wg_ref[:, rows], ref[...])
        gates = g if gates is None else gates + g
    for rows, ref in placed:
        k = jnp.dot(ref[...], wk_ref[rows, :], preferred_element_type=f32)
        keys = k if keys is None else keys + k
    for rows, ref in placed:
        v = jnp.dot(ref[...], wv_ref[rows, :], preferred_element_type=f32)
        values = v if values is None else values + v
    return gates, keys, values


def part_kernel(masks, prior, *refs):
    pieces = len(masks)
    weights, rest = refs[pieces : pieces + 3], refs[pieces + 3 :]
    sums = (None, None, None)
    if prior:
        sums, rest = tuple(ref[...] for ref in rest[:3]), rest[3:]
    for ref, x in zip(rest, project(masks, refs[:pieces], *weights, sums)):
        ref[...] = x


def prepare_kernel(heads, *refs):
    wk_hbm, wv_hbm = refs[:2]
    wk_ref, wv_ref, wg_ref, small_ref, forget_ref, query_ref = refs[8:14]
    few, sems = refs[14:20], refs[20]
    wb_ref, wd_ref, bias_ref, rate_ref, forget_in, query_in = few
    lead = lax.axis_index("sp") % heads
    first = lax.axis_index("tp") * heads
    early = [
        pltpu.make_async_copy(hbm, ref, sems.at[2 * heads + i])
        for i, (hbm, ref) in enumerate(zip(refs[2:8], few))
    ]
    copies = []
    for k in range(heads):
        source = pl.ds(pl.multiple_of((lead ^ k) * DK, DK), DK)
        target = pl.ds(k * DK, DK)
        for i, (hbm, ref) in enumerate(((wk_hbm, wk_ref), (wv_hbm, wv_ref))):
            copies.append(
                pltpu.make_async_copy(hbm.at[:, source], ref.at[:, target], sems.at[2 * k + i])
            )
    for copy in early + copies:
        copy.start()
    for copy in early:
        copy.wait()
    many = bias_ref.shape[1]
    row = lax.broadcasted_iota(jnp.int32, (2 * SUB, 2 * many), 0)
    col = lax.broadcasted_iota(jnp.int32, (2 * SUB, 2 * many), 1)
    k = row & (SUB - 1)
    wanted = first + (lead ^ k) + jnp.where(row >= SUB, many, 0)
    pick = jnp.where(jnp.logical_and(col == wanted, k < heads), 1.0, 0.0)
    both = jnp.concatenate([wb_ref[...], wd_ref[...]], axis=0)
    wg_ref[...] = dot(pick, both).astype(bf16)
    row = lax.broadcasted_iota(jnp.int32, (SUB, many), 0)
    col = lax.broadcasted_iota(jnp.int32, (SUB, many), 1)
    mine = col == first + (lead ^ row)
    bias = jnp.sum(jnp.where(mine, bias_ref[...], 0.0), axis=1, keepdims=True)
    rate = jnp.sum(jnp.where(mine, rate_ref[...], 0.0), axis=1, keepdims=True)
    lane = lax.broadcasted_iota(jnp.int32, (SUB, DK), 1)
    small_ref[...] = jnp.where(lane == 0, bias, jnp.where(lane == 1, rate, 0.0))
    seats = query_in.shape[1]
    place = lax.axis_index("sp") * seats
    row = lax.broadcasted_iota(jnp.int32, (seats, DK), 0)
    col = lax.broadcasted_iota(jnp.int32, (seats, DK), 1)
    query = dot(query_in[...], jnp.where(col == row + place, 1.0, 0.0))
    forget = forget_in[...]
    size = forget.shape[1]
    wide = lax.broadcasted_iota(jnp.int32, (SUB, size), 0)
    slim = lax.broadcasted_iota(jnp.int32, (SUB, DK), 0)
    forget_out = jnp.zeros((SUB, size), f32)
    query_out = jnp.zeros((SUB, DK), f32)
    for h in range(heads):
        forget_out = jnp.where((lead ^ wide) == h, forget[h : h + 1], forget_out)
        query_out = jnp.where((lead ^ slim) == h, query[h : h + 1], query_out)
    forget_ref[...] = forget_out
    query_ref[...] = query_out
    for copy in copies:
        copy.wait()


def chunk_kernel(heads, index, last, masks, prior, *refs):
    pieces = len(masks)
    piece_refs = refs[:pieces]
    wk_ref, wv_ref, wg_ref, small_ref, forget_ref = refs[pieces : pieces + 5]
    rest = refs[pieces + 5 :]
    sums = (None, None, None)
    if prior:
        sums, rest = tuple(ref[...] for ref in rest[:3]), rest[3:]
    if index > 0:
        state_ref, rest = rest[0], rest[1:]
    if last:
        query_ref, rest = rest[0], rest[1:]
    gates, key_acc, value_acc = project(masks, piece_refs, wk_ref, wv_ref, wg_ref, sums)
    size = key_acc.shape[0]
    bias, rate = small_ref[:, 0:1], small_ref[:, 1:2]
    forget = forget_ref[:, index * size : (index + 1) * size]
    beta_row = jax.nn.sigmoid(gates[0:SUB] + bias)
    log_row = forget - rate * jax.nn.softplus(gates[SUB : 2 * SUB])
    row = lax.broadcasted_iota(jnp.int32, (size, size), 0)
    col = lax.broadcasted_iota(jnp.int32, (size, size), 1)
    strict = row > col
    after = dot_ones(log_row, jnp.where(strict, 1.0, 0.0))
    keep = jnp.exp(after[:, 0:1] + log_row[:, 0:1])
    remain = jnp.exp(after)

    key_raw = key_acc.astype(bf16).astype(f32)
    value_raw = value_acc.astype(bf16)
    keys, lowers = [], []
    for h in range(heads):
        kw = key_raw[:, h * DK : (h + 1) * DK]
        ku = kw * lax.rsqrt(jnp.sum(kw * kw, axis=-1, keepdims=True) + norm_eps)
        keys.append(ku)
        lowers.append(jnp.where(strict, dot_nt(ku, ku), 0.0) * beta_row[h : h + 1, :])
    if index > 0:
        states = [state_ref[h] for h in range(heads)]
    else:
        kr = lax.broadcasted_iota(jnp.int32, (DK, DV + DK), 0)
        kc = lax.broadcasted_iota(jnp.int32, (DK, DV + DK), 1)
        states = [jnp.where(kc == kr + DV, 1.0, 0.0)] * heads
    rights, turned = [], []
    for h in range(heads):
        value = value_raw[:, h * DV : (h + 1) * DV]
        padded = jnp.concatenate([value, jnp.zeros((size, DK), bf16)], axis=1)
        seen = dot(keys[h], states[h]).astype(bf16)
        rights.append(jnp.concatenate([padded, seen], axis=0))
        turned.append(keys[h].T * beta_row[h : h + 1, :])
    fresh = []
    for h, inverse in enumerate(unit_inverses(lowers, size)):
        left = jnp.concatenate(
            [inverse * remain[h : h + 1, :], inverse * -keep[h : h + 1, :]], axis=1
        )
        fresh.append(dot(left, rights[h]))
    for h in range(heads):
        new = keep[h : h + 1, :] * states[h] + dot(turned[h], fresh[h])
        if last:
            rest[h][...] = passed_on(new, jnp.broadcast_to(query_ref[h : h + 1, :], (SUB, DK)))
        else:
            rest[-1][h] = new


def compose(pairs, product):
    while len(pairs) > 1:
        merged = []
        for early, late in zip(pairs[0::2], pairs[1::2]):
            new = product(late[:, DV:], early)
            merged.append(jnp.concatenate([new[:, :DV] + late[:, :DV], new[:, DV:]], axis=1))
        pairs, product = merged, dot3
    return pairs[0]


def pad_rows(x, rows):
    return jnp.concatenate([x, jnp.zeros((rows - x.shape[0], x.shape[1]), x.dtype)], axis=0)


def late_side(mask):
    return lax.rem(lax.div(lax.axis_index("sp"), jnp.int32(mask)), jnp.int32(2)) == 1


def finish(total, query, out):
    out[0][...] = total
    out[1][...] = query
    if len(out) == 2:
        return
    half = DK // 2
    through = dot3(query, total)
    a, b = total[:, DV:], total[:, :DV]
    high = late_side(lax.axis_size("sp") // 2)
    body = jnp.where(high, jnp.concatenate([a[:half], b[:half]], axis=0), b)
    ah, al = split(through[0:1, DV:])
    bh, bl = split(through[0:1, :DV])
    tail = [query[0:1]] + [x.astype(f32) for x in (ah, al, bh, bl)]
    tail = pad_rows(jnp.concatenate(tail, axis=0), 2 * SUB)
    out[2][0:DK, :] = body.astype(bf16)
    out[2][DK:, :] = tail.astype(bf16)


def passed_on(total, query):
    return jnp.concatenate([total[:, :DV], total[:, DV:], query, query], axis=0).astype(bf16)


def received(ref):
    total = jnp.concatenate([ref[:DK, :], ref[DK : 2 * DK, :]], axis=1)
    return total.astype(f32), ref[2 * DK :, :].astype(f32)[:SUB]


def compose_kernel(heads, final, *refs):
    own_ref, got = refs[0], refs[1:heads]
    out, scratch = refs[heads:-1], refs[-1]
    lead = lax.axis_index("sp") % heads
    scratch[lead], query = received(own_ref)
    for k in range(1, heads):
        scratch[lead ^ k], asked = received(got[k - 1])
        query = query + asked
    total = compose([scratch[i] for i in range(heads)], dot)
    if final:
        finish(total, query, out)
    else:
        out[0][...], out[1][...] = total, query
        out[2][...] = passed_on(total, query)


def merge_kernel(mask, final, own_ref, query_ref, got_ref, *out):
    high = late_side(mask)
    own, (got, asked) = own_ref[...], received(got_ref)
    query = query_ref[...] + asked
    early, late = jnp.where(high, got, own), jnp.where(high, own, got)
    total = compose([early, late], dot3)
    if final:
        finish(total, query, out)
    else:
        out[0][...], out[1][...] = total, query
        out[2][...] = passed_on(total, query)


def rows_kernel(heads, groups, rows, own_ref, query_ref, *refs):
    if groups > 1:
        got_ref, refs = refs[0], refs[1:]
    scratch = refs[-1]
    own, query = own_ref[...], query_ref[...]
    half = DK // 2
    place = lax.axis_index("sp")
    if groups > 1:
        high = late_side(lax.axis_size("sp") // 2)
        got = got_ref[...].astype(f32)
        a, b = own[:, DV:], own[:, :DV]
        early = jnp.where(high, got[:DK], b)
        late_a = jnp.where(high, a[half:], got[:half])
        late_b = jnp.where(high, b[half:], got[half:DK])
        tail = got[DK:]
        cross = dot3(jnp.broadcast_to(tail[0:1], (SUB, DK)), own)[0:1]
        through_a = jnp.where(high, cross[:, DV:], tail[1:2] + tail[2:3])
        through_b = jnp.where(high, cross[:, :DV], tail[3:4] + tail[4:5])
        both = dot3(pad_rows(jnp.concatenate([late_a, through_a], axis=0), half + SUB), early)
        state = both[:half] + late_b
        asked = jnp.where(high, query[:, half:], query[:, :half])
        read = dot3(asked, state)[0:1] + (both[half : half + 1] + through_b)
    else:
        state = own[:, :DV]
        read = dot3(query, state)[0:1]
    members = state.shape[0] // rows
    for i in range(members):
        scratch[i] = state[i * rows : (i + 1) * rows]
    place = place % members
    rh, rl = split(read)
    tail = pad_rows(jnp.concatenate([rh.astype(f32), rl.astype(f32)], axis=0), 16)
    for k in range(heads):
        body = scratch[place ^ k]
        refs[k][...] = jnp.concatenate([body, tail], axis=0).astype(bf16)


def final_kernel(heads, rows, gain_ref, *refs):
    lead = lax.axis_index("sp") % heads
    state_ref, read_ref, scratch = refs[heads:]
    for k in range(heads):
        part = refs[k][...]
        state_ref[lead ^ k] = part[:rows]
        wide = part[rows : rows + 2].astype(f32)
        scratch[lead ^ k] = jnp.broadcast_to(wide[0:1] + wide[1:2], (SUB, DV))
    raw = jnp.concatenate([scratch[h][0:1] for h in range(heads)], axis=0)
    norm = lax.rsqrt(jnp.mean(raw * raw, axis=-1, keepdims=True) + norm_eps)
    read_ref[...] = raw * norm * gain_ref[...].astype(f32)


def shape(dims, dtype=f32):
    return jax.ShapeDtypeStruct(dims, dtype)


vmem = pl.BlockSpec(memory_space=pltpu.VMEM)


def call(body, arrays, outs, scratch=(), mib=8, flops=0):
    return pl.pallas_call(
        body,
        out_shape=outs,
        in_specs=[vmem] * len(arrays),
        out_specs=jax.tree.map(lambda _: vmem, outs),
        scratch_shapes=list(scratch),
        compiler_params=pltpu.CompilerParams(vmem_limit_bytes=mib * 1024 * 1024),
        cost_estimate=pl.CostEstimate(flops=flops, bytes_accessed=0, transcendentals=0)
        if flops
        else None,
    )(*arrays)


def per_device(
    tokens,
    w_key,
    w_value,
    w_beta,
    w_decay,
    beta_bias,
    decay_rate,
    forgetting_increment,
    new_query,
    read_gain,
):
    heads = w_key.shape[1] // DK
    length, width = tokens.shape
    count = lax.axis_size("sp")
    ranks = lax.axis_size("tp")
    groups = count // heads
    rows = DK // count
    chunk = min(CHUNK, length)
    chunks = length // chunk

    owns = [tokens[:chunk]]
    later = lax.optimization_barrier(tokens)
    owns += [later[c * chunk : (c + 1) * chunk] for c in range(1, chunks)]
    gathered = []
    for c in range(chunks):
        found = [(0, 0, owns[c], False)]
        found.append((1, 0, swap(owns[c], "tp", 1), False))
        halves = 2 if c == chunks - 1 and width % 256 == 0 else 1
        part_width = width // halves
        for half in range(halves):
            shift = half * part_width
            block = owns[c][:, shift : shift + part_width]
            late = half == halves - 1
            for hop in range(1, ranks // 2):
                near = swap(block, "tp", 2 * hop)
                far = swap(near, "tp", 1)
                found += [(2 * hop, shift, near, late), (2 * hop + 1, shift, far, late)]
        gathered.append(found)

    plain = [
        pltpu.with_memory_space_constraint(x, pltpu.HBM)
        for x in (
            w_key,
            w_value,
            w_beta.T,
            w_decay.T,
            beta_bias[None],
            decay_rate[None],
            forgetting_increment,
            new_query,
        )
    ]
    w_key, w_value, gate_weights, small, forget, query = pl.pallas_call(
        functools.partial(prepare_kernel, heads),
        out_shape=[
            shape(w_key.shape, bf16),
            shape(w_value.shape, bf16),
            shape((2 * SUB, w_beta.shape[0]), bf16),
            shape((SUB, DK)),
            shape((SUB, length)),
            shape((SUB, DK)),
        ],
        in_specs=[pl.BlockSpec(memory_space=pltpu.HBM)] * 8,
        out_specs=[vmem] * 6,
        scratch_shapes=[pltpu.VMEM(x.shape, x.dtype) for x in plain[2:]]
        + [pltpu.SemaphoreType.DMA((2 * heads + 6,))],
        compiler_params=pltpu.CompilerParams(vmem_limit_bytes=24 * 1024 * 1024),
    )(*plain)

    state = None
    flops = 2 * chunk * width * ranks * (2 * heads * DK + DK) + heads * 24 * 2 * chunk * chunk * DK
    weights = [w_key, w_value, gate_weights]
    sums_shape = [shape((2 * SUB, chunk)), shape((chunk, heads * DK)), shape((chunk, heads * DV))]

    def part(found, sums):
        out = call(
            functools.partial(part_kernel, tuple(f[:2] for f in found), len(sums) > 0),
            [f[2] for f in found] + weights + sums,
            sums_shape,
            mib=16,
            flops=2 * chunk * sum(f[2].shape[1] for f in found) * (2 * heads * DK + DK),
        )
        return list(out)

    for c in range(chunks):
        found = gathered[c]
        last = c == chunks - 1
        sums = []
        if c > 0:
            sums = part([f for f in found if f[0] < 2], sums)
            found = [f for f in found if f[0] >= 2]
        if last and len(found) > 1:
            relayed = [f for f in found if f[3] and f[0] % 2 == 1]
            sums = part([f for f in found if not (f[3] and f[0] % 2 == 1)], sums)
            found = relayed
        masks = tuple(f[:2] for f in found)
        arrays = [f[2] for f in found] + weights + [small, forget] + sums
        if c > 0:
            arrays.append(state)
        outs = [shape((heads, DK, DV + DK))]
        if last:
            arrays.append(query)
            outs = [shape((DK + DV + 2 * SUB, DK), bf16)] * heads
        result = call(
            functools.partial(
                chunk_kernel, heads, c, last, masks, len(sums) > 0
            ),
            arrays,
            outs,
            mib=28,
            flops=flops,
        )
        state = result[-1]
    maps = result

    got = {}
    for k in reversed(range(1, heads)):
        got[k] = swap(maps[k], "sp", k)
    done = [shape((DK, DV + DK)), shape((SUB, DK))]
    open_ended = done + [shape((DK + DV + 2 * SUB, DK), bf16)]
    if groups > 1:
        done.append(shape((DK + 2 * SUB, DV), bf16))
    result = call(
        functools.partial(compose_kernel, heads, groups <= 2),
        [maps[0]] + [got[k] for k in range(1, heads)],
        done if groups <= 2 else open_ended,
        [pltpu.VMEM((heads, DK, DV + DK), f32)],
    )
    mask = heads
    while 2 * mask < count:
        final = 4 * mask == count
        result = call(
            functools.partial(merge_kernel, mask, final),
            [result[0], result[1], swap(result[2], "sp", mask)],
            done if final else open_ended,
        )
        mask *= 2
    arrays = list(result[:2])
    if groups > 1:
        arrays.append(swap(result[2], "sp", count // 2))
    members = count // 2 if groups > 1 else count
    parts = call(
        functools.partial(rows_kernel, heads, groups, rows),
        arrays,
        [shape((rows + 16, DV), bf16)] * heads,
        [pltpu.VMEM((members, rows, DV), f32)],
    )
    moved = {}
    for k in reversed(range(1, heads)):
        moved[k] = swap(parts[k], "sp", k)
    own_rows, first_read = call(
        functools.partial(final_kernel, heads, rows),
        [read_gain[None], parts[0]] + [moved[k] for k in range(1, heads)],
        [shape((heads, rows, DV), bf16), shape((heads, DV))],
        [pltpu.VMEM((heads, SUB, DV), f32)],
    )
    return (own_rows, first_read)


def solution(mesh):
    return jax.shard_map(
        per_device,
        mesh=mesh,
        in_specs=(
            P("sp", "tp"),
            P(None, "tp"),
            P(None, "tp"),
            P(),
            P(),
            P(),
            P(),
            P("tp", "sp"),
            P("tp", "sp"),
            P(),
        ),
        out_specs=(P("tp", "sp", None), P("tp", None)),
        check_vma=False,
    )
```

```python
import functools

import jax
import jax.numpy as jnp
from jax import lax
from jax.experimental import pallas as pl
from jax.experimental.pallas import tpu as pltpu
from jax.sharding import PartitionSpec as P


DK = 128
DV = 128
CHUNK = 128
SUB = 8

norm_eps = 1e-06
bf16 = jnp.bfloat16
f32 = jnp.float32


def flip(axis, mask):
    return [(i, i ^ mask) for i in range(lax.axis_size(axis))]


def swap(x, axis, mask):
    return lax.ppermute(x, axis, flip(axis, mask))


def dot(left, right):
    return jnp.dot(left.astype(bf16), right.astype(bf16), preferred_element_type=f32)


def split(x):
    high = x.astype(bf16)
    return high, (x - high.astype(f32)).astype(bf16)


def dot3(left, right):
    lh, ll = split(left)
    rh, rl = split(right)
    return dot(lh, rh) + (dot(lh, rl) + dot(ll, rh))


def dot_ones(left, ones):
    high, rest = split(left)
    mid = rest
    low = (left - high.astype(f32) - mid.astype(f32)).astype(bf16)
    n = left.shape[0]
    parts = jnp.concatenate([high.astype(f32), mid.astype(f32), low.astype(f32)], axis=0)
    out = dot(parts, ones)
    return out[:n] + out[n : 2 * n] + out[2 * n :]


def dot_nt(left, right):
    return lax.dot_general(
        left.astype(bf16), right.astype(bf16), (((1,), (1,)), ((), ())), preferred_element_type=f32
    )


def unit_inverses(lowers, size):
    row = lax.broadcasted_iota(jnp.int32, (size, size), 0)
    col = lax.broadcasted_iota(jnp.int32, (size, size), 1)
    width = min(16, size)
    near = (row // width) == (col // width)
    inner = [jnp.where(near, low, 0.0) for low in lowers]
    results = [jnp.where(row == col, 1.0, 0.0) - low for low in inner]
    powers = inner
    covered = 2
    while covered < width:
        powers = [dot(p, p) for p in powers]
        results = [r + dot(r, p) for r, p in zip(results, powers)]
        covered *= 2
    if width == size:
        return results
    powers = [dot(r, jnp.where(near, 0.0, low)) for r, low in zip(results, lowers)]
    results = [r - dot(p, r) for r, p in zip(results, powers)]
    covered = 2
    while covered * width < size:
        powers = [dot(p, p) for p in powers]
        results = [r + dot(p, r) for r, p in zip(results, powers)]
        covered *= 2
    return results


def project(masks, piece_refs, wk_ref, wv_ref, wg_ref, sums):
    rank = lax.axis_index("tp")
    gates, keys, values = sums
    placed = []
    for m, ref in zip(masks, piece_refs):
        width = ref.shape[1]
        placed.append((pl.ds(pl.multiple_of((rank ^ m) * width, width), width), ref))
    for rows, ref in placed:
        g = dot_nt(wg_ref[:, rows], ref[...])
        gates = g if gates is None else gates + g
    for rows, ref in placed:
        k = jnp.dot(ref[...], wk_ref[rows, :], preferred_element_type=f32)
        keys = k if keys is None else keys + k
    for rows, ref in placed:
        v = jnp.dot(ref[...], wv_ref[rows, :], preferred_element_type=f32)
        values = v if values is None else values + v
    return gates, keys, values


def part_kernel(masks, prior, *refs):
    pieces = len(masks)
    weights, rest = refs[pieces : pieces + 3], refs[pieces + 3 :]
    sums = (None, None, None)
    if prior:
        sums, rest = tuple(ref[...] for ref in rest[:3]), rest[3:]
    for ref, x in zip(rest, project(masks, refs[:pieces], *weights, sums)):
        ref[...] = x


def prepare_kernel(heads, *refs):
    wk_hbm, wv_hbm = refs[:2]
    wk_ref, wv_ref, wg_ref, small_ref, forget_ref, query_ref = refs[8:14]
    few, sems = refs[14:20], refs[20]
    wb_ref, wd_ref, bias_ref, rate_ref, forget_in, query_in = few
    lead = lax.axis_index("sp") % heads
    first = lax.axis_index("tp") * heads
    early = [
        pltpu.make_async_copy(hbm, ref, sems.at[2 * heads + i])
        for i, (hbm, ref) in enumerate(zip(refs[2:8], few))
    ]
    copies = []
    for k in range(heads):
        source = pl.ds(pl.multiple_of((lead ^ k) * DK, DK), DK)
        target = pl.ds(k * DK, DK)
        for i, (hbm, ref) in enumerate(((wk_hbm, wk_ref), (wv_hbm, wv_ref))):
            copies.append(
                pltpu.make_async_copy(hbm.at[:, source], ref.at[:, target], sems.at[2 * k + i])
            )
    for copy in early + copies:
        copy.start()
    for copy in early:
        copy.wait()
    many = bias_ref.shape[1]
    row = lax.broadcasted_iota(jnp.int32, (2 * SUB, 2 * many), 0)
    col = lax.broadcasted_iota(jnp.int32, (2 * SUB, 2 * many), 1)
    k = row & (SUB - 1)
    wanted = first + (lead ^ k) + jnp.where(row >= SUB, many, 0)
    pick = jnp.where(jnp.logical_and(col == wanted, k < heads), 1.0, 0.0)
    both = jnp.concatenate([wb_ref[...], wd_ref[...]], axis=0)
    wg_ref[...] = dot(pick, both).astype(bf16)
    row = lax.broadcasted_iota(jnp.int32, (SUB, many), 0)
    col = lax.broadcasted_iota(jnp.int32, (SUB, many), 1)
    mine = col == first + (lead ^ row)
    bias = jnp.sum(jnp.where(mine, bias_ref[...], 0.0), axis=1, keepdims=True)
    rate = jnp.sum(jnp.where(mine, rate_ref[...], 0.0), axis=1, keepdims=True)
    lane = lax.broadcasted_iota(jnp.int32, (SUB, DK), 1)
    small_ref[...] = jnp.where(lane == 0, bias, jnp.where(lane == 1, rate, 0.0))
    seats = query_in.shape[1]
    place = lax.axis_index("sp") * seats
    row = lax.broadcasted_iota(jnp.int32, (seats, DK), 0)
    col = lax.broadcasted_iota(jnp.int32, (seats, DK), 1)
    query = dot(query_in[...], jnp.where(col == row + place, 1.0, 0.0))
    forget = forget_in[...]
    size = forget.shape[1]
    wide = lax.broadcasted_iota(jnp.int32, (SUB, size), 0)
    slim = lax.broadcasted_iota(jnp.int32, (SUB, DK), 0)
    forget_out = jnp.zeros((SUB, size), f32)
    query_out = jnp.zeros((SUB, DK), f32)
    for h in range(heads):
        forget_out = jnp.where((lead ^ wide) == h, forget[h : h + 1], forget_out)
        query_out = jnp.where((lead ^ slim) == h, query[h : h + 1], query_out)
    forget_ref[...] = forget_out
    query_ref[...] = query_out
    for copy in copies:
        copy.wait()


def chunk_kernel(heads, index, last, masks, prior, *refs):
    pieces = len(masks)
    piece_refs = refs[:pieces]
    wk_ref, wv_ref, wg_ref, small_ref, forget_ref = refs[pieces : pieces + 5]
    rest = refs[pieces + 5 :]
    sums = (None, None, None)
    if prior:
        sums, rest = tuple(ref[...] for ref in rest[:3]), rest[3:]
    if index > 0:
        state_ref, rest = rest[0], rest[1:]
    if last:
        query_ref, rest = rest[0], rest[1:]
    gates, key_acc, value_acc = project(masks, piece_refs, wk_ref, wv_ref, wg_ref, sums)
    size = key_acc.shape[0]
    bias, rate = small_ref[:, 0:1], small_ref[:, 1:2]
    forget = forget_ref[:, index * size : (index + 1) * size]
    beta_row = jax.nn.sigmoid(gates[0:SUB] + bias)
    log_row = forget - rate * jax.nn.softplus(gates[SUB : 2 * SUB])
    row = lax.broadcasted_iota(jnp.int32, (size, size), 0)
    col = lax.broadcasted_iota(jnp.int32, (size, size), 1)
    strict = row > col
    after = dot_ones(log_row, jnp.where(strict, 1.0, 0.0))
    keep = jnp.exp(after[:, 0:1] + log_row[:, 0:1])
    remain = jnp.exp(after)

    key_raw = key_acc.astype(bf16).astype(f32)
    value_raw = value_acc.astype(bf16)
    keys, lowers = [], []
    for h in range(heads):
        kw = key_raw[:, h * DK : (h + 1) * DK]
        ku = kw * lax.rsqrt(jnp.sum(kw * kw, axis=-1, keepdims=True) + norm_eps)
        keys.append(ku)
        lowers.append(jnp.where(strict, dot_nt(ku, ku), 0.0) * beta_row[h : h + 1, :])
    if index > 0:
        states = [state_ref[h] for h in range(heads)]
    else:
        kr = lax.broadcasted_iota(jnp.int32, (DK, DV + DK), 0)
        kc = lax.broadcasted_iota(jnp.int32, (DK, DV + DK), 1)
        states = [jnp.where(kc == kr + DV, 1.0, 0.0)] * heads
    rights, turned = [], []
    for h in range(heads):
        value = value_raw[:, h * DV : (h + 1) * DV]
        padded = jnp.concatenate([value, jnp.zeros((size, DK), bf16)], axis=1)
        seen = dot(keys[h], states[h]).astype(bf16)
        rights.append(jnp.concatenate([padded, seen], axis=0))
        turned.append(keys[h].T * beta_row[h : h + 1, :])
    fresh = []
    for h, inverse in enumerate(unit_inverses(lowers, size)):
        left = jnp.concatenate(
            [inverse * remain[h : h + 1, :], inverse * -keep[h : h + 1, :]], axis=1
        )
        fresh.append(dot(left, rights[h]))
    for h in range(heads):
        new = keep[h : h + 1, :] * states[h] + dot(turned[h], fresh[h])
        if last:
            rest[h][...] = passed_on(new, jnp.broadcast_to(query_ref[h : h + 1, :], (SUB, DK)))
        else:
            rest[-1][h] = new


def compose(pairs, product):
    while len(pairs) > 1:
        merged = []
        for early, late in zip(pairs[0::2], pairs[1::2]):
            new = product(late[:, DV:], early)
            merged.append(jnp.concatenate([new[:, :DV] + late[:, :DV], new[:, DV:]], axis=1))
        pairs, product = merged, dot3
    return pairs[0]


def pad_rows(x, rows):
    return jnp.concatenate([x, jnp.zeros((rows - x.shape[0], x.shape[1]), x.dtype)], axis=0)


def late_side(mask):
    return lax.rem(lax.div(lax.axis_index("sp"), jnp.int32(mask)), jnp.int32(2)) == 1


def finish(total, query, out):
    out[0][...] = total
    out[1][...] = query
    if len(out) == 2:
        return
    half = DK // 2
    through = dot3(query, total)
    a, b = total[:, DV:], total[:, :DV]
    high = late_side(lax.axis_size("sp") // 2)
    body = jnp.where(high, jnp.concatenate([a[:half], b[:half]], axis=0), b)
    ah, al = split(through[0:1, DV:])
    bh, bl = split(through[0:1, :DV])
    tail = [query[0:1]] + [x.astype(f32) for x in (ah, al, bh, bl)]
    tail = pad_rows(jnp.concatenate(tail, axis=0), 2 * SUB)
    out[2][0:DK, :] = body.astype(bf16)
    out[2][DK:, :] = tail.astype(bf16)


def passed_on(total, query):
    return jnp.concatenate([total[:, :DV], total[:, DV:], query, query], axis=0).astype(bf16)


def received(ref):
    total = jnp.concatenate([ref[:DK, :], ref[DK : 2 * DK, :]], axis=1)
    return total.astype(f32), ref[2 * DK :, :].astype(f32)[:SUB]


def compose_kernel(heads, final, *refs):
    own_ref, got = refs[0], refs[1:heads]
    out, scratch = refs[heads:-1], refs[-1]
    lead = lax.axis_index("sp") % heads
    scratch[lead], query = received(own_ref)
    for k in range(1, heads):
        scratch[lead ^ k], asked = received(got[k - 1])
        query = query + asked
    total = compose([scratch[i] for i in range(heads)], dot)
    if final:
        finish(total, query, out)
    else:
        out[0][...], out[1][...] = total, query
        out[2][...] = passed_on(total, query)


def merge_kernel(mask, final, own_ref, query_ref, got_ref, *out):
    high = late_side(mask)
    own, (got, asked) = own_ref[...], received(got_ref)
    query = query_ref[...] + asked
    early, late = jnp.where(high, got, own), jnp.where(high, own, got)
    total = compose([early, late], dot3)
    if final:
        finish(total, query, out)
    else:
        out[0][...], out[1][...] = total, query
        out[2][...] = passed_on(total, query)


def rows_kernel(heads, groups, rows, own_ref, query_ref, *refs):
    if groups > 1:
        got_ref, refs = refs[0], refs[1:]
    scratch = refs[-1]
    own, query = own_ref[...], query_ref[...]
    half = DK // 2
    place = lax.axis_index("sp")
    if groups > 1:
        high = late_side(lax.axis_size("sp") // 2)
        got = got_ref[...].astype(f32)
        a, b = own[:, DV:], own[:, :DV]
        early = jnp.where(high, got[:DK], b)
        late_a = jnp.where(high, a[half:], got[:half])
        late_b = jnp.where(high, b[half:], got[half:DK])
        tail = got[DK:]
        cross = dot3(jnp.broadcast_to(tail[0:1], (SUB, DK)), own)[0:1]
        through_a = jnp.where(high, cross[:, DV:], tail[1:2] + tail[2:3])
        through_b = jnp.where(high, cross[:, :DV], tail[3:4] + tail[4:5])
        both = dot3(pad_rows(jnp.concatenate([late_a, through_a], axis=0), half + SUB), early)
        state = both[:half] + late_b
        asked = jnp.where(high, query[:, half:], query[:, :half])
        read = dot3(asked, state)[0:1] + (both[half : half + 1] + through_b)
    else:
        state = own[:, :DV]
        read = dot3(query, state)[0:1]
    members = state.shape[0] // rows
    for i in range(members):
        scratch[i] = state[i * rows : (i + 1) * rows]
    place = place % members
    rh, rl = split(read)
    tail = pad_rows(jnp.concatenate([rh.astype(f32), rl.astype(f32)], axis=0), 16)
    for k in range(heads):
        body = scratch[place ^ k]
        refs[k][...] = jnp.concatenate([body, tail], axis=0).astype(bf16)


def final_kernel(heads, rows, gain_ref, *refs):
    lead = lax.axis_index("sp") % heads
    state_ref, read_ref, scratch = refs[heads:]
    for k in range(heads):
        part = refs[k][...]
        state_ref[lead ^ k] = part[:rows]
        wide = part[rows : rows + 2].astype(f32)
        scratch[lead ^ k] = jnp.broadcast_to(wide[0:1] + wide[1:2], (SUB, DV))
    raw = jnp.concatenate([scratch[h][0:1] for h in range(heads)], axis=0)
    norm = lax.rsqrt(jnp.mean(raw * raw, axis=-1, keepdims=True) + norm_eps)
    read_ref[...] = raw * norm * gain_ref[...].astype(f32)


def shape(dims, dtype=f32):
    return jax.ShapeDtypeStruct(dims, dtype)


vmem = pl.BlockSpec(memory_space=pltpu.VMEM)


def call(body, arrays, outs, scratch=(), mib=8, flops=0):
    return pl.pallas_call(
        body,
        out_shape=outs,
        in_specs=[vmem] * len(arrays),
        out_specs=jax.tree.map(lambda _: vmem, outs),
        scratch_shapes=list(scratch),
        compiler_params=pltpu.CompilerParams(vmem_limit_bytes=mib * 1024 * 1024),
        cost_estimate=pl.CostEstimate(flops=flops, bytes_accessed=0, transcendentals=0)
        if flops
        else None,
    )(*arrays)


def per_device(
    tokens,
    w_key,
    w_value,
    w_beta,
    w_decay,
    beta_bias,
    decay_rate,
    forgetting_increment,
    new_query,
    read_gain,
):
    heads = w_key.shape[1] // DK
    length, width = tokens.shape
    count = lax.axis_size("sp")
    ranks = lax.axis_size("tp")
    groups = count // heads
    rows = DK // count
    chunk = min(CHUNK, length)
    chunks = length // chunk

    owns = [tokens[:chunk]]
    later = lax.optimization_barrier(tokens)
    owns += [later[c * chunk : (c + 1) * chunk] for c in range(1, chunks)]
    gathered = []
    for c in range(chunks):
        found = [(0, owns[c])]
        for hop in range(1, ranks // 2):
            found.append((2 * hop, swap(owns[c], "tp", 2 * hop)))
        found.append((1, swap(owns[c], "tp", 1)))
        found += [(m ^ 1, swap(x, "tp", 1)) for m, x in found[1:-1]]
        gathered.append(found)

    plain = [
        pltpu.with_memory_space_constraint(x, pltpu.HBM)
        for x in (
            w_key,
            w_value,
            w_beta.T,
            w_decay.T,
            beta_bias[None],
            decay_rate[None],
            forgetting_increment,
            new_query,
        )
    ]
    w_key, w_value, gate_weights, small, forget, query = pl.pallas_call(
        functools.partial(prepare_kernel, heads),
        out_shape=[
            shape(w_key.shape, bf16),
            shape(w_value.shape, bf16),
            shape((2 * SUB, w_beta.shape[0]), bf16),
            shape((SUB, DK)),
            shape((SUB, length)),
            shape((SUB, DK)),
        ],
        in_specs=[pl.BlockSpec(memory_space=pltpu.HBM)] * 8,
        out_specs=[vmem] * 6,
        scratch_shapes=[pltpu.VMEM(x.shape, x.dtype) for x in plain[2:]]
        + [pltpu.SemaphoreType.DMA((2 * heads + 6,))],
        compiler_params=pltpu.CompilerParams(vmem_limit_bytes=24 * 1024 * 1024),
    )(*plain)

    state = None
    flops = 2 * chunk * width * ranks * (2 * heads * DK + DK) + heads * 24 * 2 * chunk * chunk * DK
    weights = [w_key, w_value, gate_weights]
    sums_shape = [shape((2 * SUB, chunk)), shape((chunk, heads * DK)), shape((chunk, heads * DV))]

    def part(found, sums):
        return call(
            functools.partial(part_kernel, tuple(m for m, _ in found), len(sums) > 0),
            [x for _, x in found] + weights + sums,
            sums_shape,
            mib=16,
            flops=2 * chunk * width * len(found) * (2 * heads * DK + DK),
        )

    for c in range(chunks):
        found = gathered[c]
        last = c == chunks - 1
        sums = []
        if c > 0:
            here = [f for f in found if f[0] < 2]
            found = [f for f in found if f[0] >= 2]
            sums = list(part(here, sums))
        if last and len(found) > 1:
            near = [f for f in found if f[0] % 2 == 0]
            found = [f for f in found if f[0] % 2 == 1]
            sums = list(part(near, sums))
        arrays = [x for _, x in found] + weights + [small, forget] + sums
        if c > 0:
            arrays.append(state)
        outs = [shape((heads, DK, DV + DK))]
        if last:
            arrays.append(query)
            outs = [shape((DK + DV + 2 * SUB, DK), bf16)] * heads
        result = call(
            functools.partial(
                chunk_kernel, heads, c, last, tuple(m for m, _ in found), len(sums) > 0
            ),
            arrays,
            outs,
            mib=28,
            flops=flops,
        )
        state = result[-1]
    maps = result

    got = {}
    for k in reversed(range(1, heads)):
        got[k] = swap(maps[k], "sp", k)
    done = [shape((DK, DV + DK)), shape((SUB, DK))]
    open_ended = done + [shape((DK + DV + 2 * SUB, DK), bf16)]
    if groups > 1:
        done.append(shape((DK + 2 * SUB, DV), bf16))
    result = call(
        functools.partial(compose_kernel, heads, groups <= 2),
        [maps[0]] + [got[k] for k in range(1, heads)],
        done if groups <= 2 else open_ended,
        [pltpu.VMEM((heads, DK, DV + DK), f32)],
    )
    mask = heads
    while 2 * mask < count:
        final = 4 * mask == count
        result = call(
            functools.partial(merge_kernel, mask, final),
            [result[0], result[1], swap(result[2], "sp", mask)],
            done if final else open_ended,
        )
        mask *= 2
    arrays = list(result[:2])
    if groups > 1:
        arrays.append(swap(result[2], "sp", count // 2))
    members = count // 2 if groups > 1 else count
    parts = call(
        functools.partial(rows_kernel, heads, groups, rows),
        arrays,
        [shape((rows + 16, DV), bf16)] * heads,
        [pltpu.VMEM((members, rows, DV), f32)],
    )
    moved = {}
    for k in reversed(range(1, heads)):
        moved[k] = swap(parts[k], "sp", k)
    own_rows, first_read = call(
        functools.partial(final_kernel, heads, rows),
        [read_gain[None], parts[0]] + [moved[k] for k in range(1, heads)],
        [shape((heads, rows, DV), bf16), shape((heads, DV))],
        [pltpu.VMEM((heads, SUB, DV), f32)],
    )
    return (own_rows, first_read)


def solution(mesh):
    return jax.shard_map(
        per_device,
        mesh=mesh,
        in_specs=(
            P("sp", "tp"),
            P(None, "tp"),
            P(None, "tp"),
            P(),
            P(),
            P(),
            P(),
            P("tp", "sp"),
            P("tp", "sp"),
            P(),
        ),
        out_specs=(P("tp", "sp", None), P("tp", None)),
        check_vma=False,
    )
```

```python
import functools

import jax
import jax.numpy as jnp
from jax import lax
from jax.experimental import pallas as pl
from jax.experimental.pallas import tpu as pltpu
from jax.sharding import PartitionSpec as P


DK = 128
DV = 128
CHUNK = 128
SUB = 8

norm_eps = 1e-06
bf16 = jnp.bfloat16
f32 = jnp.float32


def flip(axis, mask):
    return [(i, i ^ mask) for i in range(lax.axis_size(axis))]


def swap(x, axis, mask):
    return lax.ppermute(x, axis, flip(axis, mask))


def dot(left, right):
    return jnp.dot(left.astype(bf16), right.astype(bf16), preferred_element_type=f32)


def split(x):
    high = x.astype(bf16)
    return high, (x - high.astype(f32)).astype(bf16)


def dot3(left, right):
    lh, ll = split(left)
    rh, rl = split(right)
    return dot(lh, rh) + (dot(lh, rl) + dot(ll, rh))


def dot_ones(left, ones):
    high, rest = split(left)
    mid = rest
    low = (left - high.astype(f32) - mid.astype(f32)).astype(bf16)
    n = left.shape[0]
    parts = jnp.concatenate([high.astype(f32), mid.astype(f32), low.astype(f32)], axis=0)
    out = dot(parts, ones)
    return out[:n] + out[n : 2 * n] + out[2 * n :]


def dot_nt(left, right):
    return lax.dot_general(
        left.astype(bf16), right.astype(bf16), (((1,), (1,)), ((), ())), preferred_element_type=f32
    )


def unit_inverses(lowers, size):
    row = lax.broadcasted_iota(jnp.int32, (size, size), 0)
    col = lax.broadcasted_iota(jnp.int32, (size, size), 1)
    width = min(16, size)
    near = (row // width) == (col // width)
    inner = [jnp.where(near, low, 0.0) for low in lowers]
    results = [jnp.where(row == col, 1.0, 0.0) - low for low in inner]
    powers = inner
    covered = 2
    while covered < width:
        powers = [dot(p, p) for p in powers]
        results = [r + dot(r, p) for r, p in zip(results, powers)]
        covered *= 2
    if width == size:
        return results
    powers = [dot(r, jnp.where(near, 0.0, low)) for r, low in zip(results, lowers)]
    results = [r - dot(p, r) for r, p in zip(results, powers)]
    covered = 2
    while covered * width < size:
        powers = [dot(p, p) for p in powers]
        results = [r + dot(p, r) for r, p in zip(results, powers)]
        covered *= 2
    return results


def project(masks, piece_refs, wk_ref, wv_ref, wg_ref, sums):
    rank = lax.axis_index("tp")
    gates, keys, values = sums
    placed = []
    for m, ref in zip(masks, piece_refs):
        width = ref.shape[1]
        placed.append((pl.ds(pl.multiple_of((rank ^ m) * width, width), width), ref))
    for rows, ref in placed:
        g = dot_nt(wg_ref[:, rows], ref[...])
        gates = g if gates is None else gates + g
    for rows, ref in placed:
        k = jnp.dot(ref[...], wk_ref[rows, :], preferred_element_type=f32)
        keys = k if keys is None else keys + k
    for rows, ref in placed:
        v = jnp.dot(ref[...], wv_ref[rows, :], preferred_element_type=f32)
        values = v if values is None else values + v
    return gates, keys, values


def part_kernel(masks, prior, *refs):
    pieces = len(masks)
    weights, rest = refs[pieces : pieces + 3], refs[pieces + 3 :]
    sums = (None, None, None)
    if prior:
        sums, rest = tuple(ref[...] for ref in rest[:3]), rest[3:]
    for ref, x in zip(rest, project(masks, refs[:pieces], *weights, sums)):
        ref[...] = x


def rows_copy_kernel(tokens_hbm, out_ref, sem):
    copy = pltpu.make_async_copy(tokens_hbm.at[: out_ref.shape[0]], out_ref, sem)
    copy.start()
    copy.wait()


def prepare_kernel(heads, *refs):
    wk_hbm, wv_hbm = refs[:2]
    wk_ref, wv_ref, wg_ref, small_ref, forget_ref, query_ref = refs[8:14]
    few, sems = refs[14:20], refs[20]
    wb_ref, wd_ref, bias_ref, rate_ref, forget_in, query_in = few
    lead = lax.axis_index("sp") % heads
    first = lax.axis_index("tp") * heads
    early = [
        pltpu.make_async_copy(hbm, ref, sems.at[2 * heads + i])
        for i, (hbm, ref) in enumerate(zip(refs[2:8], few))
    ]
    copies = []
    for k in range(heads):
        source = pl.ds(pl.multiple_of((lead ^ k) * DK, DK), DK)
        target = pl.ds(k * DK, DK)
        for i, (hbm, ref) in enumerate(((wk_hbm, wk_ref), (wv_hbm, wv_ref))):
            copies.append(
                pltpu.make_async_copy(hbm.at[:, source], ref.at[:, target], sems.at[2 * k + i])
            )
    for copy in early + copies:
        copy.start()
    for copy in early:
        copy.wait()
    many = bias_ref.shape[1]
    row = lax.broadcasted_iota(jnp.int32, (2 * SUB, 2 * many), 0)
    col = lax.broadcasted_iota(jnp.int32, (2 * SUB, 2 * many), 1)
    k = row & (SUB - 1)
    wanted = first + (lead ^ k) + jnp.where(row >= SUB, many, 0)
    pick = jnp.where(jnp.logical_and(col == wanted, k < heads), 1.0, 0.0)
    both = jnp.concatenate([wb_ref[...], wd_ref[...]], axis=0)
    wg_ref[...] = dot(pick, both).astype(bf16)
    row = lax.broadcasted_iota(jnp.int32, (SUB, many), 0)
    col = lax.broadcasted_iota(jnp.int32, (SUB, many), 1)
    mine = col == first + (lead ^ row)
    bias = jnp.sum(jnp.where(mine, bias_ref[...], 0.0), axis=1, keepdims=True)
    rate = jnp.sum(jnp.where(mine, rate_ref[...], 0.0), axis=1, keepdims=True)
    lane = lax.broadcasted_iota(jnp.int32, (SUB, DK), 1)
    small_ref[...] = jnp.where(lane == 0, bias, jnp.where(lane == 1, rate, 0.0))
    seats = query_in.shape[1]
    place = lax.axis_index("sp") * seats
    row = lax.broadcasted_iota(jnp.int32, (seats, DK), 0)
    col = lax.broadcasted_iota(jnp.int32, (seats, DK), 1)
    query = dot(query_in[...], jnp.where(col == row + place, 1.0, 0.0))
    forget = forget_in[...]
    size = forget.shape[1]
    wide = lax.broadcasted_iota(jnp.int32, (SUB, size), 0)
    slim = lax.broadcasted_iota(jnp.int32, (SUB, DK), 0)
    forget_out = jnp.zeros((SUB, size), f32)
    query_out = jnp.zeros((SUB, DK), f32)
    for h in range(heads):
        forget_out = jnp.where((lead ^ wide) == h, forget[h : h + 1], forget_out)
        query_out = jnp.where((lead ^ slim) == h, query[h : h + 1], query_out)
    forget_ref[...] = forget_out
    query_ref[...] = query_out
    for copy in copies:
        copy.wait()


def chunk_kernel(heads, index, last, masks, prior, *refs):
    pieces = len(masks)
    piece_refs = refs[:pieces]
    wk_ref, wv_ref, wg_ref, small_ref, forget_ref = refs[pieces : pieces + 5]
    rest = refs[pieces + 5 :]
    sums = (None, None, None)
    if prior:
        sums, rest = tuple(ref[...] for ref in rest[:3]), rest[3:]
    if index > 0:
        state_ref, rest = rest[0], rest[1:]
    if last:
        query_ref, rest = rest[0], rest[1:]
    gates, key_acc, value_acc = project(masks, piece_refs, wk_ref, wv_ref, wg_ref, sums)
    size = key_acc.shape[0]
    bias, rate = small_ref[:, 0:1], small_ref[:, 1:2]
    forget = forget_ref[:, index * size : (index + 1) * size]
    beta_row = jax.nn.sigmoid(gates[0:SUB] + bias)
    log_row = forget - rate * jax.nn.softplus(gates[SUB : 2 * SUB])
    row = lax.broadcasted_iota(jnp.int32, (size, size), 0)
    col = lax.broadcasted_iota(jnp.int32, (size, size), 1)
    strict = row > col
    after = dot_ones(log_row, jnp.where(strict, 1.0, 0.0))
    keep = jnp.exp(after[:, 0:1] + log_row[:, 0:1])
    remain = jnp.exp(after)

    key_raw = key_acc.astype(bf16).astype(f32)
    value_raw = value_acc.astype(bf16)
    keys, lowers = [], []
    for h in range(heads):
        kw = key_raw[:, h * DK : (h + 1) * DK]
        ku = kw * lax.rsqrt(jnp.sum(kw * kw, axis=-1, keepdims=True) + norm_eps)
        keys.append(ku)
        lowers.append(jnp.where(strict, dot_nt(ku, ku), 0.0) * beta_row[h : h + 1, :])
    if index > 0:
        states = [state_ref[h] for h in range(heads)]
    else:
        kr = lax.broadcasted_iota(jnp.int32, (DK, DV + DK), 0)
        kc = lax.broadcasted_iota(jnp.int32, (DK, DV + DK), 1)
        states = [jnp.where(kc == kr + DV, 1.0, 0.0)] * heads
    rights, turned = [], []
    for h in range(heads):
        value = value_raw[:, h * DV : (h + 1) * DV]
        padded = jnp.concatenate([value, jnp.zeros((size, DK), bf16)], axis=1)
        seen = dot(keys[h], states[h]).astype(bf16)
        rights.append(jnp.concatenate([padded, seen], axis=0))
        turned.append(keys[h].T * beta_row[h : h + 1, :])
    fresh = []
    for h, inverse in enumerate(unit_inverses(lowers, size)):
        left = jnp.concatenate(
            [inverse * remain[h : h + 1, :], inverse * -keep[h : h + 1, :]], axis=1
        )
        fresh.append(dot(left, rights[h]))
    for h in range(heads):
        new = keep[h : h + 1, :] * states[h] + dot(turned[h], fresh[h])
        if last:
            rest[h][...] = passed_on(new, jnp.broadcast_to(query_ref[h : h + 1, :], (SUB, DK)))
        else:
            rest[-1][h] = new


def compose(pairs, product):
    while len(pairs) > 1:
        merged = []
        for early, late in zip(pairs[0::2], pairs[1::2]):
            new = product(late[:, DV:], early)
            merged.append(jnp.concatenate([new[:, :DV] + late[:, :DV], new[:, DV:]], axis=1))
        pairs, product = merged, dot3
    return pairs[0]


def pad_rows(x, rows):
    return jnp.concatenate([x, jnp.zeros((rows - x.shape[0], x.shape[1]), x.dtype)], axis=0)


def late_side(mask):
    return lax.rem(lax.div(lax.axis_index("sp"), jnp.int32(mask)), jnp.int32(2)) == 1


def finish(total, query, out):
    out[0][...] = total
    out[1][...] = query
    if len(out) == 2:
        return
    half = DK // 2
    through = dot3(query, total)
    a, b = total[:, DV:], total[:, :DV]
    high = late_side(lax.axis_size("sp") // 2)
    body = jnp.where(high, jnp.concatenate([a[:half], b[:half]], axis=0), b)
    ah, al = split(through[0:1, DV:])
    bh, bl = split(through[0:1, :DV])
    tail = [query[0:1]] + [x.astype(f32) for x in (ah, al, bh, bl)]
    tail = pad_rows(jnp.concatenate(tail, axis=0), 2 * SUB)
    out[2][0:DK, :] = body.astype(bf16)
    out[2][DK:, :] = tail.astype(bf16)


def passed_on(total, query):
    return jnp.concatenate([total[:, :DV], total[:, DV:], query, query], axis=0).astype(bf16)


def received(ref):
    total = jnp.concatenate([ref[:DK, :], ref[DK : 2 * DK, :]], axis=1)
    return total.astype(f32), ref[2 * DK :, :].astype(f32)[:SUB]


def compose_kernel(heads, final, *refs):
    own_ref, got = refs[0], refs[1:heads]
    out, scratch = refs[heads:-1], refs[-1]
    lead = lax.axis_index("sp") % heads
    scratch[lead], query = received(own_ref)
    for k in range(1, heads):
        scratch[lead ^ k], asked = received(got[k - 1])
        query = query + asked
    total = compose([scratch[i] for i in range(heads)], dot)
    if final:
        finish(total, query, out)
    else:
        out[0][...], out[1][...] = total, query
        out[2][...] = passed_on(total, query)


def merge_kernel(mask, final, own_ref, query_ref, got_ref, *out):
    high = late_side(mask)
    own, (got, asked) = own_ref[...], received(got_ref)
    query = query_ref[...] + asked
    early, late = jnp.where(high, got, own), jnp.where(high, own, got)
    total = compose([early, late], dot3)
    if final:
        finish(total, query, out)
    else:
        out[0][...], out[1][...] = total, query
        out[2][...] = passed_on(total, query)


def rows_kernel(heads, groups, rows, own_ref, query_ref, *refs):
    if groups > 1:
        got_ref, refs = refs[0], refs[1:]
    scratch = refs[-1]
    own, query = own_ref[...], query_ref[...]
    half = DK // 2
    place = lax.axis_index("sp")
    if groups > 1:
        high = late_side(lax.axis_size("sp") // 2)
        got = got_ref[...].astype(f32)
        a, b = own[:, DV:], own[:, :DV]
        early = jnp.where(high, got[:DK], b)
        late_a = jnp.where(high, a[half:], got[:half])
        late_b = jnp.where(high, b[half:], got[half:DK])
        tail = got[DK:]
        cross = dot3(jnp.broadcast_to(tail[0:1], (SUB, DK)), own)[0:1]
        through_a = jnp.where(high, cross[:, DV:], tail[1:2] + tail[2:3])
        through_b = jnp.where(high, cross[:, :DV], tail[3:4] + tail[4:5])
        both = dot3(pad_rows(jnp.concatenate([late_a, through_a], axis=0), half + SUB), early)
        state = both[:half] + late_b
        asked = jnp.where(high, query[:, half:], query[:, :half])
        read = dot3(asked, state)[0:1] + (both[half : half + 1] + through_b)
    else:
        state = own[:, :DV]
        read = dot3(query, state)[0:1]
    members = state.shape[0] // rows
    for i in range(members):
        scratch[i] = state[i * rows : (i + 1) * rows]
    place = place % members
    rh, rl = split(read)
    tail = pad_rows(jnp.concatenate([rh.astype(f32), rl.astype(f32)], axis=0), 16)
    for k in range(heads):
        body = scratch[place ^ k]
        refs[k][...] = jnp.concatenate([body, tail], axis=0).astype(bf16)


def final_kernel(heads, rows, gain_ref, *refs):
    lead = lax.axis_index("sp") % heads
    state_ref, read_ref, scratch = refs[heads:]
    for k in range(heads):
        part = refs[k][...]
        state_ref[lead ^ k] = part[:rows]
        wide = part[rows : rows + 2].astype(f32)
        scratch[lead ^ k] = jnp.broadcast_to(wide[0:1] + wide[1:2], (SUB, DV))
    raw = jnp.concatenate([scratch[h][0:1] for h in range(heads)], axis=0)
    norm = lax.rsqrt(jnp.mean(raw * raw, axis=-1, keepdims=True) + norm_eps)
    read_ref[...] = raw * norm * gain_ref[...].astype(f32)


def shape(dims, dtype=f32):
    return jax.ShapeDtypeStruct(dims, dtype)


vmem = pl.BlockSpec(memory_space=pltpu.VMEM)


def call(body, arrays, outs, scratch=(), mib=8, flops=0):
    return pl.pallas_call(
        body,
        out_shape=outs,
        in_specs=[vmem] * len(arrays),
        out_specs=jax.tree.map(lambda _: vmem, outs),
        scratch_shapes=list(scratch),
        compiler_params=pltpu.CompilerParams(vmem_limit_bytes=mib * 1024 * 1024),
        cost_estimate=pl.CostEstimate(flops=flops, bytes_accessed=0, transcendentals=0)
        if flops
        else None,
    )(*arrays)


def per_device(
    tokens,
    w_key,
    w_value,
    w_beta,
    w_decay,
    beta_bias,
    decay_rate,
    forgetting_increment,
    new_query,
    read_gain,
):
    heads = w_key.shape[1] // DK
    length, width = tokens.shape
    count = lax.axis_size("sp")
    ranks = lax.axis_size("tp")
    groups = count // heads
    rows = DK // count
    chunk = min(CHUNK, length)
    chunks = length // chunk

    first_rows = pl.pallas_call(
        rows_copy_kernel,
        out_shape=shape((chunk, width), bf16),
        in_specs=[pl.BlockSpec(memory_space=pltpu.HBM)],
        out_specs=vmem,
        scratch_shapes=[pltpu.SemaphoreType.DMA(())],
        compiler_params=pltpu.CompilerParams(vmem_limit_bytes=4 * 1024 * 1024),
    )(pltpu.with_memory_space_constraint(tokens, pltpu.HBM))
    owns = [first_rows] + [tokens[c * chunk : (c + 1) * chunk] for c in range(1, chunks)]
    gathered = []
    for c in range(chunks):
        found = [(0, owns[c])]
        for hop in range(1, ranks // 2):
            found.append((2 * hop, swap(owns[c], "tp", 2 * hop)))
        found.append((1, swap(owns[c], "tp", 1)))
        found += [(m ^ 1, swap(x, "tp", 1)) for m, x in found[1:-1]]
        gathered.append(found)

    plain = [
        pltpu.with_memory_space_constraint(x, pltpu.HBM)
        for x in (
            w_key,
            w_value,
            w_beta.T,
            w_decay.T,
            beta_bias[None],
            decay_rate[None],
            forgetting_increment,
            new_query,
        )
    ]
    w_key, w_value, gate_weights, small, forget, query = pl.pallas_call(
        functools.partial(prepare_kernel, heads),
        out_shape=[
            shape(w_key.shape, bf16),
            shape(w_value.shape, bf16),
            shape((2 * SUB, w_beta.shape[0]), bf16),
            shape((SUB, DK)),
            shape((SUB, length)),
            shape((SUB, DK)),
        ],
        in_specs=[pl.BlockSpec(memory_space=pltpu.HBM)] * 8,
        out_specs=[vmem] * 6,
        scratch_shapes=[pltpu.VMEM(x.shape, x.dtype) for x in plain[2:]]
        + [pltpu.SemaphoreType.DMA((2 * heads + 6,))],
        compiler_params=pltpu.CompilerParams(vmem_limit_bytes=24 * 1024 * 1024),
    )(*plain)

    state = None
    flops = 2 * chunk * width * ranks * (2 * heads * DK + DK) + heads * 24 * 2 * chunk * chunk * DK
    weights = [w_key, w_value, gate_weights]
    sums_shape = [shape((2 * SUB, chunk)), shape((chunk, heads * DK)), shape((chunk, heads * DV))]

    def part(found, sums):
        return call(
            functools.partial(part_kernel, tuple(m for m, _ in found), len(sums) > 0),
            [x for _, x in found] + weights + sums,
            sums_shape,
            mib=16,
            flops=2 * chunk * width * len(found) * (2 * heads * DK + DK),
        )

    for c in range(chunks):
        found = gathered[c]
        last = c == chunks - 1
        sums = []
        if c > 0:
            here = [f for f in found if f[0] < 2]
            found = [f for f in found if f[0] >= 2]
            sums = list(part(here, sums))
        if last and len(found) > 1:
            near = [f for f in found if f[0] % 2 == 0]
            found = [f for f in found if f[0] % 2 == 1]
            sums = list(part(near, sums))
        arrays = [x for _, x in found] + weights + [small, forget] + sums
        if c > 0:
            arrays.append(state)
        outs = [shape((heads, DK, DV + DK))]
        if last:
            arrays.append(query)
            outs = [shape((DK + DV + 2 * SUB, DK), bf16)] * heads
        result = call(
            functools.partial(
                chunk_kernel, heads, c, last, tuple(m for m, _ in found), len(sums) > 0
            ),
            arrays,
            outs,
            mib=28,
            flops=flops,
        )
        state = result[-1]
    maps = result

    got = {}
    for k in reversed(range(1, heads)):
        got[k] = swap(maps[k], "sp", k)
    done = [shape((DK, DV + DK)), shape((SUB, DK))]
    open_ended = done + [shape((DK + DV + 2 * SUB, DK), bf16)]
    if groups > 1:
        done.append(shape((DK + 2 * SUB, DV), bf16))
    result = call(
        functools.partial(compose_kernel, heads, groups <= 2),
        [maps[0]] + [got[k] for k in range(1, heads)],
        done if groups <= 2 else open_ended,
        [pltpu.VMEM((heads, DK, DV + DK), f32)],
    )
    mask = heads
    while 2 * mask < count:
        final = 4 * mask == count
        result = call(
            functools.partial(merge_kernel, mask, final),
            [result[0], result[1], swap(result[2], "sp", mask)],
            done if final else open_ended,
        )
        mask *= 2
    arrays = list(result[:2])
    if groups > 1:
        arrays.append(swap(result[2], "sp", count // 2))
    members = count // 2 if groups > 1 else count
    parts = call(
        functools.partial(rows_kernel, heads, groups, rows),
        arrays,
        [shape((rows + 16, DV), bf16)] * heads,
        [pltpu.VMEM((members, rows, DV), f32)],
    )
    moved = {}
    for k in reversed(range(1, heads)):
        moved[k] = swap(parts[k], "sp", k)
    own_rows, first_read = call(
        functools.partial(final_kernel, heads, rows),
        [read_gain[None], parts[0]] + [moved[k] for k in range(1, heads)],
        [shape((heads, rows, DV), bf16), shape((heads, DV))],
        [pltpu.VMEM((heads, SUB, DV), f32)],
    )
    return (own_rows, first_read)


def solution(mesh):
    return jax.shard_map(
        per_device,
        mesh=mesh,
        in_specs=(
            P("sp", "tp"),
            P(None, "tp"),
            P(None, "tp"),
            P(),
            P(),
            P(),
            P(),
            P("tp", "sp"),
            P("tp", "sp"),
            P(),
        ),
        out_specs=(P("tp", "sp", None), P("tp", None)),
        check_vma=False,
    )
```

```python
import functools

import jax
import jax.numpy as jnp
from jax import lax
from jax.experimental import pallas as pl
from jax.experimental.pallas import tpu as pltpu
from jax.sharding import PartitionSpec as P


DK = 128
DV = 128
CHUNK = 128
SUB = 8

norm_eps = 1e-06
bf16 = jnp.bfloat16
f32 = jnp.float32


def flip(axis, mask):
    return [(i, i ^ mask) for i in range(lax.axis_size(axis))]


def swap(x, axis, mask):
    return lax.ppermute(x, axis, flip(axis, mask))


def dot(left, right):
    return jnp.dot(left.astype(bf16), right.astype(bf16), preferred_element_type=f32)


def split(x):
    high = x.astype(bf16)
    return high, (x - high.astype(f32)).astype(bf16)


def dot3(left, right):
    lh, ll = split(left)
    rh, rl = split(right)
    return dot(lh, rh) + (dot(lh, rl) + dot(ll, rh))


def dot_ones(left, ones):
    high, rest = split(left)
    mid = rest
    low = (left - high.astype(f32) - mid.astype(f32)).astype(bf16)
    n = left.shape[0]
    parts = jnp.concatenate([high.astype(f32), mid.astype(f32), low.astype(f32)], axis=0)
    out = dot(parts, ones)
    return out[:n] + out[n : 2 * n] + out[2 * n :]


def dot_nt(left, right):
    return lax.dot_general(
        left.astype(bf16), right.astype(bf16), (((1,), (1,)), ((), ())), preferred_element_type=f32
    )


def unit_inverses(lowers, size):
    row = lax.broadcasted_iota(jnp.int32, (size, size), 0)
    col = lax.broadcasted_iota(jnp.int32, (size, size), 1)
    width = min(16, size)
    near = (row // width) == (col // width)
    inner = [jnp.where(near, low, 0.0) for low in lowers]
    results = [jnp.where(row == col, 1.0, 0.0) - low for low in inner]
    powers = inner
    covered = 2
    while covered < width:
        powers = [dot(p, p) for p in powers]
        results = [r + dot(r, p) for r, p in zip(results, powers)]
        covered *= 2
    if width == size:
        return results
    powers = [dot(r, jnp.where(near, 0.0, low)) for r, low in zip(results, lowers)]
    results = [r - dot(p, r) for r, p in zip(results, powers)]
    covered = 2
    while covered * width < size:
        powers = [dot(p, p) for p in powers]
        results = [r + dot(p, r) for r, p in zip(results, powers)]
        covered *= 2
    return results


def project(masks, piece_refs, wk_ref, wv_ref, wg_ref, sums):
    rank = lax.axis_index("tp")
    gates, keys, values = sums
    placed = []
    for m, ref in zip(masks, piece_refs):
        width = ref.shape[1]
        placed.append((pl.ds(pl.multiple_of((rank ^ m) * width, width), width), ref))
    for rows, ref in placed:
        g = dot_nt(wg_ref[:, rows], ref[...])
        gates = g if gates is None else gates + g
    for rows, ref in placed:
        k = jnp.dot(ref[...], wk_ref[rows, :], preferred_element_type=f32)
        keys = k if keys is None else keys + k
    for rows, ref in placed:
        v = jnp.dot(ref[...], wv_ref[rows, :], preferred_element_type=f32)
        values = v if values is None else values + v
    return gates, keys, values


def part_kernel(masks, prior, *refs):
    pieces = len(masks)
    weights, rest = refs[pieces : pieces + 3], refs[pieces + 3 :]
    sums = (None, None, None)
    if prior:
        sums, rest = tuple(ref[...] for ref in rest[:3]), rest[3:]
    for ref, x in zip(rest, project(masks, refs[:pieces], *weights, sums)):
        ref[...] = x


def prepare_kernel(heads, *refs):
    wk_hbm, wv_hbm = refs[:2]
    wk_ref, wv_ref, wg_ref, small_ref, forget_ref, query_ref = refs[8:14]
    few, sems = refs[14:20], refs[20]
    wb_ref, wd_ref, bias_ref, rate_ref, forget_in, query_in = few
    lead = lax.axis_index("sp") % heads
    first = lax.axis_index("tp") * heads
    early = [
        pltpu.make_async_copy(hbm, ref, sems.at[2 * heads + i])
        for i, (hbm, ref) in enumerate(zip(refs[2:8], few))
    ]
    copies = []
    for k in range(heads):
        source = pl.ds(pl.multiple_of((lead ^ k) * DK, DK), DK)
        target = pl.ds(k * DK, DK)
        for i, (hbm, ref) in enumerate(((wk_hbm, wk_ref), (wv_hbm, wv_ref))):
            copies.append(
                pltpu.make_async_copy(hbm.at[:, source], ref.at[:, target], sems.at[2 * k + i])
            )
    for copy in early + copies:
        copy.start()
    for copy in early:
        copy.wait()
    many = bias_ref.shape[1]
    row = lax.broadcasted_iota(jnp.int32, (2 * SUB, 2 * many), 0)
    col = lax.broadcasted_iota(jnp.int32, (2 * SUB, 2 * many), 1)
    k = row & (SUB - 1)
    wanted = first + (lead ^ k) + jnp.where(row >= SUB, many, 0)
    pick = jnp.where(jnp.logical_and(col == wanted, k < heads), 1.0, 0.0)
    both = jnp.concatenate([wb_ref[...], wd_ref[...]], axis=0)
    wg_ref[...] = dot(pick, both).astype(bf16)
    row = lax.broadcasted_iota(jnp.int32, (SUB, many), 0)
    col = lax.broadcasted_iota(jnp.int32, (SUB, many), 1)
    mine = col == first + (lead ^ row)
    bias = jnp.sum(jnp.where(mine, bias_ref[...], 0.0), axis=1, keepdims=True)
    rate = jnp.sum(jnp.where(mine, rate_ref[...], 0.0), axis=1, keepdims=True)
    lane = lax.broadcasted_iota(jnp.int32, (SUB, DK), 1)
    small_ref[...] = jnp.where(lane == 0, bias, jnp.where(lane == 1, rate, 0.0))
    seats = query_in.shape[1]
    place = lax.axis_index("sp") * seats
    row = lax.broadcasted_iota(jnp.int32, (seats, DK), 0)
    col = lax.broadcasted_iota(jnp.int32, (seats, DK), 1)
    query = dot(query_in[...], jnp.where(col == row + place, 1.0, 0.0))
    forget = forget_in[...]
    size = forget.shape[1]
    wide = lax.broadcasted_iota(jnp.int32, (SUB, size), 0)
    slim = lax.broadcasted_iota(jnp.int32, (SUB, DK), 0)
    forget_out = jnp.zeros((SUB, size), f32)
    query_out = jnp.zeros((SUB, DK), f32)
    for h in range(heads):
        forget_out = jnp.where((lead ^ wide) == h, forget[h : h + 1], forget_out)
        query_out = jnp.where((lead ^ slim) == h, query[h : h + 1], query_out)
    forget_ref[...] = forget_out
    query_ref[...] = query_out
    for copy in copies:
        copy.wait()


def chunk_kernel(heads, begin, last, masks, prior, *refs):
    pieces = len(masks)
    piece_refs = refs[:pieces]
    wk_ref, wv_ref, wg_ref, small_ref, forget_ref = refs[pieces : pieces + 5]
    rest = refs[pieces + 5 :]
    sums = (None, None, None)
    if prior:
        sums, rest = tuple(ref[...] for ref in rest[:3]), rest[3:]
    if begin > 0:
        state_ref, rest = rest[0], rest[1:]
    if last:
        query_ref, rest = rest[0], rest[1:]
    gates, key_acc, value_acc = project(masks, piece_refs, wk_ref, wv_ref, wg_ref, sums)
    size = key_acc.shape[0]
    bias, rate = small_ref[:, 0:1], small_ref[:, 1:2]
    forget = forget_ref[:, begin : begin + size]
    beta_row = jax.nn.sigmoid(gates[0:SUB] + bias)
    log_row = forget - rate * jax.nn.softplus(gates[SUB : 2 * SUB])
    row = lax.broadcasted_iota(jnp.int32, (size, size), 0)
    col = lax.broadcasted_iota(jnp.int32, (size, size), 1)
    strict = row > col
    after = dot_ones(log_row, jnp.where(strict, 1.0, 0.0))
    keep = jnp.exp(after[:, 0:1] + log_row[:, 0:1])
    remain = jnp.exp(after)

    key_raw = key_acc.astype(bf16).astype(f32)
    value_raw = value_acc.astype(bf16)
    keys, lowers = [], []
    for h in range(heads):
        kw = key_raw[:, h * DK : (h + 1) * DK]
        ku = kw * lax.rsqrt(jnp.sum(kw * kw, axis=-1, keepdims=True) + norm_eps)
        keys.append(ku)
        lowers.append(jnp.where(strict, dot_nt(ku, ku), 0.0) * beta_row[h : h + 1, :])
    if begin > 0:
        states = [state_ref[h] for h in range(heads)]
    else:
        kr = lax.broadcasted_iota(jnp.int32, (DK, DV + DK), 0)
        kc = lax.broadcasted_iota(jnp.int32, (DK, DV + DK), 1)
        states = [jnp.where(kc == kr + DV, 1.0, 0.0)] * heads
    rights, turned = [], []
    for h in range(heads):
        value = value_raw[:, h * DV : (h + 1) * DV]
        padded = jnp.concatenate([value, jnp.zeros((size, DK), bf16)], axis=1)
        seen = dot(keys[h], states[h]).astype(bf16)
        rights.append(jnp.concatenate([padded, seen], axis=0))
        turned.append(keys[h].T * beta_row[h : h + 1, :])
    fresh = []
    for h, inverse in enumerate(unit_inverses(lowers, size)):
        ours, theirs = inverse * remain[h : h + 1, :], inverse * -keep[h : h + 1, :]
        if size % DK == 0:
            fresh.append(dot(jnp.concatenate([ours, theirs], axis=1), rights[h]))
        else:
            fresh.append(dot(ours, rights[h][:size]) + dot(theirs, rights[h][size:]))
    for h in range(heads):
        new = keep[h : h + 1, :] * states[h] + dot(turned[h], fresh[h])
        if last:
            rest[h][...] = passed_on(new, jnp.broadcast_to(query_ref[h : h + 1, :], (SUB, DK)))
        else:
            rest[-1][h] = new


def compose(pairs, product):
    while len(pairs) > 1:
        merged = []
        for early, late in zip(pairs[0::2], pairs[1::2]):
            new = product(late[:, DV:], early)
            merged.append(jnp.concatenate([new[:, :DV] + late[:, :DV], new[:, DV:]], axis=1))
        pairs, product = merged, dot3
    return pairs[0]


def pad_rows(x, rows):
    return jnp.concatenate([x, jnp.zeros((rows - x.shape[0], x.shape[1]), x.dtype)], axis=0)


def late_side(mask):
    return lax.rem(lax.div(lax.axis_index("sp"), jnp.int32(mask)), jnp.int32(2)) == 1


def finish(total, query, out):
    out[0][...] = total
    out[1][...] = query
    if len(out) == 2:
        return
    half = DK // 2
    through = dot3(query, total)
    a, b = total[:, DV:], total[:, :DV]
    high = late_side(lax.axis_size("sp") // 2)
    body = jnp.where(high, jnp.concatenate([a[:half], b[:half]], axis=0), b)
    ah, al = split(through[0:1, DV:])
    bh, bl = split(through[0:1, :DV])
    tail = [query[0:1]] + [x.astype(f32) for x in (ah, al, bh, bl)]
    tail = pad_rows(jnp.concatenate(tail, axis=0), 2 * SUB)
    out[2][0:DK, :] = body.astype(bf16)
    out[2][DK:, :] = tail.astype(bf16)


def passed_on(total, query):
    return jnp.concatenate([total[:, :DV], total[:, DV:], query, query], axis=0).astype(bf16)


def received(ref):
    total = jnp.concatenate([ref[:DK, :], ref[DK : 2 * DK, :]], axis=1)
    return total.astype(f32), ref[2 * DK :, :].astype(f32)[:SUB]


def compose_kernel(heads, final, *refs):
    own_ref, got = refs[0], refs[1:heads]
    out, scratch = refs[heads:-1], refs[-1]
    lead = lax.axis_index("sp") % heads
    scratch[lead], query = received(own_ref)
    for k in range(1, heads):
        scratch[lead ^ k], asked = received(got[k - 1])
        query = query + asked
    total = compose([scratch[i] for i in range(heads)], dot)
    if final:
        finish(total, query, out)
    else:
        out[0][...], out[1][...] = total, query
        out[2][...] = passed_on(total, query)


def merge_kernel(mask, final, own_ref, query_ref, got_ref, *out):
    high = late_side(mask)
    own, (got, asked) = own_ref[...], received(got_ref)
    query = query_ref[...] + asked
    early, late = jnp.where(high, got, own), jnp.where(high, own, got)
    total = compose([early, late], dot3)
    if final:
        finish(total, query, out)
    else:
        out[0][...], out[1][...] = total, query
        out[2][...] = passed_on(total, query)


def rows_kernel(heads, groups, rows, own_ref, query_ref, *refs):
    if groups > 1:
        got_ref, refs = refs[0], refs[1:]
    scratch = refs[-1]
    own, query = own_ref[...], query_ref[...]
    half = DK // 2
    place = lax.axis_index("sp")
    if groups > 1:
        high = late_side(lax.axis_size("sp") // 2)
        got = got_ref[...].astype(f32)
        a, b = own[:, DV:], own[:, :DV]
        early = jnp.where(high, got[:DK], b)
        late_a = jnp.where(high, a[half:], got[:half])
        late_b = jnp.where(high, b[half:], got[half:DK])
        tail = got[DK:]
        cross = dot3(jnp.broadcast_to(tail[0:1], (SUB, DK)), own)[0:1]
        through_a = jnp.where(high, cross[:, DV:], tail[1:2] + tail[2:3])
        through_b = jnp.where(high, cross[:, :DV], tail[3:4] + tail[4:5])
        both = dot3(pad_rows(jnp.concatenate([late_a, through_a], axis=0), half + SUB), early)
        state = both[:half] + late_b
        asked = jnp.where(high, query[:, half:], query[:, :half])
        read = dot3(asked, state)[0:1] + (both[half : half + 1] + through_b)
    else:
        state = own[:, :DV]
        read = dot3(query, state)[0:1]
    members = state.shape[0] // rows
    for i in range(members):
        scratch[i] = state[i * rows : (i + 1) * rows]
    place = place % members
    rh, rl = split(read)
    tail = pad_rows(jnp.concatenate([rh.astype(f32), rl.astype(f32)], axis=0), 16)
    for k in range(heads):
        body = scratch[place ^ k]
        refs[k][...] = jnp.concatenate([body, tail], axis=0).astype(bf16)


def final_kernel(heads, rows, gain_ref, *refs):
    lead = lax.axis_index("sp") % heads
    state_ref, read_ref, scratch = refs[heads:]
    for k in range(heads):
        part = refs[k][...]
        state_ref[lead ^ k] = part[:rows]
        wide = part[rows : rows + 2].astype(f32)
        scratch[lead ^ k] = jnp.broadcast_to(wide[0:1] + wide[1:2], (SUB, DV))
    raw = jnp.concatenate([scratch[h][0:1] for h in range(heads)], axis=0)
    norm = lax.rsqrt(jnp.mean(raw * raw, axis=-1, keepdims=True) + norm_eps)
    read_ref[...] = raw * norm * gain_ref[...].astype(f32)


def shape(dims, dtype=f32):
    return jax.ShapeDtypeStruct(dims, dtype)


vmem = pl.BlockSpec(memory_space=pltpu.VMEM)


def call(body, arrays, outs, scratch=(), mib=8, flops=0):
    return pl.pallas_call(
        body,
        out_shape=outs,
        in_specs=[vmem] * len(arrays),
        out_specs=jax.tree.map(lambda _: vmem, outs),
        scratch_shapes=list(scratch),
        compiler_params=pltpu.CompilerParams(vmem_limit_bytes=mib * 1024 * 1024),
        cost_estimate=pl.CostEstimate(flops=flops, bytes_accessed=0, transcendentals=0)
        if flops
        else None,
    )(*arrays)


def per_device(
    tokens,
    w_key,
    w_value,
    w_beta,
    w_decay,
    beta_bias,
    decay_rate,
    forgetting_increment,
    new_query,
    read_gain,
):
    heads = w_key.shape[1] // DK
    length, width = tokens.shape
    count = lax.axis_size("sp")
    ranks = lax.axis_size("tp")
    groups = count // heads
    rows = DK // count
    chunk = min(CHUNK, length)
    chunks = length // chunk
    moved_on = chunk // 4 if chunks > 1 and chunk % 64 == 0 else 0
    sizes = [chunk] * chunks
    sizes[0], sizes[-1] = sizes[0] + moved_on, sizes[-1] - moved_on
    begins = [sum(sizes[:c]) for c in range(chunks)]

    owns = [tokens[: sizes[0]]]
    later = lax.optimization_barrier(tokens)
    owns += [later[b : b + size] for b, size in zip(begins[1:], sizes[1:])]
    gathered = []
    for c in range(chunks):
        found = [(0, owns[c])]
        for hop in range(1, ranks // 2):
            found.append((2 * hop, swap(owns[c], "tp", 2 * hop)))
        found.append((1, swap(owns[c], "tp", 1)))
        found += [(m ^ 1, swap(x, "tp", 1)) for m, x in found[1:-1]]
        gathered.append(found)

    plain = [
        pltpu.with_memory_space_constraint(x, pltpu.HBM)
        for x in (
            w_key,
            w_value,
            w_beta.T,
            w_decay.T,
            beta_bias[None],
            decay_rate[None],
            forgetting_increment,
            new_query,
        )
    ]
    w_key, w_value, gate_weights, small, forget, query = pl.pallas_call(
        functools.partial(prepare_kernel, heads),
        out_shape=[
            shape(w_key.shape, bf16),
            shape(w_value.shape, bf16),
            shape((2 * SUB, w_beta.shape[0]), bf16),
            shape((SUB, DK)),
            shape((SUB, length)),
            shape((SUB, DK)),
        ],
        in_specs=[pl.BlockSpec(memory_space=pltpu.HBM)] * 8,
        out_specs=[vmem] * 6,
        scratch_shapes=[pltpu.VMEM(x.shape, x.dtype) for x in plain[2:]]
        + [pltpu.SemaphoreType.DMA((2 * heads + 6,))],
        compiler_params=pltpu.CompilerParams(vmem_limit_bytes=24 * 1024 * 1024),
    )(*plain)

    state = None
    flops = 2 * chunk * width * ranks * (2 * heads * DK + DK) + heads * 24 * 2 * chunk * chunk * DK
    weights = [w_key, w_value, gate_weights]

    def part(found, sums):
        size = found[0][1].shape[0]
        return call(
            functools.partial(part_kernel, tuple(m for m, _ in found), len(sums) > 0),
            [x for _, x in found] + weights + sums,
            [shape((2 * SUB, size)), shape((size, heads * DK)), shape((size, heads * DV))],
            mib=16,
            flops=2 * size * width * len(found) * (2 * heads * DK + DK),
        )

    for c in range(chunks):
        found = gathered[c]
        last = c == chunks - 1
        sums = []
        if c > 0:
            here = [f for f in found if f[0] < 2]
            found = [f for f in found if f[0] >= 2]
            sums = list(part(here, sums))
        if last and len(found) > 1:
            near = [f for f in found if f[0] % 2 == 0]
            found = [f for f in found if f[0] % 2 == 1]
            sums = list(part(near, sums))
        arrays = [x for _, x in found] + weights + [small, forget] + sums
        if c > 0:
            arrays.append(state)
        outs = [shape((heads, DK, DV + DK))]
        if last:
            arrays.append(query)
            outs = [shape((DK + DV + 2 * SUB, DK), bf16)] * heads
        result = call(
            functools.partial(
                chunk_kernel, heads, begins[c], last, tuple(m for m, _ in found), len(sums) > 0
            ),
            arrays,
            outs,
            mib=28,
            flops=flops,
        )
        state = result[-1]
    maps = result

    got = {}
    for k in reversed(range(1, heads)):
        got[k] = swap(maps[k], "sp", k)
    done = [shape((DK, DV + DK)), shape((SUB, DK))]
    open_ended = done + [shape((DK + DV + 2 * SUB, DK), bf16)]
    if groups > 1:
        done.append(shape((DK + 2 * SUB, DV), bf16))
    result = call(
        functools.partial(compose_kernel, heads, groups <= 2),
        [maps[0]] + [got[k] for k in range(1, heads)],
        done if groups <= 2 else open_ended,
        [pltpu.VMEM((heads, DK, DV + DK), f32)],
    )
    mask = heads
    while 2 * mask < count:
        final = 4 * mask == count
        result = call(
            functools.partial(merge_kernel, mask, final),
            [result[0], result[1], swap(result[2], "sp", mask)],
            done if final else open_ended,
        )
        mask *= 2
    arrays = list(result[:2])
    if groups > 1:
        arrays.append(swap(result[2], "sp", count // 2))
    members = count // 2 if groups > 1 else count
    parts = call(
        functools.partial(rows_kernel, heads, groups, rows),
        arrays,
        [shape((rows + 16, DV), bf16)] * heads,
        [pltpu.VMEM((members, rows, DV), f32)],
    )
    moved = {}
    for k in reversed(range(1, heads)):
        moved[k] = swap(parts[k], "sp", k)
    own_rows, first_read = call(
        functools.partial(final_kernel, heads, rows),
        [read_gain[None], parts[0]] + [moved[k] for k in range(1, heads)],
        [shape((heads, rows, DV), bf16), shape((heads, DV))],
        [pltpu.VMEM((heads, SUB, DV), f32)],
    )
    return (own_rows, first_read)


def solution(mesh):
    return jax.shard_map(
        per_device,
        mesh=mesh,
        in_specs=(
            P("sp", "tp"),
            P(None, "tp"),
            P(None, "tp"),
            P(),
            P(),
            P(),
            P(),
            P("tp", "sp"),
            P("tp", "sp"),
            P(),
        ),
        out_specs=(P("tp", "sp", None), P("tp", None)),
        check_vma=False,
    )
```

```python
import functools

import jax
import jax.numpy as jnp
from jax import lax
from jax.experimental import pallas as pl
from jax.experimental.pallas import tpu as pltpu
from jax.sharding import PartitionSpec as P


DK = 128
DV = 128
CHUNK = 128
SUB = 8

norm_eps = 1e-06
bf16 = jnp.bfloat16
f32 = jnp.float32


def flip(axis, mask):
    return [(i, i ^ mask) for i in range(lax.axis_size(axis))]


def swap(x, axis, mask):
    return lax.ppermute(x, axis, flip(axis, mask))


def dot(left, right):
    return jnp.dot(left.astype(bf16), right.astype(bf16), preferred_element_type=f32)


def split(x):
    high = x.astype(bf16)
    return high, (x - high.astype(f32)).astype(bf16)


def dot3(left, right):
    lh, ll = split(left)
    rh, rl = split(right)
    whole = dot(jnp.concatenate([lh, ll], axis=1), jnp.concatenate([rh, rh], axis=0))
    return whole + dot(lh, rl)


def dot_ones(left, ones):
    high, rest = split(left)
    mid = rest
    low = (left - high.astype(f32) - mid.astype(f32)).astype(bf16)
    n = left.shape[0]
    parts = jnp.concatenate([high.astype(f32), mid.astype(f32), low.astype(f32)], axis=0)
    out = dot(parts, ones)
    return out[:n] + out[n : 2 * n] + out[2 * n :]


def dot_nt(left, right):
    return lax.dot_general(
        left.astype(bf16), right.astype(bf16), (((1,), (1,)), ((), ())), preferred_element_type=f32
    )


def unit_inverses(lowers, size):
    row = lax.broadcasted_iota(jnp.int32, (size, size), 0)
    col = lax.broadcasted_iota(jnp.int32, (size, size), 1)
    width = min(16, size)
    near = (row // width) == (col // width)
    inner = [jnp.where(near, low, 0.0) for low in lowers]
    results = [jnp.where(row == col, 1.0, 0.0) - low for low in inner]
    if width > 2:
        results = series([dot(low, low) for low in inner], results, width, size)
    if width == size:
        return results
    powers = [dot(r, jnp.where(near, 0.0, low)) for r, low in zip(results, lowers)]
    if size // width == 2:
        return [r - dot(p, r) for r, p in zip(results, powers)]
    both = [dot(p, jnp.concatenate([p, r], axis=1)) for r, p in zip(results, powers)]
    results = [r - x[:, size:] for r, x in zip(results, both)]
    return series([x[:, :size] for x in both], results, size // width, size)


def series(powers, results, reach, size):
    covered = 2
    while 2 * covered < reach:
        both = [dot(p, jnp.concatenate([p, r], axis=1)) for r, p in zip(results, powers)]
        results = [r + x[:, size:] for r, x in zip(results, both)]
        powers = [x[:, :size] for x in both]
        covered *= 2
    return [r + dot(p, r) for r, p in zip(results, powers)]


def project(masks, piece_refs, wk_ref, wv_ref, wg_ref, sums):
    rank = lax.axis_index("tp")
    gates, keys, values = sums
    placed = []
    for m, ref in zip(masks, piece_refs):
        width = ref.shape[1]
        placed.append((pl.ds(pl.multiple_of((rank ^ m) * width, width), width), ref))
    for rows, ref in placed:
        g = dot_nt(wg_ref[:, rows], ref[...])
        gates = g if gates is None else gates + g
    for rows, ref in placed:
        k = jnp.dot(ref[...], wk_ref[rows, :], preferred_element_type=f32)
        keys = k if keys is None else keys + k
    for rows, ref in placed:
        v = jnp.dot(ref[...], wv_ref[rows, :], preferred_element_type=f32)
        values = v if values is None else values + v
    return gates, keys, values


def part_kernel(masks, prior, *refs):
    pieces = len(masks)
    weights, rest = refs[pieces : pieces + 3], refs[pieces + 3 :]
    sums = (None, None, None)
    if prior:
        sums, rest = tuple(ref[...] for ref in rest[:3]), rest[3:]
    for ref, x in zip(rest, project(masks, refs[:pieces], *weights, sums)):
        ref[...] = x


def prepare_kernel(heads, *refs):
    wk_hbm, wv_hbm = refs[:2]
    wk_ref, wv_ref, wg_ref, small_ref, forget_ref, query_ref = refs[8:14]
    few, sems = refs[14:20], refs[20]
    wb_ref, wd_ref, bias_ref, rate_ref, forget_in, query_in = few
    lead = lax.axis_index("sp") % heads
    first = lax.axis_index("tp") * heads
    early = [
        pltpu.make_async_copy(hbm, ref, sems.at[2 * heads + i])
        for i, (hbm, ref) in enumerate(zip(refs[2:8], few))
    ]
    copies = []
    for k in range(heads):
        source = pl.ds(pl.multiple_of((lead ^ k) * DK, DK), DK)
        target = pl.ds(k * DK, DK)
        for i, (hbm, ref) in enumerate(((wk_hbm, wk_ref), (wv_hbm, wv_ref))):
            copies.append(
                pltpu.make_async_copy(hbm.at[:, source], ref.at[:, target], sems.at[2 * k + i])
            )
    for copy in early + copies:
        copy.start()
    for copy in early:
        copy.wait()
    many = bias_ref.shape[1]
    row = lax.broadcasted_iota(jnp.int32, (2 * SUB, 2 * many), 0)
    col = lax.broadcasted_iota(jnp.int32, (2 * SUB, 2 * many), 1)
    k = row & (SUB - 1)
    wanted = first + (lead ^ k) + jnp.where(row >= SUB, many, 0)
    pick = jnp.where(jnp.logical_and(col == wanted, k < heads), 1.0, 0.0)
    both = jnp.concatenate([wb_ref[...], wd_ref[...]], axis=0)
    wg_ref[...] = dot(pick, both).astype(bf16)
    row = lax.broadcasted_iota(jnp.int32, (SUB, many), 0)
    col = lax.broadcasted_iota(jnp.int32, (SUB, many), 1)
    mine = col == first + (lead ^ row)
    bias = jnp.sum(jnp.where(mine, bias_ref[...], 0.0), axis=1, keepdims=True)
    rate = jnp.sum(jnp.where(mine, rate_ref[...], 0.0), axis=1, keepdims=True)
    lane = lax.broadcasted_iota(jnp.int32, (SUB, DK), 1)
    small_ref[...] = jnp.where(lane == 0, bias, jnp.where(lane == 1, rate, 0.0))
    seats = query_in.shape[1]
    place = lax.axis_index("sp") * seats
    row = lax.broadcasted_iota(jnp.int32, (seats, DK), 0)
    col = lax.broadcasted_iota(jnp.int32, (seats, DK), 1)
    query = dot(query_in[...], jnp.where(col == row + place, 1.0, 0.0))
    forget = forget_in[...]
    size = forget.shape[1]
    wide = lax.broadcasted_iota(jnp.int32, (SUB, size), 0)
    slim = lax.broadcasted_iota(jnp.int32, (SUB, DK), 0)
    forget_out = jnp.zeros((SUB, size), f32)
    query_out = jnp.zeros((SUB, DK), f32)
    for h in range(heads):
        forget_out = jnp.where((lead ^ wide) == h, forget[h : h + 1], forget_out)
        query_out = jnp.where((lead ^ slim) == h, query[h : h + 1], query_out)
    forget_ref[...] = forget_out
    query_ref[...] = query_out
    for copy in copies:
        copy.wait()


def chunk_kernel(heads, index, last, masks, prior, *refs):
    pieces = len(masks)
    piece_refs = refs[:pieces]
    wk_ref, wv_ref, wg_ref, small_ref, forget_ref = refs[pieces : pieces + 5]
    rest = refs[pieces + 5 :]
    sums = (None, None, None)
    if prior:
        sums, rest = tuple(ref[...] for ref in rest[:3]), rest[3:]
    if index > 0:
        state_ref, rest = rest[0], rest[1:]
    if last:
        query_ref, rest = rest[0], rest[1:]
    gates, key_acc, value_acc = project(masks, piece_refs, wk_ref, wv_ref, wg_ref, sums)
    size = key_acc.shape[0]
    bias, rate = small_ref[:, 0:1], small_ref[:, 1:2]
    forget = forget_ref[:, index * size : (index + 1) * size]
    beta_row = jax.nn.sigmoid(gates[0:SUB] + bias)
    log_row = forget - rate * jax.nn.softplus(gates[SUB : 2 * SUB])
    row = lax.broadcasted_iota(jnp.int32, (size, size), 0)
    col = lax.broadcasted_iota(jnp.int32, (size, size), 1)
    strict = row > col
    after = dot_ones(log_row, jnp.where(strict, 1.0, 0.0))
    keep = jnp.exp(after[:, 0:1] + log_row[:, 0:1])
    remain = jnp.exp(after)

    key_raw = key_acc.astype(bf16).astype(f32)
    value_raw = value_acc.astype(bf16)
    keys, lowers = [], []
    for h in range(heads):
        kw = key_raw[:, h * DK : (h + 1) * DK]
        ku = kw * lax.rsqrt(jnp.sum(kw * kw, axis=-1, keepdims=True) + norm_eps)
        keys.append(ku)
        lowers.append(jnp.where(strict, dot_nt(ku, ku), 0.0) * beta_row[h : h + 1, :])
    if index > 0:
        states = [state_ref[h] for h in range(heads)]
    else:
        kr = lax.broadcasted_iota(jnp.int32, (DK, DV + DK), 0)
        kc = lax.broadcasted_iota(jnp.int32, (DK, DV + DK), 1)
        states = [jnp.where(kc == kr + DV, 1.0, 0.0)] * heads
    rights, turned = [], []
    for h in range(heads):
        value = value_raw[:, h * DV : (h + 1) * DV]
        padded = jnp.concatenate([value, jnp.zeros((size, DK), bf16)], axis=1)
        seen = dot(keys[h], states[h]).astype(bf16)
        rights.append(jnp.concatenate([padded, seen], axis=0))
        turned.append(keys[h].T * beta_row[h : h + 1, :])
    fresh = []
    for h, inverse in enumerate(unit_inverses(lowers, size)):
        left = jnp.concatenate(
            [inverse * remain[h : h + 1, :], inverse * -keep[h : h + 1, :]], axis=1
        )
        fresh.append(dot(left, rights[h]))
    for h in range(heads):
        new = keep[h : h + 1, :] * states[h] + dot(turned[h], fresh[h])
        if last:
            rest[h][...] = passed_on(new, jnp.broadcast_to(query_ref[h : h + 1, :], (SUB, DK)))
        else:
            rest[-1][h] = new


def compose(pairs, product):
    while len(pairs) > 1:
        merged = []
        for early, late in zip(pairs[0::2], pairs[1::2]):
            new = product(late[:, DV:], early)
            merged.append(jnp.concatenate([new[:, :DV] + late[:, :DV], new[:, DV:]], axis=1))
        pairs, product = merged, dot3
    return pairs[0]


def pad_rows(x, rows):
    return jnp.concatenate([x, jnp.zeros((rows - x.shape[0], x.shape[1]), x.dtype)], axis=0)


def late_side(mask):
    return lax.rem(lax.div(lax.axis_index("sp"), jnp.int32(mask)), jnp.int32(2)) == 1


def finish(total, query, out):
    out[0][...] = total
    out[1][...] = query
    if len(out) == 2:
        return
    half = DK // 2
    through = dot3(query, total)
    a, b = total[:, DV:], total[:, :DV]
    high = late_side(lax.axis_size("sp") // 2)
    body = jnp.where(high, jnp.concatenate([a[:half], b[:half]], axis=0), b)
    ah, al = split(through[0:1, DV:])
    bh, bl = split(through[0:1, :DV])
    tail = [query[0:1]] + [x.astype(f32) for x in (ah, al, bh, bl)]
    tail = pad_rows(jnp.concatenate(tail, axis=0), 2 * SUB)
    out[2][0:DK, :] = body.astype(bf16)
    out[2][DK:, :] = tail.astype(bf16)


def passed_on(total, query):
    return jnp.concatenate([total[:, :DV], total[:, DV:], query, query], axis=0).astype(bf16)


def received(ref):
    total = jnp.concatenate([ref[:DK, :], ref[DK : 2 * DK, :]], axis=1)
    return total.astype(f32), ref[2 * DK :, :].astype(f32)[:SUB]


def compose_kernel(heads, final, *refs):
    own_ref, got = refs[0], refs[1:heads]
    out, scratch = refs[heads:-1], refs[-1]
    lead = lax.axis_index("sp") % heads
    scratch[lead], query = received(own_ref)
    for k in range(1, heads):
        scratch[lead ^ k], asked = received(got[k - 1])
        query = query + asked
    total = compose([scratch[i] for i in range(heads)], dot)
    if final:
        finish(total, query, out)
    else:
        out[0][...], out[1][...] = total, query
        out[2][...] = passed_on(total, query)


def merge_kernel(mask, final, own_ref, query_ref, got_ref, *out):
    high = late_side(mask)
    own, (got, asked) = own_ref[...], received(got_ref)
    query = query_ref[...] + asked
    early, late = jnp.where(high, got, own), jnp.where(high, own, got)
    total = compose([early, late], dot3)
    if final:
        finish(total, query, out)
    else:
        out[0][...], out[1][...] = total, query
        out[2][...] = passed_on(total, query)


def rows_kernel(heads, groups, rows, own_ref, query_ref, *refs):
    if groups > 1:
        got_ref, refs = refs[0], refs[1:]
    scratch = refs[-1]
    own, query = own_ref[...], query_ref[...]
    half = DK // 2
    place = lax.axis_index("sp")
    if groups > 1:
        high = late_side(lax.axis_size("sp") // 2)
        got = got_ref[...].astype(f32)
        a, b = own[:, DV:], own[:, :DV]
        early = jnp.where(high, got[:DK], b)
        late_a = jnp.where(high, a[half:], got[:half])
        late_b = jnp.where(high, b[half:], got[half:DK])
        tail = got[DK:]
        cross = dot3(jnp.broadcast_to(tail[0:1], (SUB, DK)), own)[0:1]
        through_a = jnp.where(high, cross[:, DV:], tail[1:2] + tail[2:3])
        through_b = jnp.where(high, cross[:, :DV], tail[3:4] + tail[4:5])
        both = dot3(pad_rows(jnp.concatenate([late_a, through_a], axis=0), half + SUB), early)
        state = both[:half] + late_b
        asked = jnp.where(high, query[:, half:], query[:, :half])
        read = dot3(asked, state)[0:1] + (both[half : half + 1] + through_b)
    else:
        state = own[:, :DV]
        read = dot3(query, state)[0:1]
    members = state.shape[0] // rows
    for i in range(members):
        scratch[i] = state[i * rows : (i + 1) * rows]
    place = place % members
    rh, rl = split(read)
    tail = pad_rows(jnp.concatenate([rh.astype(f32), rl.astype(f32)], axis=0), 16)
    for k in range(heads):
        body = scratch[place ^ k]
        refs[k][...] = jnp.concatenate([body, tail], axis=0).astype(bf16)


def final_kernel(heads, rows, gain_ref, *refs):
    lead = lax.axis_index("sp") % heads
    state_ref, read_ref, scratch = refs[heads:]
    for k in range(heads):
        part = refs[k][...]
        state_ref[lead ^ k] = part[:rows]
        wide = part[rows : rows + 2].astype(f32)
        scratch[lead ^ k] = jnp.broadcast_to(wide[0:1] + wide[1:2], (SUB, DV))
    raw = jnp.concatenate([scratch[h][0:1] for h in range(heads)], axis=0)
    norm = lax.rsqrt(jnp.mean(raw * raw, axis=-1, keepdims=True) + norm_eps)
    read_ref[...] = raw * norm * gain_ref[...].astype(f32)


def shape(dims, dtype=f32):
    return jax.ShapeDtypeStruct(dims, dtype)


vmem = pl.BlockSpec(memory_space=pltpu.VMEM)


def call(body, arrays, outs, scratch=(), mib=8, flops=0):
    return pl.pallas_call(
        body,
        out_shape=outs,
        in_specs=[vmem] * len(arrays),
        out_specs=jax.tree.map(lambda _: vmem, outs),
        scratch_shapes=list(scratch),
        compiler_params=pltpu.CompilerParams(vmem_limit_bytes=mib * 1024 * 1024),
        cost_estimate=pl.CostEstimate(flops=flops, bytes_accessed=0, transcendentals=0)
        if flops
        else None,
    )(*arrays)


def per_device(
    tokens,
    w_key,
    w_value,
    w_beta,
    w_decay,
    beta_bias,
    decay_rate,
    forgetting_increment,
    new_query,
    read_gain,
):
    heads = w_key.shape[1] // DK
    length, width = tokens.shape
    count = lax.axis_size("sp")
    ranks = lax.axis_size("tp")
    groups = count // heads
    rows = DK // count
    chunk = min(CHUNK, length)
    chunks = length // chunk

    owns = [tokens[:chunk]]
    later = lax.optimization_barrier(tokens)
    owns += [later[c * chunk : (c + 1) * chunk] for c in range(1, chunks)]
    gathered = []
    for c in range(chunks):
        found = [(0, owns[c])]
        for hop in range(1, ranks // 2):
            found.append((2 * hop, swap(owns[c], "tp", 2 * hop)))
        found.append((1, swap(owns[c], "tp", 1)))
        found += [(m ^ 1, swap(x, "tp", 1)) for m, x in found[1:-1]]
        gathered.append(found)

    plain = [
        pltpu.with_memory_space_constraint(x, pltpu.HBM)
        for x in (
            w_key,
            w_value,
            w_beta.T,
            w_decay.T,
            beta_bias[None],
            decay_rate[None],
            forgetting_increment,
            new_query,
        )
    ]
    w_key, w_value, gate_weights, small, forget, query = pl.pallas_call(
        functools.partial(prepare_kernel, heads),
        out_shape=[
            shape(w_key.shape, bf16),
            shape(w_value.shape, bf16),
            shape((2 * SUB, w_beta.shape[0]), bf16),
            shape((SUB, DK)),
            shape((SUB, length)),
            shape((SUB, DK)),
        ],
        in_specs=[pl.BlockSpec(memory_space=pltpu.HBM)] * 8,
        out_specs=[vmem] * 6,
        scratch_shapes=[pltpu.VMEM(x.shape, x.dtype) for x in plain[2:]]
        + [pltpu.SemaphoreType.DMA((2 * heads + 6,))],
        compiler_params=pltpu.CompilerParams(vmem_limit_bytes=24 * 1024 * 1024),
    )(*plain)

    state = None
    flops = 2 * chunk * width * ranks * (2 * heads * DK + DK) + heads * 24 * 2 * chunk * chunk * DK
    weights = [w_key, w_value, gate_weights]
    sums_shape = [shape((2 * SUB, chunk)), shape((chunk, heads * DK)), shape((chunk, heads * DV))]

    def part(found, sums):
        return call(
            functools.partial(part_kernel, tuple(m for m, _ in found), len(sums) > 0),
            [x for _, x in found] + weights + sums,
            sums_shape,
            mib=16,
            flops=2 * chunk * width * len(found) * (2 * heads * DK + DK),
        )

    for c in range(chunks):
        found = gathered[c]
        last = c == chunks - 1
        sums = []
        if c > 0:
            here = [f for f in found if f[0] < 2]
            found = [f for f in found if f[0] >= 2]
            sums = list(part(here, sums))
        if last and len(found) > 1:
            near = [f for f in found if f[0] % 2 == 0]
            found = [f for f in found if f[0] % 2 == 1]
            sums = list(part(near, sums))
        arrays = [x for _, x in found] + weights + [small, forget] + sums
        if c > 0:
            arrays.append(state)
        outs = [shape((heads, DK, DV + DK))]
        if last:
            arrays.append(query)
            outs = [shape((DK + DV + 2 * SUB, DK), bf16)] * heads
        result = call(
            functools.partial(
                chunk_kernel, heads, c, last, tuple(m for m, _ in found), len(sums) > 0
            ),
            arrays,
            outs,
            mib=28,
            flops=flops,
        )
        state = result[-1]
    maps = result

    got = {}
    for k in reversed(range(1, heads)):
        got[k] = swap(maps[k], "sp", k)
    done = [shape((DK, DV + DK)), shape((SUB, DK))]
    open_ended = done + [shape((DK + DV + 2 * SUB, DK), bf16)]
    if groups > 1:
        done.append(shape((DK + 2 * SUB, DV), bf16))
    result = call(
        functools.partial(compose_kernel, heads, groups <= 2),
        [maps[0]] + [got[k] for k in range(1, heads)],
        done if groups <= 2 else open_ended,
        [pltpu.VMEM((heads, DK, DV + DK), f32)],
    )
    mask = heads
    while 2 * mask < count:
        final = 4 * mask == count
        result = call(
            functools.partial(merge_kernel, mask, final),
            [result[0], result[1], swap(result[2], "sp", mask)],
            done if final else open_ended,
        )
        mask *= 2
    arrays = list(result[:2])
    if groups > 1:
        arrays.append(swap(result[2], "sp", count // 2))
    members = count // 2 if groups > 1 else count
    parts = call(
        functools.partial(rows_kernel, heads, groups, rows),
        arrays,
        [shape((rows + 16, DV), bf16)] * heads,
        [pltpu.VMEM((members, rows, DV), f32)],
    )
    moved = {}
    for k in reversed(range(1, heads)):
        moved[k] = swap(parts[k], "sp", k)
    own_rows, first_read = call(
        functools.partial(final_kernel, heads, rows),
        [read_gain[None], parts[0]] + [moved[k] for k in range(1, heads)],
        [shape((heads, rows, DV), bf16), shape((heads, DV))],
        [pltpu.VMEM((heads, SUB, DV), f32)],
    )
    return (own_rows, first_read)


def solution(mesh):
    return jax.shard_map(
        per_device,
        mesh=mesh,
        in_specs=(
            P("sp", "tp"),
            P(None, "tp"),
            P(None, "tp"),
            P(),
            P(),
            P(),
            P(),
            P("tp", "sp"),
            P("tp", "sp"),
            P(),
        ),
        out_specs=(P("tp", "sp", None), P("tp", None)),
        check_vma=False,
    )
```
